32 devices in a mesh: sp: 16 (over z, y, x), tp: 2 (over core).
Axes of the slice: x: 2, y: 2, z: 4, core: 2. Of those that a mesh axis runs over, the one named last changes fastest.
Arguments:
- tokens: bfloat16 [16384, 2048], P('sp', 'tp'), may hold values from -6 to 6
- norm_gain: float32 [2048], replicated, may hold values from 0.1 to 1.9
- w_conv_a: bfloat16 [2048, 1024], P('sp', 'tp'), may hold values from -0.125 to 0.125
- w_conv_gate: bfloat16 [2048, 1024], P('sp', 'tp'), may hold values from -0.125 to 0.125
- conv_weight: float32 [31, 1024], P(None, 'tp'), may hold values from -16 to 16
- conv_gain: float32 [1024], P('tp'), may hold values from 0.1 to 1.9
- w_query: bfloat16 [2048, 512], P('sp', 'tp'), may hold values from -0.125 to 0.125
- w_key: bfloat16 [2048, 512], P('sp', 'tp'), may hold values from -0.125 to 0.125
- w_value: bfloat16 [2048, 1024], P('sp', 'tp'), may hold values from -0.125 to 0.125
- w_outgate: bfloat16 [2048, 1024], P('sp', 'tp'), may hold values from -0.125 to 0.125
- w_decay: bfloat16 [2048, 512], P('sp', 'tp'), may hold values from -0.125 to 0.125
- decay_bias: float32 [512], P('tp'), may hold values from 0 to 12
- decay_extra: float32 [16384, 512], P('sp', 'tp'), may hold values from -2 to 0
- head_gain: float32 [128], replicated, may hold values from 0.1 to 1.9
- init_state: float32 [8, 64, 128], P('tp'), may hold values from -768 to 768
- w_out_conv: bfloat16 [1024, 2048], P('tp', 'sp'), may hold values from -0.125 to 0.125
- w_out_gla: bfloat16 [1024, 2048], P('tp', 'sp'), may hold values from -0.125 to 0.125
Outputs:
- mixed: bfloat16 [16384, 2048], P(('sp', 'tp'))
The draws below stay inside these ranges and needn't reach their ends.
All inputs are finite; a program needn't handle non-finite values.
Results may differ from the reference program's by a relative error of at most 0.022.
Values may be sent and summed in bfloat16 or wider, within the bound.
A program may use at most 128 MiB of HBM per device.

```python
import jax
import jax.numpy as jnp
from jax import lax

D = 2048
D_CONV = 1024
HEADS = 8
HK = 64
HV = 128
KERNEL = 31
BLOCK = 64
TOK_DEV = 1024
SEQUENCE_TOKENS = 16384
GLA_K = 512
GLA_V = 1024
N_TP = 2


def draw_conv_weight(key, part):
    key_base = jax.random.fold_in(key, 0)
    base = jax.random.normal(key_base, (KERNEL, D_CONV), jnp.float32) * KERNEL ** (-0.5)
    rising = 3.0 ** (jnp.arange(D_CONV, dtype=jnp.float32) / (D_CONV - 1))
    return base * rising[None, :]


def draw_decay_bias(key, part):
    key_pick, key_fast, key_slow = jax.random.split(key, 3)
    fast_share = 0.5
    fast_head = jax.random.bernoulli(key_pick, fast_share, (HEADS,))
    fast_values = jax.random.uniform(key_fast, (HEADS, HK), jnp.float32, 0.0, 1.0)
    slow_values = jax.random.uniform(key_slow, (HEADS, HK), jnp.float32, 8.0, 12.0)
    return jnp.where(fast_head[:, None], fast_values, slow_values).reshape(HEADS * HK)


def draw_decay_extra(key, part):
    key_factor, key_location, key_width, key_channel = jax.random.split(key, 4)
    factor = jax.random.uniform(key_factor, (SEQUENCE_TOKENS // TOK_DEV, 1), jnp.float32, 1.0, 3.0)
    row_each = jnp.repeat(factor, TOK_DEV, axis=0)
    channel_index = jax.random.uniform(key_channel, (1, HEADS * HK), jnp.float32, 0.5, 1.5)
    spike_locations = jax.random.randint(key_location, (3,), 0, SEQUENCE_TOKENS)
    spike_depth = jax.random.uniform(key_width, (3, 1), jnp.float32, 0.22, 0.5)
    spike_events = (jnp.arange(SEQUENCE_TOKENS)[:, None] == spike_locations[None, :]).astype(jnp.float32)
    return -(0.4 / SEQUENCE_TOKENS) * row_each * channel_index - jnp.dot(spike_events, spike_depth)


def block_scale(rng, extent, cuts, least, high):
    def one(dim, shards_of):
        steps = jax.random.uniform(jax.random.fold_in(jax.random.fold_in(rng, 6), dim), (shards_of,), jnp.float32, least / len(cuts), high / len(cuts))
        return jnp.repeat(jnp.exp(steps), extent[dim] // shards_of).reshape((-1,) + (1,) * (len(extent) - dim - 1))

    factor_of = one(*cuts[0])
    for cut in cuts[1:]:
        factor_of = factor_of * one(*cut)
    return factor_of


def bell_draw(key, shape, scale, most, shards=(), kind=jnp.bfloat16):
    entries = jax.random.normal(key, shape, jnp.float32) * scale
    if len(shards) > 0:
        entries = block_scale(key, shape, shards, -0.22, 0.18) * entries
    return jnp.clip(entries, min=-most, max=most).astype(kind)


def setup_inputs(seed: int = 0) -> dict:
    streams_of = jax.random.split(jax.random.key(seed), 18)
    return {
        "tokens": bell_draw(streams_of[0], (SEQUENCE_TOKENS, D), 1.0, 6.0, ((0, 16), (1, 2))),
        "norm_gain": jnp.clip(1.0 + 0.18 * jax.random.normal(streams_of[1], (D,), jnp.float32), 0.1, 1.9),
        "w_conv_a": bell_draw(streams_of[2], (D, D_CONV), D ** -0.5, 0.125, ((0, 16), (1, 2))),
        "w_conv_gate": bell_draw(streams_of[3], (D, D_CONV), D ** -0.5, 0.125, ((0, 16), (1, 2))),
        "conv_weight": draw_conv_weight(jax.random.fold_in(streams_of[17], 71), 0),
        "conv_gain": jnp.clip(1.0 + 0.18 * jax.random.normal(streams_of[5], (D_CONV,), jnp.float32), 0.1, 1.9),
        "w_query": bell_draw(streams_of[6], (D, GLA_K), D ** -0.5, 0.125, ((0, 16), (1, 2))),
        "w_key": bell_draw(streams_of[7], (D, GLA_K), D ** -0.5, 0.125, ((0, 16), (1, 2))),
        "w_value": bell_draw(streams_of[8], (D, GLA_V), D ** -0.5, 0.125, ((0, 16), (1, 2))),
        "w_outgate": bell_draw(streams_of[9], (D, GLA_V), D ** -0.5, 0.125, ((0, 16), (1, 2))),
        "w_decay": bell_draw(streams_of[10], (D, GLA_K), D ** -0.5, 0.125, ((0, 16), (1, 2))),
        "decay_bias": draw_decay_bias(jax.random.fold_in(streams_of[17], 71), 0),
        "decay_extra": draw_decay_extra(jax.random.fold_in(streams_of[17], 71), 0),
        "head_gain": jnp.clip(1.0 + 0.18 * jax.random.normal(streams_of[13], (HV,), jnp.float32), 0.1, 1.9),
        "init_state": bell_draw(streams_of[14], (HEADS, HK, HV), (SEQUENCE_TOKENS ** 0.5), 768.0, ((0, 2),), jnp.float32),
        "w_out_conv": bell_draw(streams_of[15], (D_CONV, D), (D_CONV + GLA_V) ** -0.5, 0.125, ((0, 2), (1, 16))),
        "w_out_gla": bell_draw(streams_of[16], (GLA_V, D), (D_CONV + GLA_V) ** -0.5, 0.125, ((0, 2), (1, 16))),
    }


epsilon = 1e-06
gate_divisor = 16.0
highest_precision = lax.Precision.HIGHEST

def project(hidden, weight):
    return jnp.dot(hidden, weight, preferred_element_type=jnp.float32)

def rounded(values_f32):
    return lax.optimization_barrier(values_f32.astype(jnp.bfloat16)).astype(jnp.float32)

def reference(tokens, norm_gain, w_conv_a, w_conv_gate, conv_weight, conv_gain, w_query, w_key, w_value, w_outgate, w_decay, decay_bias, decay_extra, head_gain, init_state, w_out_conv, w_out_gla):
    widened = tokens.astype(jnp.float32)
    normed = (widened * lax.rsqrt(lax.optimization_barrier(jnp.mean(widened * widened, axis=-1, keepdims=True)) + epsilon) * norm_gain).astype(jnp.bfloat16)
    conv_a = rounded(project(normed, w_conv_a))
    conv_gate = rounded(project(normed, w_conv_gate))
    query = rounded(project(normed, w_query))
    keys = rounded(project(normed, w_key))
    values = rounded(project(normed, w_value))
    out_gate = rounded(project(normed, w_outgate))
    decay_pre = project(normed, w_decay)
    gated = rounded(conv_a * jax.nn.sigmoid(conv_gate))
    padded = jnp.pad(gated, ((KERNEL - 1, 0), (0, 0)))
    conv_sum = jnp.zeros((SEQUENCE_TOKENS, D_CONV), jnp.float32)
    for tap_index in range(KERNEL):
        conv_sum = conv_sum + conv_weight[tap_index][None, :] * padded[tap_index:tap_index + SEQUENCE_TOKENS]
    mean_val = lax.optimization_barrier(jnp.mean(conv_sum, axis=-1, keepdims=True))
    square_mean = lax.optimization_barrier(jnp.mean(conv_sum * conv_sum, axis=-1, keepdims=True))
    conv_norm = (conv_sum - mean_val) * lax.rsqrt(square_mean - mean_val * mean_val + epsilon) * conv_gain
    conv_out = jax.nn.silu(conv_norm).astype(jnp.bfloat16)
    log_decay = jax.nn.log_sigmoid(decay_pre + decay_bias) / gate_divisor + decay_extra
    blocks = SEQUENCE_TOKENS // BLOCK

    def to_heads(array, width):
        return array.astype(jnp.float32).reshape(blocks, BLOCK, HEADS, width).transpose(0, 2, 1, 3)
    query_heads = to_heads(query, HK) * HK ** (-0.5)
    key_heads = to_heads(keys, HK)
    value_heads = to_heads(values, HV)
    cum_log = jnp.cumsum(to_heads(log_decay, HK), axis=2)
    block_total = cum_log[:, :, -1:, :]
    query_decayed = query_heads * jnp.exp(cum_log)
    key_inverse = key_heads * jnp.exp(-cum_log)
    key_to_end = key_heads * jnp.exp(block_total - cum_log)
    causal = jnp.tril(jnp.ones((BLOCK, BLOCK), dtype=bool))
    scores = jnp.where(causal, jnp.einsum('nhik,nhjk->nhij', query_decayed, key_inverse, precision=highest_precision), 0.0)
    within = jnp.einsum('nhij,nhjv->nhiv', scores, value_heads, precision=highest_precision)

    def advance(state_current, block_items):
        query_block, key_block, value_block, decay_block = block_items
        carried_state = jnp.einsum('yau,yub->yab', query_block, state_current, precision=highest_precision)
        state_following = state_current * decay_block[:, 0, :, None] + jnp.einsum('tie,tis->tes', key_block, value_block, precision=highest_precision)
        return (state_following, carried_state)
    final_state, carried_out = lax.scan(advance, init_state.astype(jnp.float32), (query_decayed, key_to_end, value_heads, jnp.exp(block_total)))
    attn = within + carried_out
    normal_attn = attn * lax.rsqrt(lax.optimization_barrier(jnp.mean(attn * attn, axis=-1, keepdims=True)) + epsilon) * head_gain
    normal_attn = normal_attn.transpose(0, 2, 1, 3).reshape(SEQUENCE_TOKENS, HEADS * HV)
    gla_out = (normal_attn * jax.nn.silu(out_gate)).astype(jnp.bfloat16)
    conv_share = D_CONV // N_TP
    value_share = HEADS * HV // N_TP
    totals = jnp.zeros((SEQUENCE_TOKENS, D), jnp.float32)
    for group_index in range(N_TP):
        partial_value = project(conv_out[:, group_index * conv_share:(group_index + 1) * conv_share], w_out_conv[group_index * conv_share:(group_index + 1) * conv_share])
        partial_value = partial_value + project(gla_out[:, group_index * value_share:(group_index + 1) * value_share], w_out_gla[group_index * value_share:(group_index + 1) * value_share])
        totals = totals + rounded(partial_value)
    return totals.astype(jnp.bfloat16)
```

```python
import functools

import jax
import jax.numpy as jnp
from jax import lax
from jax.experimental import pallas as pl
from jax.experimental.pallas import tpu as pltpu
from jax.sharding import PartitionSpec as P

D_CONV = 1024
HK = 64
HV = 128
BLOCK = 64

epsilon = 1e-06
gate_divisor = 16.0

MESH = pl.DeviceIdType.MESH


def dot(a, b, dims):
    return lax.dot_general(a, b, (dims, ((), ())), preferred_element_type=jnp.float32)


def folded(n_sp, n_tp):
    return n_sp == 16 and n_tp == 2


class Mover:
    def __init__(self):
        self.me = lax.axis_index("sp")
        self.tp = lax.axis_index("tp")
        self.z, self.y, self.x = self.me // 4, (self.me // 2) % 2, self.me % 2
        self.other = {"x": self.me + 1 - 2 * self.x, "y": self.me + 2 - 4 * self.y}
        self.sent = []

    def copy(self, source, target, send, recv, place, core=None):
        core = self.tp if core is None else core
        return pltpu.make_async_remote_copy(
            src_ref=source, dst_ref=target, send_sem=send, recv_sem=recv, device_id=(place, core), device_id_type=MESH
        )

    def piece(self, j):
        z = self.z
        return (z, z + 1 - 2 * (z % 2), 2 - z // 2, 3 - 3 * (z // 2))[j]


class Flow:
    def __init__(self, mover, number, view, first, sems):
        self.m, self.number, self.view, self.first = mover, number, view, first
        self.last = {"x": "y", "y": "x"}[first]
        self.sems = sems

    def own(self, p):
        return self.view(p, self.m.y, self.m.x)

    def pair(self, p):
        every = slice(None)
        return self.view(p, self.m.y, every) if self.first == "x" else self.view(p, every, self.m.x)

    def first_copy(self, p):
        own = self.own(p)
        fs, fr = self.sems["first_send"], self.sems["first_recv"]
        return self.m.copy(own, own, fs.at[self.number, p], fr.at[self.number, p], self.m.other[self.first])

    def last_copy(self, p):
        pair = self.pair(p)
        ls, lr = self.sems["last_send"], self.sems["last_recv"]
        return self.m.copy(pair, pair, ls.at[self.number, p], lr.at[self.number, p], self.m.other[self.last])


class Line:
    def __init__(self, mover, number, view, sems):
        self.m, self.number, self.view, self.sems = mover, number, view, sems

    def up(self, p):
        return self.m.copy(
            self.view(p), self.view(p), self.sems["up_send"].at[self.number, p], self.sems["z_recv"].at[self.number, p],
            self.m.me + 4,
        )

    def down(self, p):
        return self.m.copy(
            self.view(p), self.view(p), self.sems["down_send"].at[self.number, p],
            self.sems["z_recv"].at[self.number, p], self.m.me - 4,
        )

    def start_own(self):
        z = self.m.z

        @pl.when(z < 3)
        def _():
            self.up(z).start()

        @pl.when(z > 0)
        def _():
            self.down(z).start()

    def relay(self, step, then):
        z = self.m.z

        @pl.when(z >= step)
        def _():
            p = z - step
            self.up(p).wait_recv()

            @pl.when(z < 3)
            def _():
                self.up(p).start()

            then(p)

        @pl.when(z + step <= 3)
        def _():
            p = z + step
            self.down(p).wait_recv()

            @pl.when(z > 0)
            def _():
                self.down(p).start()

            then(p)

    def drain(self):
        z = self.m.z
        for p in range(4):
            @pl.when((p <= z) & (z < 3))
            def _():
                self.up(p).wait_send()

            @pl.when((p >= z) & (z > 0))
            def _():
                self.down(p).wait_send()


def at_step(z, step, then):
    if step == 0:
        then(z)
        return

    @pl.when(z >= step)
    def _():
        then(z - step)

    @pl.when(z + step <= 3)
    def _():
        then(z + step)


def layer_kernel(
    tokens, gain, wa, wg, taps, conv_gain, wq, wk, wv, wog, wd, bias, extra_in, head_gain, init, woc, wogl, out,
    w1, w2, w3, wo, both, normed, acc1, acc2, acc3, extra, seq, attn, since, act, psend, pown, precv, outv,
    halo_out, halo_in, stat_own, stat_in, packs, state, prefix, before,
    local, first_send, first_recv, last_send, last_recv, up_send, down_send, z_recv, misc_send, misc_recv, end_send, end_recv,
    part_send, part_recv, out_sem,
):
    m = Mover()
    me, tp, z, y, x = m.me, m.tp, m.z, m.y, m.x
    rows = normed.shape[0]
    half = rows // 2
    width = both.shape[2]
    n_key = acc1.shape[1] // 5
    n_conv = 2 * n_key
    heads = n_key // HK
    sems = dict(
        first_send=first_send, first_recv=first_recv, last_send=last_send, last_recv=last_recv,
        up_send=up_send, down_send=down_send, z_recv=z_recv,
    )

    def lanes(ref, low, size):
        return lambda p, yy, xx: ref.at[p, yy, xx, :, pl.ds(low, size)]

    def depth(low, size):
        return lambda p, yy, xx: wo.at[p, yy, xx, pl.ds(low, size), :]

    mid = w1.shape[-1] // 2
    b1 = Flow(m, 0, lanes(w1, 0, mid), "x", sems)
    b2 = Flow(m, 1, lanes(w1, mid, mid), "y", sems)
    pairs = [
        (Flow(m, 2, lanes(w2, 0, n_conv), "x", sems), Flow(m, 3, lanes(w2, n_conv, n_conv), "y", sems)),
        (Flow(m, 4, lanes(w3, 0, n_key), "x", sems), Flow(m, 5, lanes(w3, n_key, n_key), "y", sems)),
        (Flow(m, 6, depth(0, n_conv), "x", sems), Flow(m, 7, depth(n_conv, n_conv), "y", sems)),
    ]
    whole = Line(m, 0, lambda p: w1.at[p, y, x], sems)
    lines = [tuple(Line(m, f.number - 1, f.pair, sems) for f in pair) for pair in pairs]

    loads = [
        (wq, w1.at[z, y, x, :, pl.ds(0, n_key)]),
        (wk, w1.at[z, y, x, :, pl.ds(n_key, n_key)]),
        (wd, w1.at[z, y, x, :, pl.ds(2 * n_key, n_key)]),
        (wv, w1.at[z, y, x, :, pl.ds(3 * n_key, n_conv)]),
        (wa, w2.at[z, y, x, :, pl.ds(0, n_conv)]),
        (wg, w2.at[z, y, x, :, pl.ds(n_conv, n_conv)]),
        (wog, w3.at[z, y, x]),
        (woc, wo.at[z, y, x, pl.ds(0, n_conv), :]),
        (wogl, wo.at[z, y, x, pl.ds(n_conv, n_conv), :]),
        (tokens, both.at[tp]),
        (extra_in, extra),
    ]
    loads = [pltpu.make_async_copy(a, b, local.at[i]) for i, (a, b) in enumerate(loads)]
    for load in loads:
        load.start()

    barrier = pltpu.get_barrier_semaphore()
    partners = [(m.other["x"], tp), (m.other["y"], tp), (me, 1 - tp)]
    partners += [((me + k) % 16, tp) for k in (4, 8, 12, 1, 15)]
    for place, core in partners:
        pl.semaphore_signal(barrier, inc=1, device_id=(place, core), device_id_type=MESH)
    pl.semaphore_wait(barrier, len(partners))

    for i in range(4):
        loads[i].wait()
    whole.start_own()
    b1.first_copy(z).start()
    b2.first_copy(z).start()
    loads[9].wait()
    swap = m.copy(both.at[tp], both.at[tp], misc_send.at[0], misc_recv.at[0], me, 1 - tp)
    swap.start()
    loads[4].wait()
    loads[5].wait()
    for f in pairs[0]:
        f.first_copy(z).start()
    for i in (6, 7, 8):
        loads[i].wait()
    for pair in pairs[1:]:
        for f in pair:
            f.first_copy(z).start()
    loads[10].wait()

    def head_firsts(step):
        def one(p):
            b1.first_copy(p).wait_recv()
            b1.last_copy(p).start()
            b2.first_copy(p).wait_recv()
            b2.last_copy(p).start()

        at_step(z, step, one)

    def head_line(step):
        def then(p):
            b1.first_copy(p).start()
            b2.first_copy(p).start()

        whole.relay(step, then)

    def enter(k):
        for f, line in zip(pairs[k], lines[k]):
            f.first_copy(z).wait_recv()
            line.start_own()
            f.last_copy(z).start()

    def pass_on(k, step):
        for f, line in zip(pairs[k], lines[k]):
            line.relay(step, lambda p: f.last_copy(p).start())

    def arrived(flows, p):
        for f in flows:
            f.last_copy(p).wait_recv()

    def norm_tiles(low, high):
        def body(i, carry):
            at = pl.ds(pl.multiple_of(i * 128, 128), 128)
            a = both[0, at, :].astype(jnp.float32)
            b = both[1, at, :].astype(jnp.float32)
            square = jnp.sum(a * a + b * b, axis=1, keepdims=True)
            scale = lax.rsqrt(square / (2 * width) + epsilon)
            normed[at, :width] = (a * scale * gain[:, :width]).astype(jnp.bfloat16)
            normed[at, width:] = (b * scale * gain[:, width:]).astype(jnp.bfloat16)
            return carry

        lax.fori_loop(low, high, body, 0)

    def slab(acc, ref, p, first):
        size = ref.shape[1] * ref.shape[2] * ref.shape[3]

        def body(c, carry):
            at = pl.ds(pl.multiple_of(c * 256, 256), 256)
            left = normed[:, pl.ds(pl.multiple_of(p * size, size), size)]
            right = ref[p, :, :, :, at].reshape(size, 256)
            got = dot(left, right, ((1,), (0,)))
            if first:
                acc[:, at] = got
            else:
                acc[:, at] += got
            return carry

        lax.fori_loop(0, acc.shape[1] // 256, body, 0)

    swap.wait_recv()
    norm_tiles(0, 4)
    head_line(1)
    head_firsts(0)
    norm_tiles(4, 8)
    head_line(2)
    enter(0)
    head_firsts(1)
    head_line(3)
    head_firsts(2)
    arrived((b1, b2), m.piece(0))
    slab(acc1, w1, m.piece(0), True)
    head_firsts(3)
    arrived((b1, b2), m.piece(1))
    slab(acc1, w1, m.piece(1), False)
    pass_on(0, 1)
    arrived((b1, b2), m.piece(2))
    slab(acc1, w1, m.piece(2), False)
    pass_on(0, 2)
    enter(1)
    arrived((b1, b2), m.piece(3))
    slab(acc1, w1, m.piece(3), False)

    state[...] = jnp.zeros_like(state)
    prefix[...] = jnp.zeros_like(prefix)
    r_iota = lax.broadcasted_iota(jnp.int32, (BLOCK, BLOCK), 0)
    c_iota = lax.broadcasted_iota(jnp.int32, (BLOCK, BLOCK), 1)
    causal = r_iota >= c_iota
    lower = causal.astype(jnp.float32)

    def block(i, carry):
        at = pl.ds(pl.multiple_of(i * BLOCK, BLOCK), BLOCK)
        pre = acc1[at, 2 * n_key : 3 * n_key] + bias[...]
        logs = jax.nn.log_sigmoid(pre) / gate_divisor + extra[at, :]
        cum = lax.dot_general(
            lower, logs, (((1,), (0,)), ((), ())), precision=lax.Precision.HIGHEST, preferred_element_type=jnp.float32
        )
        total = cum[BLOCK - 1 :, :]
        middle = cum[BLOCK // 2 - 1 : BLOCK // 2, :]
        query = acc1[at, 0:n_key].astype(jnp.bfloat16).astype(jnp.float32) * HK ** (-0.5)
        keys = acc1[at, n_key : 2 * n_key].astype(jnp.bfloat16).astype(jnp.float32)
        decayed = query * jnp.exp(cum)
        since[at, :] = (decayed * jnp.exp(prefix[...])).astype(jnp.bfloat16)
        decayed = decayed.astype(jnp.bfloat16)
        query = (query * jnp.exp(cum - middle)).astype(jnp.bfloat16)
        inverse = (keys * jnp.exp(middle - cum)).astype(jnp.bfloat16)
        to_end = (keys * jnp.exp(total - cum)).astype(jnp.bfloat16)
        entering = state[...].astype(jnp.bfloat16)
        added = []
        for h in range(heads):
            ks, vs = slice(h * HK, (h + 1) * HK), slice(h * HV, (h + 1) * HV)
            values = acc1[at, 3 * n_key + h * HV : 3 * n_key + (h + 1) * HV].astype(jnp.bfloat16)
            scores = jnp.where(causal, dot(query[:, ks], inverse[:, ks], ((1,), (1,))), 0.0)
            attn[at, vs] = dot(scores.astype(jnp.bfloat16), values, ((1,), (0,))) + dot(
                decayed[:, ks], entering[:, ks], ((1,), (1,))
            )
            added.append(dot(values, to_end[:, ks], ((0,), (0,))))
        state[...] = state[...] * jnp.exp(total) + jnp.concatenate(added, axis=1)
        prefix[...] = prefix[...] + total
        return carry

    blocks = rows // BLOCK
    quarter = blocks // 4

    def attend(i, carry):
        block(i, 0)

        @pl.when(i == quarter)
        def _():
            pass_on(0, 3)

        @pl.when(i == 3 * quarter)
        def _():
            pass_on(1, 1)

        return carry

    lax.fori_loop(0, blocks, attend, 0)

    def pack(slot, decay, end):
        packs[slot, 0:HV, :] = end.astype(jnp.bfloat16)
        packs[slot, HV:, :] = jnp.broadcast_to(decay, (16, n_key)).astype(jnp.bfloat16)

    def read(slot):
        return packs[slot, HV : HV + 1, :].astype(jnp.float32), packs[slot, 0:HV, :].astype(jnp.float32)

    def end_copy(source, target, number, place):
        return m.copy(packs.at[source], packs.at[target], end_send.at[number], end_recv.at[target], place)

    def join(early, late):
        return early[0] * late[0], early[1] * late[0] + late[1]

    def choose(flag, a, b):
        return jnp.where(flag, a[0], b[0]), jnp.where(flag, a[1], b[1])

    end_x = end_copy(0, 3, 0, m.other["x"])
    end_y = end_copy(1, 4, 1, m.other["y"])
    own_end = (jnp.exp(prefix[...]), state[...])
    pack(0, *own_end)

    arrived(pairs[0], m.piece(0))
    slab(acc2, w2, m.piece(0), True)
    end_x.start()
    pass_on(1, 2)
    enter(2)
    arrived(pairs[0], m.piece(1))
    slab(acc2, w2, m.piece(1), False)

    end_x.wait_recv()
    got = read(3)
    own_end = (jnp.exp(prefix[...]), state[...])
    none = (jnp.ones_like(got[0]), jnp.zeros_like(got[1]))
    late = x == 1
    pre = choose(late, got, none)
    two = choose(late, join(got, own_end), join(own_end, got))
    before[0:HV, :] = pre[1]
    before[HV:, :] = jnp.broadcast_to(pre[0], (8, n_key))
    pack(1, *two)
    pass_on(1, 3)
    arrived(pairs[0], m.piece(2))
    slab(acc2, w2, m.piece(2), False)
    end_y.start()
    arrived(pairs[0], m.piece(3))
    slab(acc2, w2, m.piece(3), False)
    end_y.wait_recv()
    got = read(4)
    two = read(1)
    pre = (before[HV : HV + 1, :], before[0:HV, :])
    late = y == 1
    pre = choose(late, join(got, pre), pre)
    four = choose(late, join(got, two), join(two, got))
    before[0:HV, :] = pre[1]
    before[HV:, :] = jnp.broadcast_to(pre[0], (8, n_key))
    pack(2, *four)

    pad = seq.shape[1] - rows

    def gate_tiles(low, high):
        def body(i, carry):
            at = pl.ds(pl.multiple_of(i * 128, 128), 128)
            for c in range(n_conv // 128):
                a = acc2[at, c * 128 : (c + 1) * 128].astype(jnp.bfloat16).astype(jnp.float32)
                g = acc2[at, n_conv + c * 128 : n_conv + (c + 1) * 128].astype(jnp.bfloat16).astype(jnp.float32)
                value = (a * jax.nn.sigmoid(g)).astype(jnp.bfloat16)
                seq[c, pl.ds(pl.multiple_of(i * 128 + pad, 32), 128), :] = value.astype(jnp.float32)
            return carry

        lax.fori_loop(low, high, body, 0)

    gate_tiles(rows // 128 - 1, rows // 128)
    for c in range(n_conv // 128):
        halo_out[:, c * 128 : (c + 1) * 128] = seq[c, rows : rows + pad, :].astype(jnp.bfloat16)
    gate_tiles(0, rows // 128 - 1)
    halo = m.copy(halo_out, halo_in, misc_send.at[1], misc_recv.at[1], me + 1)

    @pl.when(me < 15)
    def _():
        halo.start()

    for k in (1, 2, 3):
        @pl.when(z + k <= 3)
        def _():
            end_copy(2, 4 + k, 1 + k, me + 4 * k).start()

    n_taps = taps.shape[0]
    shift = pad - (n_taps - 1)

    def conv_chunk(i):
        base = pl.multiple_of(i * 128, 128)
        sums = jnp.zeros((128, 128), jnp.float32)
        squares = jnp.zeros((128, 128), jnp.float32)
        for c in range(n_conv // 128):
            part = seq[c, pl.ds(base, 128 + pad), :]
            total = jnp.zeros((128, 128), jnp.float32)
            for turn in range(8):
                moved = part if turn == 0 else pltpu.roll(part, 128 + pad - turn, 0)
                for tap in range(n_taps):
                    if (shift + tap) % 8 == turn:
                        start = shift + tap - turn
                        total = total + taps[tap : tap + 1, c * 128 : (c + 1) * 128] * moved[start : start + 128]
            acc2[pl.ds(base, 128), c * 128 : (c + 1) * 128] = total
            sums = sums + total
            squares = squares + total * total
        first = jnp.sum(sums, axis=1, keepdims=True)
        second = jnp.sum(squares, axis=1, keepdims=True)
        lane = lax.broadcasted_iota(jnp.int32, (128, 128), 1)
        stat_own[pl.ds(base, 128), :] = jnp.where(lane == 0, first, second)

    chunks = rows // 128

    def conv_loop(i, carry):
        conv_chunk(i)

        @pl.when(i == chunks // 2)
        def _():
            pass_on(2, 1)

        return carry

    lax.fori_loop(1, chunks, conv_loop, 0)

    @pl.when(me > 0)
    def _():
        halo.wait_recv()
        for c in range(n_conv // 128):
            seq[c, 0:pad, :] = halo_in[:, c * 128 : (c + 1) * 128].astype(jnp.float32)

    @pl.when(me == 0)
    def _():
        seq[:, 0:pad, :] = jnp.zeros((n_conv // 128, pad, 128), jnp.float32)

    lax.fori_loop(0, 1, conv_loop, 0)

    arrived(pairs[1], m.piece(0))
    slab(acc3, w3, m.piece(0), True)
    stats = m.copy(stat_own, stat_in, misc_send.at[2], misc_recv.at[2], me, 1 - tp)
    stats.start()
    arrived(pairs[1], m.piece(1))
    slab(acc3, w3, m.piece(1), False)
    pass_on(2, 2)
    arrived(pairs[1], m.piece(2))
    slab(acc3, w3, m.piece(2), False)
    arrived(pairs[1], m.piece(3))
    slab(acc3, w3, m.piece(3), False)

    stats.wait_recv()

    def conv_finish(i, carry):
        at = pl.ds(pl.multiple_of(i * 128, 128), 128)
        both_stats = stat_own[at, :] + stat_in[at, :]
        mean_val = both_stats[:, 0:1] / (2 * n_conv)
        square_mean = both_stats[:, 1:2] / (2 * n_conv)
        scale = lax.rsqrt(square_mean - mean_val * mean_val + epsilon)
        value = (acc2[at, 0:n_conv] - mean_val) * scale * conv_gain[...]
        act[at, 0:n_conv] = (value * jax.nn.sigmoid(value)).astype(jnp.bfloat16)
        return carry

    lax.fori_loop(0, chunks, conv_finish, 0)

    for k in (1, 2, 3):
        @pl.when(z - k >= 0)
        def _():
            end_copy(2, 4 + k, 1 + k, me).wait_recv()
            pre = join(read(4 + k), (before[HV : HV + 1, :], before[0:HV, :]))
            before[0:HV, :] = pre[1]
            before[HV:, :] = jnp.broadcast_to(pre[0], (8, n_key))

    state[...] = init[...] * before[HV : HV + 1, :] + before[0:HV, :]

    def gla_finish(i, carry):
        at = pl.ds(pl.multiple_of(i * 256, 256), 256)
        entering = state[...].astype(jnp.bfloat16)
        for h in range(heads):
            ks, vs = slice(h * HK, (h + 1) * HK), slice(h * HV, (h + 1) * HV)
            value = attn[at, vs] + dot(since[at, ks], entering[:, ks], ((1,), (1,)))
            value = value * lax.rsqrt(jnp.mean(value * value, axis=-1, keepdims=True) + epsilon) * head_gain[...]
            gate = acc3[at, vs].astype(jnp.bfloat16).astype(jnp.float32)
            act[at, n_conv + h * HV : n_conv + (h + 1) * HV] = (value * (gate * jax.nn.sigmoid(gate))).astype(jnp.bfloat16)
        return carry

    lax.fori_loop(0, rows // 256, gla_finish, 0)

    def part_copy(b):
        return m.copy(psend.at[b], precv.at[b], part_send.at[b], part_recv.at[b], me, 1 - tp)

    def out_block(p, yy):
        b = p * 2 + yy
        weight = jnp.concatenate([wo[p, yy, 0], wo[p, yy, 1]], axis=1)
        left = act[pl.ds(pl.multiple_of((1 - tp) * half, half), half), :]
        psend[b] = dot(left, weight, ((1,), (0,))).astype(jnp.bfloat16)
        left = act[pl.ds(pl.multiple_of(tp * half, half), half), :]
        pown[b] = dot(left, weight, ((1,), (0,))).astype(jnp.bfloat16)
        part_copy(b).start()

    def out_copy(b):
        return pltpu.make_async_copy(outv.at[b], out.at[:, pl.ds(pl.multiple_of(b * 256, 256), 256)], out_sem.at[b])

    def merge(p, yy):
        b = p * 2 + yy
        part_copy(b).wait_recv()
        outv[b] = (pown[b].astype(jnp.float32) + precv[b].astype(jnp.float32)).astype(jnp.bfloat16)
        out_copy(b).start()

    def out_pieces(j):
        def body(yy, carry):
            out_block(m.piece(j), yy)
            return carry

        arrived(pairs[2], m.piece(j))
        lax.fori_loop(0, 2, body, 0)

    def merges(j):
        def body(yy, carry):
            merge(m.piece(j), yy)
            return carry

        lax.fori_loop(0, 2, body, 0)

    out_pieces(0)
    out_pieces(1)
    merges(0)
    pass_on(2, 3)
    out_pieces(2)
    merges(1)
    out_pieces(3)
    merges(2)
    merges(3)

    swap.wait_send()
    stats.wait_send()

    @pl.when(me < 15)
    def _():
        halo.wait_send()

    end_x.wait_send()
    end_y.wait_send()
    for k in (1, 2, 3):
        @pl.when(z + k <= 3)
        def _():
            end_copy(2, 4 + k, 1 + k, me + 4 * k).wait_send()

    for p in range(4):
        for f in (b1, b2):
            f.first_copy(p).wait_send()
            f.last_copy(p).wait_send()
        for pair in pairs:
            for f in pair:
                f.last_copy(p).wait_send()
    for pair in pairs:
        for f in pair:
            f.first_copy(z).wait_send()
    whole.drain()
    for pair in lines:
        for line in pair:
            line.drain()
    for b in range(8):
        part_copy(b).wait_send()
        out_copy(b).wait()


def fused_layer(
    tokens, norm_gain, w_conv_a, w_conv_gate, conv_weight, conv_gain, w_query, w_key, w_value, w_outgate,
    w_decay, decay_bias, decay_extra, head_gain, init_state, w_out_conv, w_out_gla,
):
    rows, width = tokens.shape
    depth = w_query.shape[0]
    n_key = w_query.shape[1]
    n_conv = w_conv_a.shape[1]
    cols = w_out_conv.shape[1]
    init = init_state.transpose(2, 0, 1).reshape(HV, n_key)
    half = rows // 2
    pad = 32
    bf16, f32 = jnp.bfloat16, jnp.float32
    dma = pltpu.SemaphoreType.DMA
    vm = pl.BlockSpec(memory_space=pltpu.VMEM)
    hbm = pl.BlockSpec(memory_space=pl.ANY)
    return pl.pallas_call(
        layer_kernel,
        out_shape=jax.ShapeDtypeStruct((half, 2 * width), bf16),
        in_specs=[hbm, vm, hbm, hbm, vm, vm, hbm, hbm, hbm, hbm, hbm, vm, hbm, vm, vm, hbm, hbm],
        out_specs=hbm,
        scratch_shapes=[
            pltpu.VMEM((4, 2, 2, depth, 5 * n_key), bf16),
            pltpu.VMEM((4, 2, 2, depth, 2 * n_conv), bf16),
            pltpu.VMEM((4, 2, 2, depth, n_conv), bf16),
            pltpu.VMEM((4, 2, 2, 2 * n_conv, cols), bf16),
            pltpu.VMEM((2, rows, width), bf16),
            pltpu.VMEM((rows, 2 * width), bf16),
            pltpu.VMEM((rows, 5 * n_key), f32),
            pltpu.VMEM((rows, 2 * n_conv), f32),
            pltpu.VMEM((rows, n_conv), f32),
            pltpu.VMEM((rows, n_key), f32),
            pltpu.VMEM((n_conv // 128, rows + pad, 128), f32),
            pltpu.VMEM((rows, n_conv), f32),
            pltpu.VMEM((rows, n_key), bf16),
            pltpu.VMEM((rows, 2 * n_conv), bf16),
            pltpu.VMEM((8, half, 256), bf16),
            pltpu.VMEM((8, half, 256), bf16),
            pltpu.VMEM((8, half, 256), bf16),
            pltpu.VMEM((8, half, 256), bf16),
            pltpu.VMEM((pad, n_conv), bf16),
            pltpu.VMEM((pad, n_conv), bf16),
            pltpu.VMEM((rows, 128), f32),
            pltpu.VMEM((rows, 128), f32),
            pltpu.VMEM((8, HV + 16, n_key), bf16),
            pltpu.VMEM((HV, n_key), f32),
            pltpu.VMEM((1, n_key), f32),
            pltpu.VMEM((HV + 8, n_key), f32),
            dma((11,)), dma((8, 4)), dma((8, 4)), dma((8, 4)), dma((8, 4)), dma((7, 4)), dma((7, 4)), dma((7, 4)),
            dma((3,)), dma((3,)), dma((5,)), dma((8,)), dma((8,)), dma((8,)), dma((8,)),
        ],
        compiler_params=pltpu.CompilerParams(collective_id=0, has_side_effects=True, vmem_limit_bytes=67043328),
        name="layer",
    )(
        tokens, norm_gain[None, :], w_conv_a, w_conv_gate, conv_weight, conv_gain[None, :], w_query, w_key, w_value,
        w_outgate, w_decay, decay_bias[None, :], decay_extra, head_gain[None, :], init, w_out_conv, w_out_gla,
    )


def local_kernel(heads, pieces, q_ref, k_ref, v_ref, pre_ref, extra_ref, bias_ref, attn_ref, since_ref, end_ref, log_ref, state, prefix):
    step = pl.program_id(0)

    @pl.when(step == 0)
    def _():
        state[...] = jnp.zeros_like(state)
        prefix[...] = jnp.zeros_like(prefix)

    rows = lax.broadcasted_iota(jnp.int32, (BLOCK, BLOCK), 0)
    columns = lax.broadcasted_iota(jnp.int32, (BLOCK, BLOCK), 1)
    causal = rows >= columns
    lower = causal.astype(jnp.float32)
    for piece in range(pieces):
        at = pl.ds(piece * BLOCK, BLOCK)
        pre = pre_ref[at, :] + bias_ref[...]
        logs = jax.nn.log_sigmoid(pre) / gate_divisor + extra_ref[at, :]
        cum = lax.dot_general(
            lower, logs, (((1,), (0,)), ((), ())), precision=lax.Precision.HIGHEST, preferred_element_type=jnp.float32
        )
        total = cum[BLOCK - 1 :, :]
        middle = cum[BLOCK // 2 - 1 : BLOCK // 2, :]
        query = q_ref[at, :].astype(jnp.float32) * HK ** (-0.5)
        keys = k_ref[at, :].astype(jnp.float32)
        decayed = query * jnp.exp(cum)
        since_ref[at, :] = (decayed * jnp.exp(prefix[...])).astype(jnp.bfloat16)
        decayed = decayed.astype(jnp.bfloat16)
        query = (query * jnp.exp(cum - middle)).astype(jnp.bfloat16)
        inverse = (keys * jnp.exp(middle - cum)).astype(jnp.bfloat16)
        to_end = (keys * jnp.exp(total - cum)).astype(jnp.bfloat16)
        entering = state[...].astype(jnp.bfloat16)
        added = []
        for h in range(heads):
            ks, vs = slice(h * HK, (h + 1) * HK), slice(h * HV, (h + 1) * HV)
            values = v_ref[at, vs]
            scores = jnp.where(causal, dot(query[:, ks], inverse[:, ks], ((1,), (1,))), 0.0)
            attn_ref[at, vs] = dot(scores.astype(jnp.bfloat16), values, ((1,), (0,))) + dot(
                decayed[:, ks], entering[:, ks], ((1,), (1,))
            )
            added.append(dot(values, to_end[:, ks], ((0,), (0,))))
        added = added[0] if heads == 1 else jnp.concatenate(added, axis=1)
        state[...] = state[...] * jnp.exp(total) + added
        prefix[...] = prefix[...] + total
    end_ref[...] = state[...]
    log_ref[...] = prefix[...]


def gla_local(query, keys, values, decay_pre, decay_extra, decay_bias):
    rows, width = query.shape
    heads = width // HK
    pieces = 4
    tile = pieces * BLOCK

    def tiled(array):
        return pl.BlockSpec((tile, array.shape[1]), lambda i: (i, 0))

    def whole(shape):
        return pl.BlockSpec(shape, lambda i: (0, 0))

    return pl.pallas_call(
        functools.partial(local_kernel, heads, pieces),
        grid=(rows // tile,),
        in_specs=[tiled(query), tiled(keys), tiled(values), tiled(decay_pre), tiled(decay_extra), whole((1, width))],
        out_specs=[tiled(values), tiled(query), whole((HV, width)), whole((1, width))],
        out_shape=[
            jax.ShapeDtypeStruct(values.shape, jnp.float32),
            jax.ShapeDtypeStruct(query.shape, jnp.bfloat16),
            jax.ShapeDtypeStruct((HV, width), jnp.float32),
            jax.ShapeDtypeStruct((1, width), jnp.float32),
        ],
        scratch_shapes=[pltpu.VMEM((HV, width), jnp.float32), pltpu.VMEM((1, width), jnp.float32)],
        cost_estimate=pl.CostEstimate(flops=10**10, bytes_accessed=10**7, transcendentals=10**6),
        name="gla_local",
    )(query, keys, values, decay_pre, decay_extra, decay_bias[None, :])


def finish_kernel(heads, size, where_ref, attn_ref, since_ref, gate_ref, ends_ref, init_ref, gain_ref, out_ref, state):
    me = where_ref[0]

    @pl.when(pl.program_id(0) == 0)
    def _():
        state[...] = init_ref[...]

        def one(device, carry):
            at = device
            decay = ends_ref[pl.ds(pl.multiple_of(at * size + HV, 16), 16), :].astype(jnp.float32)[:1]
            end = ends_ref[pl.ds(pl.multiple_of(at * size, 16), HV), :].astype(jnp.float32)
            state[...] = state[...] * decay + end
            return carry

        lax.fori_loop(0, me, one, 0)

    entering = state[...].astype(jnp.bfloat16)
    for h in range(heads):
        ks, vs = slice(h * HK, (h + 1) * HK), slice(h * HV, (h + 1) * HV)
        attn = attn_ref[:, vs] + dot(since_ref[:, ks], entering[:, ks], ((1,), (1,)))
        attn = attn * lax.rsqrt(jnp.mean(attn * attn, axis=-1, keepdims=True) + epsilon) * gain_ref[...]
        gate = gate_ref[:, vs].astype(jnp.float32)
        out_ref[:, vs] = (attn * (gate * jax.nn.sigmoid(gate))).astype(jnp.bfloat16)


def gla_finish(attn, since, out_gate, ends, init_state, head_gain, me):
    rows, width = since.shape
    heads = width // HK
    tile = 256

    def tiled(array):
        return pl.BlockSpec((tile, array.shape[1]), lambda i, w: (i, 0))

    def whole(array):
        return pl.BlockSpec(array.shape, lambda i, w: (0, 0))

    init = init_state.transpose(2, 0, 1).reshape(HV, width)
    gain = head_gain[None, :]
    return pl.pallas_call(
        functools.partial(finish_kernel, heads, HV + 16),
        grid_spec=pltpu.PrefetchScalarGridSpec(
            num_scalar_prefetch=1,
            grid=(rows // tile,),
            in_specs=[tiled(attn), tiled(since), tiled(out_gate), whole(ends), whole(init), whole(gain)],
            out_specs=tiled(attn),
            scratch_shapes=[pltpu.VMEM((HV, width), jnp.float32)],
        ),
        out_shape=jax.ShapeDtypeStruct(attn.shape, jnp.bfloat16),
        cost_estimate=pl.CostEstimate(flops=3 * 10**9, bytes_accessed=10**7, transcendentals=10**6),
        name="gla_finish",
    )(me[None], attn, since, out_gate, ends, init, gain)


def conv_branch(gated, conv_weight, conv_gain):
    taps = conv_weight.shape[0]
    row_count = gated.shape[0]
    count = lax.axis_size("sp")
    earlier = lax.ppermute(gated[row_count - taps + 1 :], "sp", [(i, i + 1) for i in range(count - 1)])
    extended = jnp.concatenate([earlier, gated], axis=0).astype(jnp.float32)
    conv_sum = jnp.zeros(gated.shape, jnp.float32)
    for tap in range(taps):
        conv_sum = conv_sum + conv_weight[tap][None, :] * extended[tap : tap + row_count]
    row_sums, row_squares = lax.psum((jnp.sum(conv_sum, axis=1), jnp.sum(conv_sum * conv_sum, axis=1)), "tp")
    mean_val = (row_sums / D_CONV)[:, None]
    square_mean = (row_squares / D_CONV)[:, None]
    conv_norm = (conv_sum - mean_val) * lax.rsqrt(square_mean - mean_val * mean_val + epsilon) * conv_gain
    return jax.nn.silu(conv_norm).astype(jnp.bfloat16)


def project(hidden, weight):
    return dot(hidden, weight, ((1,), (0,)))


def plain_layer(
    tokens, norm_gain, w_conv_a, w_conv_gate, conv_weight, conv_gain, w_query, w_key, w_value, w_outgate,
    w_decay, decay_bias, decay_extra, head_gain, init_state, w_out_conv, w_out_gla,
):
    me = lax.axis_index("sp")

    def gather(shard):
        return lax.all_gather(shard, "sp", axis=0, tiled=True)

    widened = lax.all_gather(tokens, "tp", axis=1, tiled=True).astype(jnp.float32)
    normed = (
        widened * lax.rsqrt(jnp.mean(widened * widened, axis=-1, keepdims=True) + epsilon) * norm_gain
    ).astype(jnp.bfloat16)
    half = w_query.shape[1]
    conv_a = project(normed, gather(w_conv_a)).astype(jnp.bfloat16)
    conv_gate = project(normed, gather(w_conv_gate)).astype(jnp.bfloat16)
    full_qkd = gather(jnp.concatenate([w_query, w_key, w_decay], axis=1))
    full_v = gather(w_value)
    gated = (conv_a.astype(jnp.float32) * jax.nn.sigmoid(conv_gate.astype(jnp.float32))).astype(jnp.bfloat16)
    conv_out = conv_branch(gated, conv_weight, conv_gain)
    query_keys = project(normed, full_qkd[:, : 2 * half]).astype(jnp.bfloat16)
    decay_pre = project(normed, full_qkd[:, 2 * half :])
    values = project(normed, full_v).astype(jnp.bfloat16)
    attn, since, end, end_log = gla_local(
        query_keys[:, :half], query_keys[:, half:], values, decay_pre, decay_extra, decay_bias
    )
    packed = jnp.concatenate([end, jnp.broadcast_to(jnp.exp(end_log), (16, half))], axis=0).astype(jnp.bfloat16)
    ends = gather(packed)
    out_gate = project(normed, gather(w_outgate)).astype(jnp.bfloat16)
    gla_out = gla_finish(attn, since, out_gate, ends, init_state, head_gain, me)
    total = dot(conv_out, gather(w_out_conv.T), ((1,), (1,))) + dot(gla_out, gather(w_out_gla.T), ((1,), (1,)))
    return lax.psum_scatter(total.astype(jnp.bfloat16), "tp", scatter_dimension=0, tiled=True)


def per_device(*arrays):
    if folded(lax.axis_size("sp"), lax.axis_size("tp")):
        return fused_layer(*arrays)
    return plain_layer(*arrays)


def solution(mesh):
    placed = (
        P("sp", "tp"), P(), P("sp", "tp"), P("sp", "tp"), P(None, "tp"), P("tp"), P("sp", "tp"), P("sp", "tp"),
        P("sp", "tp"), P("sp", "tp"), P("sp", "tp"), P("tp"), P("sp", "tp"), P(), P("tp", None, None),
        P("tp", "sp"), P("tp", "sp"),
    )
    return jax.shard_map(
        per_device, mesh=mesh, in_specs=placed, out_specs=P(("sp", "tp"), None), check_vma=False
    )
```

```python
import functools

import jax
import jax.numpy as jnp
from jax import lax
from jax.experimental import pallas as pl
from jax.experimental.pallas import tpu as pltpu
from jax.sharding import PartitionSpec as P

D_CONV = 1024
HK = 64
HV = 128
BLOCK = 64

epsilon = 1e-06
gate_divisor = 16.0

MESH = pl.DeviceIdType.MESH


def dot(a, b, dims):
    return lax.dot_general(a, b, (dims, ((), ())), preferred_element_type=jnp.float32)


def folded(n_sp, n_tp):
    return n_sp == 16 and n_tp == 2


class Mover:
    def __init__(self):
        self.me = lax.axis_index("sp")
        self.tp = lax.axis_index("tp")
        self.z, self.y, self.x = self.me // 4, (self.me // 2) % 2, self.me % 2
        self.other = {"x": self.me + 1 - 2 * self.x, "y": self.me + 2 - 4 * self.y}
        self.sent = []

    def copy(self, source, target, send, recv, place, core=None):
        core = self.tp if core is None else core
        return pltpu.make_async_remote_copy(
            src_ref=source, dst_ref=target, send_sem=send, recv_sem=recv, device_id=(place, core), device_id_type=MESH
        )

    def piece(self, j):
        z = self.z
        return (z, z + 1 - 2 * (z % 2), 2 - z // 2, 3 - 3 * (z // 2))[j]


class Flow:
    def __init__(self, mover, number, view, first, sems):
        self.m, self.number, self.view, self.first = mover, number, view, first
        self.last = {"x": "y", "y": "x"}[first]
        self.sems = sems

    def own(self, p):
        return self.view(p, self.m.y, self.m.x)

    def pair(self, p):
        every = slice(None)
        return self.view(p, self.m.y, every) if self.first == "x" else self.view(p, every, self.m.x)

    def first_copy(self, p):
        own = self.own(p)
        fs, fr = self.sems["first_send"], self.sems["first_recv"]
        return self.m.copy(own, own, fs.at[self.number, p], fr.at[self.number, p], self.m.other[self.first])

    def last_copy(self, p):
        pair = self.pair(p)
        ls, lr = self.sems["last_send"], self.sems["last_recv"]
        return self.m.copy(pair, pair, ls.at[self.number, p], lr.at[self.number, p], self.m.other[self.last])


class Line:
    def __init__(self, mover, number, view, sems):
        self.m, self.number, self.view, self.sems = mover, number, view, sems

    def up(self, p):
        return self.m.copy(
            self.view(p), self.view(p), self.sems["up_send"].at[self.number, p], self.sems["z_recv"].at[self.number, p],
            self.m.me + 4,
        )

    def down(self, p):
        return self.m.copy(
            self.view(p), self.view(p), self.sems["down_send"].at[self.number, p],
            self.sems["z_recv"].at[self.number, p], self.m.me - 4,
        )

    def start_own(self):
        z = self.m.z

        @pl.when(z < 3)
        def _():
            self.up(z).start()

        @pl.when(z > 0)
        def _():
            self.down(z).start()

    def relay(self, step, then):
        z = self.m.z

        @pl.when(z >= step)
        def _():
            p = z - step
            self.up(p).wait_recv()

            @pl.when(z < 3)
            def _():
                self.up(p).start()

            then(p)

        @pl.when(z + step <= 3)
        def _():
            p = z + step
            self.down(p).wait_recv()

            @pl.when(z > 0)
            def _():
                self.down(p).start()

            then(p)

    def drain(self):
        z = self.m.z
        for p in range(4):
            @pl.when((p <= z) & (z < 3))
            def _():
                self.up(p).wait_send()

            @pl.when((p >= z) & (z > 0))
            def _():
                self.down(p).wait_send()


def at_step(z, step, then):
    if step == 0:
        then(z)
        return

    @pl.when(z >= step)
    def _():
        then(z - step)

    @pl.when(z + step <= 3)
    def _():
        then(z + step)


def layer_kernel(
    tokens, gain, wa, wg, taps, conv_gain, wq, wk, wv, wog, wd, bias, extra_in, head_gain, init, woc, wogl, out,
    w1, w2, w3, wo, both, normed, acc1, acc2, acc3, extra, seq, attn, since, act, psend, pown, precv, outv,
    halo_out, halo_in, stat_own, stat_in, packs, state, prefix, before,
    local, first_send, first_recv, last_send, last_recv, up_send, down_send, z_recv, misc_send, misc_recv, end_send, end_recv,
    part_send, part_recv, out_sem,
):
    m = Mover()
    me, tp, z, y, x = m.me, m.tp, m.z, m.y, m.x
    rows = normed.shape[0]
    half = rows // 2
    width = both.shape[2]
    n_key = acc1.shape[1] // 5
    n_conv = 2 * n_key
    heads = n_key // HK
    sems = dict(
        first_send=first_send, first_recv=first_recv, last_send=last_send, last_recv=last_recv,
        up_send=up_send, down_send=down_send, z_recv=z_recv,
    )

    def lanes(ref, low, size):
        return lambda p, yy, xx: ref.at[p, yy, xx, :, pl.ds(low, size)]

    def depth(low, size):
        return lambda p, yy, xx: wo.at[p, yy, xx, pl.ds(low, size), :]

    mid = w1.shape[-1] // 2
    b1 = Flow(m, 0, lanes(w1, 0, mid), "x", sems)
    b2 = Flow(m, 1, lanes(w1, mid, mid), "y", sems)
    pairs = [
        (Flow(m, 2, lanes(w2, 0, n_conv), "x", sems), Flow(m, 3, lanes(w2, n_conv, n_conv), "y", sems)),
        (Flow(m, 4, lanes(w3, 0, n_key), "x", sems), Flow(m, 5, lanes(w3, n_key, n_key), "y", sems)),
        (Flow(m, 6, depth(0, n_key), "x", sems), Flow(m, 7, depth(n_key, n_key), "y", sems)),
        (Flow(m, 8, depth(n_conv, n_key), "x", sems), Flow(m, 9, depth(n_conv + n_key, n_key), "y", sems)),
    ]
    whole = Line(m, 0, lambda p: w1.at[p, y, x], sems)
    lines = [tuple(Line(m, f.number - 1, f.pair, sems) for f in pair) for pair in pairs]

    loads = [
        (wq, w1.at[z, y, x, :, pl.ds(0, n_key)]),
        (wk, w1.at[z, y, x, :, pl.ds(n_key, n_key)]),
        (wd, w1.at[z, y, x, :, pl.ds(2 * n_key, n_key)]),
        (wv, w1.at[z, y, x, :, pl.ds(3 * n_key, n_conv)]),
        (wa, w2.at[z, y, x, :, pl.ds(0, n_conv)]),
        (wg, w2.at[z, y, x, :, pl.ds(n_conv, n_conv)]),
        (wog, w3.at[z, y, x]),
        (woc, wo.at[z, y, x, pl.ds(0, n_conv), :]),
        (wogl, wo.at[z, y, x, pl.ds(n_conv, n_conv), :]),
        (tokens, both.at[tp]),
        (extra_in, extra),
    ]
    loads = [pltpu.make_async_copy(a, b, local.at[i]) for i, (a, b) in enumerate(loads)]
    for load in loads:
        load.start()

    barrier = pltpu.get_barrier_semaphore()
    partners = [(m.other["x"], tp), (m.other["y"], tp), (me, 1 - tp)]
    partners += [((me + k) % 16, tp) for k in (4, 8, 12, 1, 15)]
    for place, core in partners:
        pl.semaphore_signal(barrier, inc=1, device_id=(place, core), device_id_type=MESH)
    pl.semaphore_wait(barrier, len(partners))

    for i in range(4):
        loads[i].wait()
    whole.start_own()
    b1.first_copy(z).start()
    b2.first_copy(z).start()
    loads[9].wait()
    swap = m.copy(both.at[tp], both.at[tp], misc_send.at[0], misc_recv.at[0], me, 1 - tp)
    swap.start()
    loads[4].wait()
    loads[5].wait()
    for f in pairs[0]:
        f.first_copy(z).start()
    loads[6].wait()
    for f in pairs[1]:
        f.first_copy(z).start()
    for i in (7, 8, 10):
        loads[i].wait()

    def head_firsts(step):
        def one(p):
            b1.first_copy(p).wait_recv()
            b1.last_copy(p).start()
            b2.first_copy(p).wait_recv()
            b2.last_copy(p).start()

        at_step(z, step, one)

    def head_line(step):
        def then(p):
            b1.first_copy(p).start()
            b2.first_copy(p).start()

        whole.relay(step, then)

    def begin(k):
        for f in pairs[k]:
            f.first_copy(z).start()

    def enter(k):
        for f, line in zip(pairs[k], lines[k]):
            f.first_copy(z).wait_recv()
            line.start_own()

    def own_last(k):
        for f in pairs[k]:
            f.last_copy(z).start()

    def pass_on(k, step):
        for f, line in zip(pairs[k], lines[k]):
            line.relay(step, lambda p: f.last_copy(p).start())

    def arrived(flows, p):
        for f in flows:
            f.last_copy(p).wait_recv()

    def norm_tiles(low, high):
        def body(i, carry):
            at = pl.ds(pl.multiple_of(i * 128, 128), 128)
            a = both[0, at, :].astype(jnp.float32)
            b = both[1, at, :].astype(jnp.float32)
            square = jnp.sum(a * a + b * b, axis=1, keepdims=True)
            scale = lax.rsqrt(square / (2 * width) + epsilon)
            normed[at, :width] = (a * scale * gain[:, :width]).astype(jnp.bfloat16)
            normed[at, width:] = (b * scale * gain[:, width:]).astype(jnp.bfloat16)
            return carry

        lax.fori_loop(low, high, body, 0)

    def slab(acc, ref, p, first):
        size = ref.shape[1] * ref.shape[2] * ref.shape[3]

        def body(c, carry):
            at = pl.ds(pl.multiple_of(c * 256, 256), 256)
            left = normed[:, pl.ds(pl.multiple_of(p * size, size), size)]
            right = ref[p, :, :, :, at].reshape(size, 256)
            got = dot(left, right, ((1,), (0,)))
            if first:
                acc[:, at] = got
            else:
                acc[:, at] += got
            return carry

        lax.fori_loop(0, acc.shape[1] // 256, body, 0)

    swap.wait_recv()
    norm_tiles(0, 4)
    head_line(1)
    head_firsts(0)
    norm_tiles(4, 8)
    head_line(2)
    enter(0)
    head_firsts(1)
    head_line(3)
    arrived((b1, b2), m.piece(0))
    slab(acc1, w1, m.piece(0), True)
    head_firsts(2)
    begin(2)
    begin(3)
    pass_on(0, 1)
    arrived((b1, b2), m.piece(1))
    slab(acc1, w1, m.piece(1), False)
    head_firsts(3)
    enter(1)
    own_last(0)
    pass_on(0, 2)
    arrived((b1, b2), m.piece(2))
    slab(acc1, w1, m.piece(2), False)
    pass_on(1, 1)
    enter(2)
    arrived((b1, b2), m.piece(3))
    slab(acc1, w1, m.piece(3), False)

    state[...] = jnp.zeros_like(state)
    prefix[...] = jnp.zeros_like(prefix)
    r_iota = lax.broadcasted_iota(jnp.int32, (BLOCK, BLOCK), 0)
    c_iota = lax.broadcasted_iota(jnp.int32, (BLOCK, BLOCK), 1)
    causal = r_iota >= c_iota
    lower = causal.astype(jnp.float32)

    def block(i, carry):
        at = pl.ds(pl.multiple_of(i * BLOCK, BLOCK), BLOCK)
        pre = acc1[at, 2 * n_key : 3 * n_key] + bias[...]
        logs = jax.nn.log_sigmoid(pre) / gate_divisor + extra[at, :]
        cum = lax.dot_general(
            lower, logs, (((1,), (0,)), ((), ())), precision=lax.Precision.HIGHEST, preferred_element_type=jnp.float32
        )
        total = cum[BLOCK - 1 :, :]
        middle = cum[BLOCK // 2 - 1 : BLOCK // 2, :]
        query = acc1[at, 0:n_key].astype(jnp.bfloat16).astype(jnp.float32) * HK ** (-0.5)
        keys = acc1[at, n_key : 2 * n_key].astype(jnp.bfloat16).astype(jnp.float32)
        decayed = query * jnp.exp(cum)
        since[at, :] = (decayed * jnp.exp(prefix[...])).astype(jnp.bfloat16)
        decayed = decayed.astype(jnp.bfloat16)
        query = (query * jnp.exp(cum - middle)).astype(jnp.bfloat16)
        inverse = (keys * jnp.exp(middle - cum)).astype(jnp.bfloat16)
        to_end = (keys * jnp.exp(total - cum)).astype(jnp.bfloat16)
        entering = state[...].astype(jnp.bfloat16)
        added = []
        for h in range(heads):
            ks, vs = slice(h * HK, (h + 1) * HK), slice(h * HV, (h + 1) * HV)
            values = acc1[at, 3 * n_key + h * HV : 3 * n_key + (h + 1) * HV].astype(jnp.bfloat16)
            scores = jnp.where(causal, dot(query[:, ks], inverse[:, ks], ((1,), (1,))), 0.0)
            attn[at, vs] = dot(scores.astype(jnp.bfloat16), values, ((1,), (0,))) + dot(
                decayed[:, ks], entering[:, ks], ((1,), (1,))
            )
            added.append(dot(values, to_end[:, ks], ((0,), (0,))))
        state[...] = state[...] * jnp.exp(total) + jnp.concatenate(added, axis=1)
        prefix[...] = prefix[...] + total
        return carry

    blocks = rows // BLOCK

    def attend(i, carry):
        block(i, 0)

        @pl.when(i == blocks // 2)
        def _():
            own_last(1)
            pass_on(0, 3)

        @pl.when(i == blocks - 3)
        def _():
            pass_on(1, 2)

        return carry

    lax.fori_loop(0, blocks, attend, 0)

    def pack(slot, decay, end):
        packs[slot, 0:HV, :] = end.astype(jnp.bfloat16)
        packs[slot, HV:, :] = jnp.broadcast_to(decay, (16, n_key)).astype(jnp.bfloat16)

    def read(slot):
        return packs[slot, HV : HV + 1, :].astype(jnp.float32), packs[slot, 0:HV, :].astype(jnp.float32)

    def end_copy(source, target, number, place):
        return m.copy(packs.at[source], packs.at[target], end_send.at[number], end_recv.at[target], place)

    def join(early, late):
        return early[0] * late[0], early[1] * late[0] + late[1]

    def choose(flag, a, b):
        return jnp.where(flag, a[0], b[0]), jnp.where(flag, a[1], b[1])

    end_x = end_copy(0, 3, 0, m.other["x"])
    end_y = end_copy(1, 4, 1, m.other["y"])
    own_end = (jnp.exp(prefix[...]), state[...])
    pack(0, *own_end)

    arrived(pairs[0], m.piece(0))
    slab(acc2, w2, m.piece(0), True)
    end_x.start()
    pass_on(2, 1)
    enter(3)
    arrived(pairs[0], m.piece(1))
    slab(acc2, w2, m.piece(1), False)
    arrived(pairs[0], m.piece(2))
    slab(acc2, w2, m.piece(2), False)
    arrived(pairs[0], m.piece(3))
    slab(acc2, w2, m.piece(3), False)
    pass_on(1, 3)
    own_last(2)

    def join_x():
        end_x.wait_recv()
        got = read(3)
        own = (jnp.exp(prefix[...]), state[...])
        none = (jnp.ones_like(got[0]), jnp.zeros_like(got[1]))
        late = x == 1
        pre = choose(late, got, none)
        before[0:HV, :] = pre[1]
        before[HV:, :] = jnp.broadcast_to(pre[0], (8, n_key))
        pack(1, *choose(late, join(got, own), join(own, got)))

    def join_y():
        end_y.wait_recv()
        got = read(4)
        two = read(1)
        pre = (before[HV : HV + 1, :], before[0:HV, :])
        late = y == 1
        pre = choose(late, join(got, pre), pre)
        before[0:HV, :] = pre[1]
        before[HV:, :] = jnp.broadcast_to(pre[0], (8, n_key))
        pack(2, *choose(late, join(got, two), join(two, got)))

    pad = seq.shape[1] - rows

    def gate_tiles(low, high):
        def body(i, carry):
            at = pl.ds(pl.multiple_of(i * 128, 128), 128)
            for c in range(n_conv // 128):
                a = acc2[at, c * 128 : (c + 1) * 128].astype(jnp.bfloat16).astype(jnp.float32)
                g = acc2[at, n_conv + c * 128 : n_conv + (c + 1) * 128].astype(jnp.bfloat16).astype(jnp.float32)
                value = (a * jax.nn.sigmoid(g)).astype(jnp.bfloat16)
                seq[c, pl.ds(pl.multiple_of(i * 128 + pad, 32), 128), :] = value.astype(jnp.float32)
            return carry

        lax.fori_loop(low, high, body, 0)

    gate_tiles(rows // 128 - 1, rows // 128)
    for c in range(n_conv // 128):
        halo_out[:, c * 128 : (c + 1) * 128] = seq[c, rows : rows + pad, :].astype(jnp.bfloat16)
    gate_tiles(0, rows // 128 - 1)
    halo = m.copy(halo_out, halo_in, misc_send.at[1], misc_recv.at[1], me + 1)

    @pl.when(me < 15)
    def _():
        halo.start()

    join_x()
    n_taps = taps.shape[0]
    shift = pad - (n_taps - 1)

    def conv_chunk(i):
        base = pl.multiple_of(i * 128, 128)
        sums = jnp.zeros((128, 128), jnp.float32)
        squares = jnp.zeros((128, 128), jnp.float32)
        for c in range(n_conv // 128):
            part = seq[c, pl.ds(base, 128 + pad), :]
            total = jnp.zeros((128, 128), jnp.float32)
            for turn in range(8):
                moved = part if turn == 0 else pltpu.roll(part, 128 + pad - turn, 0)
                for tap in range(n_taps):
                    if (shift + tap) % 8 == turn:
                        start = shift + tap - turn
                        total = total + taps[tap : tap + 1, c * 128 : (c + 1) * 128] * moved[start : start + 128]
            acc2[pl.ds(base, 128), c * 128 : (c + 1) * 128] = total
            sums = sums + total
            squares = squares + total * total
        first = jnp.sum(sums, axis=1, keepdims=True)
        second = jnp.sum(squares, axis=1, keepdims=True)
        lane = lax.broadcasted_iota(jnp.int32, (128, 128), 1)
        stat_own[pl.ds(base, 128), :] = jnp.where(lane == 0, first, second)

    chunks = rows // 128

    def conv_loop(i, carry):
        conv_chunk(i)

        @pl.when(i == chunks // 2)
        def _():
            end_y.start()
            pass_on(2, 2)

        return carry

    lax.fori_loop(1, chunks, conv_loop, 0)

    @pl.when(me > 0)
    def _():
        halo.wait_recv()
        for c in range(n_conv // 128):
            seq[c, 0:pad, :] = halo_in[:, c * 128 : (c + 1) * 128].astype(jnp.float32)

    @pl.when(me == 0)
    def _():
        seq[:, 0:pad, :] = jnp.zeros((n_conv // 128, pad, 128), jnp.float32)

    lax.fori_loop(0, 1, conv_loop, 0)

    pass_on(3, 1)
    own_last(3)
    arrived(pairs[1], m.piece(0))
    slab(acc3, w3, m.piece(0), True)
    stats = m.copy(stat_own, stat_in, misc_send.at[2], misc_recv.at[2], me, 1 - tp)
    stats.start()
    join_y()
    arrived(pairs[1], m.piece(1))
    slab(acc3, w3, m.piece(1), False)
    for k in (1, 2, 3):
        @pl.when(z + k <= 3)
        def _():
            end_copy(2, 4 + k, 1 + k, me + 4 * k).start()

    arrived(pairs[1], m.piece(2))
    slab(acc3, w3, m.piece(2), False)
    arrived(pairs[1], m.piece(3))
    slab(acc3, w3, m.piece(3), False)
    pass_on(2, 3)

    stats.wait_recv()

    def conv_finish(i, carry):
        at = pl.ds(pl.multiple_of(i * 128, 128), 128)
        both_stats = stat_own[at, :] + stat_in[at, :]
        mean_val = both_stats[:, 0:1] / (2 * n_conv)
        square_mean = both_stats[:, 1:2] / (2 * n_conv)
        scale = lax.rsqrt(square_mean - mean_val * mean_val + epsilon)
        value = (acc2[at, 0:n_conv] - mean_val) * scale * conv_gain[...]
        act[at, 0:n_conv] = (value * jax.nn.sigmoid(value)).astype(jnp.bfloat16)
        return carry

    lax.fori_loop(0, chunks, conv_finish, 0)

    for k in (1, 2, 3):
        @pl.when(z - k >= 0)
        def _():
            end_copy(2, 4 + k, 1 + k, me).wait_recv()
            pre = join(read(4 + k), (before[HV : HV + 1, :], before[0:HV, :]))
            before[0:HV, :] = pre[1]
            before[HV:, :] = jnp.broadcast_to(pre[0], (8, n_key))

    entry = jnp.concatenate([init[h].T for h in range(heads)], axis=1)
    state[...] = entry * before[HV : HV + 1, :] + before[0:HV, :]

    def gla_finish(i, carry):
        at = pl.ds(pl.multiple_of(i * 256, 256), 256)
        entering = state[...].astype(jnp.bfloat16)
        for h in range(heads):
            ks, vs = slice(h * HK, (h + 1) * HK), slice(h * HV, (h + 1) * HV)
            value = attn[at, vs] + dot(since[at, ks], entering[:, ks], ((1,), (1,)))
            value = value * lax.rsqrt(jnp.mean(value * value, axis=-1, keepdims=True) + epsilon) * head_gain[...]
            gate = acc3[at, vs].astype(jnp.bfloat16).astype(jnp.float32)
            act[at, n_conv + h * HV : n_conv + (h + 1) * HV] = (value * (gate * jax.nn.sigmoid(gate))).astype(jnp.bfloat16)
        return carry

    lax.fori_loop(0, rows // 256, gla_finish, 0)

    def part_copy(b):
        return m.copy(psend.at[b], precv.at[b], part_send.at[b], part_recv.at[b], me, 1 - tp)

    def out_block(p, yy):
        b = p * 2 + yy
        weight = jnp.concatenate([wo[p, yy, 0], wo[p, yy, 1]], axis=1)
        left = act[pl.ds(pl.multiple_of((1 - tp) * half, half), half), :]
        psend[b] = dot(left, weight, ((1,), (0,))).astype(jnp.bfloat16)
        left = act[pl.ds(pl.multiple_of(tp * half, half), half), :]
        pown[b] = dot(left, weight, ((1,), (0,))).astype(jnp.bfloat16)
        part_copy(b).start()

    def out_copy(b):
        return pltpu.make_async_copy(outv.at[b], out.at[:, pl.ds(pl.multiple_of(b * 256, 256), 256)], out_sem.at[b])

    def merge(p, yy):
        b = p * 2 + yy
        part_copy(b).wait_recv()
        outv[b] = (pown[b].astype(jnp.float32) + precv[b].astype(jnp.float32)).astype(jnp.bfloat16)
        out_copy(b).start()

    def out_pieces(j):
        def body(yy, carry):
            out_block(m.piece(j), yy)
            return carry

        arrived(pairs[2] + pairs[3], m.piece(j))
        lax.fori_loop(0, 2, body, 0)

    def merges(j):
        def body(yy, carry):
            merge(m.piece(j), yy)
            return carry

        lax.fori_loop(0, 2, body, 0)

    out_pieces(0)
    out_pieces(1)
    merges(0)
    pass_on(3, 2)
    out_pieces(2)
    merges(1)
    pass_on(3, 3)
    merges(2)
    out_pieces(3)
    merges(3)

    swap.wait_send()
    stats.wait_send()

    @pl.when(me < 15)
    def _():
        halo.wait_send()

    end_x.wait_send()
    end_y.wait_send()
    for k in (1, 2, 3):
        @pl.when(z + k <= 3)
        def _():
            end_copy(2, 4 + k, 1 + k, me + 4 * k).wait_send()

    for p in range(4):
        for f in (b1, b2):
            f.first_copy(p).wait_send()
            f.last_copy(p).wait_send()
        for pair in pairs:
            for f in pair:
                f.last_copy(p).wait_send()
    for pair in pairs:
        for f in pair:
            f.first_copy(z).wait_send()
    whole.drain()
    for pair in lines:
        for line in pair:
            line.drain()
    for b in range(8):
        part_copy(b).wait_send()
        out_copy(b).wait()


def fused_layer(
    tokens, norm_gain, w_conv_a, w_conv_gate, conv_weight, conv_gain, w_query, w_key, w_value, w_outgate,
    w_decay, decay_bias, decay_extra, head_gain, init_state, w_out_conv, w_out_gla,
):
    rows, width = tokens.shape
    depth = w_query.shape[0]
    n_key = w_query.shape[1]
    n_conv = w_conv_a.shape[1]
    cols = w_out_conv.shape[1]
    half = rows // 2
    pad = 32
    bf16, f32 = jnp.bfloat16, jnp.float32
    dma = pltpu.SemaphoreType.DMA
    vm = pl.BlockSpec(memory_space=pltpu.VMEM)
    hbm = pl.BlockSpec(memory_space=pl.ANY)
    return pl.pallas_call(
        layer_kernel,
        out_shape=jax.ShapeDtypeStruct((half, 2 * width), bf16),
        in_specs=[hbm, vm, hbm, hbm, vm, vm, hbm, hbm, hbm, hbm, hbm, vm, hbm, vm, vm, hbm, hbm],
        out_specs=hbm,
        scratch_shapes=[
            pltpu.VMEM((4, 2, 2, depth, 5 * n_key), bf16),
            pltpu.VMEM((4, 2, 2, depth, 2 * n_conv), bf16),
            pltpu.VMEM((4, 2, 2, depth, n_conv), bf16),
            pltpu.VMEM((4, 2, 2, 2 * n_conv, cols), bf16),
            pltpu.VMEM((2, rows, width), bf16),
            pltpu.VMEM((rows, 2 * width), bf16),
            pltpu.VMEM((rows, 5 * n_key), f32),
            pltpu.VMEM((rows, 2 * n_conv), f32),
            pltpu.VMEM((rows, n_conv), f32),
            pltpu.VMEM((rows, n_key), f32),
            pltpu.VMEM((n_conv // 128, rows + pad, 128), f32),
            pltpu.VMEM((rows, n_conv), f32),
            pltpu.VMEM((rows, n_key), bf16),
            pltpu.VMEM((rows, 2 * n_conv), bf16),
            pltpu.VMEM((8, half, 256), bf16),
            pltpu.VMEM((8, half, 256), bf16),
            pltpu.VMEM((8, half, 256), bf16),
            pltpu.VMEM((8, half, 256), bf16),
            pltpu.VMEM((pad, n_conv), bf16),
            pltpu.VMEM((pad, n_conv), bf16),
            pltpu.VMEM((rows, 128), f32),
            pltpu.VMEM((rows, 128), f32),
            pltpu.VMEM((8, HV + 16, n_key), bf16),
            pltpu.VMEM((HV, n_key), f32),
            pltpu.VMEM((1, n_key), f32),
            pltpu.VMEM((HV + 8, n_key), f32),
            dma((11,)), dma((10, 4)), dma((10, 4)), dma((10, 4)), dma((10, 4)), dma((9, 4)), dma((9, 4)), dma((9, 4)),
            dma((3,)), dma((3,)), dma((5,)), dma((8,)), dma((8,)), dma((8,)), dma((8,)),
        ],
        compiler_params=pltpu.CompilerParams(collective_id=0, has_side_effects=True, vmem_limit_bytes=67043328),
        name="layer",
    )(
        tokens, norm_gain[None, :], w_conv_a, w_conv_gate, conv_weight, conv_gain[None, :], w_query, w_key, w_value,
        w_outgate, w_decay, decay_bias[None, :], decay_extra, head_gain[None, :], init_state, w_out_conv, w_out_gla,
    )


def local_kernel(heads, pieces, q_ref, k_ref, v_ref, pre_ref, extra_ref, bias_ref, attn_ref, since_ref, end_ref, log_ref, state, prefix):
    step = pl.program_id(0)

    @pl.when(step == 0)
    def _():
        state[...] = jnp.zeros_like(state)
        prefix[...] = jnp.zeros_like(prefix)

    rows = lax.broadcasted_iota(jnp.int32, (BLOCK, BLOCK), 0)
    columns = lax.broadcasted_iota(jnp.int32, (BLOCK, BLOCK), 1)
    causal = rows >= columns
    lower = causal.astype(jnp.float32)
    for piece in range(pieces):
        at = pl.ds(piece * BLOCK, BLOCK)
        pre = pre_ref[at, :] + bias_ref[...]
        logs = jax.nn.log_sigmoid(pre) / gate_divisor + extra_ref[at, :]
        cum = lax.dot_general(
            lower, logs, (((1,), (0,)), ((), ())), precision=lax.Precision.HIGHEST, preferred_element_type=jnp.float32
        )
        total = cum[BLOCK - 1 :, :]
        middle = cum[BLOCK // 2 - 1 : BLOCK // 2, :]
        query = q_ref[at, :].astype(jnp.float32) * HK ** (-0.5)
        keys = k_ref[at, :].astype(jnp.float32)
        decayed = query * jnp.exp(cum)
        since_ref[at, :] = (decayed * jnp.exp(prefix[...])).astype(jnp.bfloat16)
        decayed = decayed.astype(jnp.bfloat16)
        query = (query * jnp.exp(cum - middle)).astype(jnp.bfloat16)
        inverse = (keys * jnp.exp(middle - cum)).astype(jnp.bfloat16)
        to_end = (keys * jnp.exp(total - cum)).astype(jnp.bfloat16)
        entering = state[...].astype(jnp.bfloat16)
        added = []
        for h in range(heads):
            ks, vs = slice(h * HK, (h + 1) * HK), slice(h * HV, (h + 1) * HV)
            values = v_ref[at, vs]
            scores = jnp.where(causal, dot(query[:, ks], inverse[:, ks], ((1,), (1,))), 0.0)
            attn_ref[at, vs] = dot(scores.astype(jnp.bfloat16), values, ((1,), (0,))) + dot(
                decayed[:, ks], entering[:, ks], ((1,), (1,))
            )
            added.append(dot(values, to_end[:, ks], ((0,), (0,))))
        added = added[0] if heads == 1 else jnp.concatenate(added, axis=1)
        state[...] = state[...] * jnp.exp(total) + added
        prefix[...] = prefix[...] + total
    end_ref[...] = state[...]
    log_ref[...] = prefix[...]


def gla_local(query, keys, values, decay_pre, decay_extra, decay_bias):
    rows, width = query.shape
    heads = width // HK
    pieces = 4
    tile = pieces * BLOCK

    def tiled(array):
        return pl.BlockSpec((tile, array.shape[1]), lambda i: (i, 0))

    def whole(shape):
        return pl.BlockSpec(shape, lambda i: (0, 0))

    return pl.pallas_call(
        functools.partial(local_kernel, heads, pieces),
        grid=(rows // tile,),
        in_specs=[tiled(query), tiled(keys), tiled(values), tiled(decay_pre), tiled(decay_extra), whole((1, width))],
        out_specs=[tiled(values), tiled(query), whole((HV, width)), whole((1, width))],
        out_shape=[
            jax.ShapeDtypeStruct(values.shape, jnp.float32),
            jax.ShapeDtypeStruct(query.shape, jnp.bfloat16),
            jax.ShapeDtypeStruct((HV, width), jnp.float32),
            jax.ShapeDtypeStruct((1, width), jnp.float32),
        ],
        scratch_shapes=[pltpu.VMEM((HV, width), jnp.float32), pltpu.VMEM((1, width), jnp.float32)],
        cost_estimate=pl.CostEstimate(flops=10**10, bytes_accessed=10**7, transcendentals=10**6),
        name="gla_local",
    )(query, keys, values, decay_pre, decay_extra, decay_bias[None, :])


def finish_kernel(heads, size, where_ref, attn_ref, since_ref, gate_ref, ends_ref, init_ref, gain_ref, out_ref, state):
    me = where_ref[0]

    @pl.when(pl.program_id(0) == 0)
    def _():
        state[...] = init_ref[...]

        def one(device, carry):
            at = device
            decay = ends_ref[pl.ds(pl.multiple_of(at * size + HV, 16), 16), :].astype(jnp.float32)[:1]
            end = ends_ref[pl.ds(pl.multiple_of(at * size, 16), HV), :].astype(jnp.float32)
            state[...] = state[...] * decay + end
            return carry

        lax.fori_loop(0, me, one, 0)

    entering = state[...].astype(jnp.bfloat16)
    for h in range(heads):
        ks, vs = slice(h * HK, (h + 1) * HK), slice(h * HV, (h + 1) * HV)
        attn = attn_ref[:, vs] + dot(since_ref[:, ks], entering[:, ks], ((1,), (1,)))
        attn = attn * lax.rsqrt(jnp.mean(attn * attn, axis=-1, keepdims=True) + epsilon) * gain_ref[...]
        gate = gate_ref[:, vs].astype(jnp.float32)
        out_ref[:, vs] = (attn * (gate * jax.nn.sigmoid(gate))).astype(jnp.bfloat16)


def gla_finish(attn, since, out_gate, ends, init_state, head_gain, me):
    rows, width = since.shape
    heads = width // HK
    tile = 256

    def tiled(array):
        return pl.BlockSpec((tile, array.shape[1]), lambda i, w: (i, 0))

    def whole(array):
        return pl.BlockSpec(array.shape, lambda i, w: (0, 0))

    init = init_state.transpose(2, 0, 1).reshape(HV, width)
    gain = head_gain[None, :]
    return pl.pallas_call(
        functools.partial(finish_kernel, heads, HV + 16),
        grid_spec=pltpu.PrefetchScalarGridSpec(
            num_scalar_prefetch=1,
            grid=(rows // tile,),
            in_specs=[tiled(attn), tiled(since), tiled(out_gate), whole(ends), whole(init), whole(gain)],
            out_specs=tiled(attn),
            scratch_shapes=[pltpu.VMEM((HV, width), jnp.float32)],
        ),
        out_shape=jax.ShapeDtypeStruct(attn.shape, jnp.bfloat16),
        cost_estimate=pl.CostEstimate(flops=3 * 10**9, bytes_accessed=10**7, transcendentals=10**6),
        name="gla_finish",
    )(me[None], attn, since, out_gate, ends, init, gain)


def conv_branch(gated, conv_weight, conv_gain):
    taps = conv_weight.shape[0]
    row_count = gated.shape[0]
    count = lax.axis_size("sp")
    earlier = lax.ppermute(gated[row_count - taps + 1 :], "sp", [(i, i + 1) for i in range(count - 1)])
    extended = jnp.concatenate([earlier, gated], axis=0).astype(jnp.float32)
    conv_sum = jnp.zeros(gated.shape, jnp.float32)
    for tap in range(taps):
        conv_sum = conv_sum + conv_weight[tap][None, :] * extended[tap : tap + row_count]
    row_sums, row_squares = lax.psum((jnp.sum(conv_sum, axis=1), jnp.sum(conv_sum * conv_sum, axis=1)), "tp")
    mean_val = (row_sums / D_CONV)[:, None]
    square_mean = (row_squares / D_CONV)[:, None]
    conv_norm = (conv_sum - mean_val) * lax.rsqrt(square_mean - mean_val * mean_val + epsilon) * conv_gain
    return jax.nn.silu(conv_norm).astype(jnp.bfloat16)


def project(hidden, weight):
    return dot(hidden, weight, ((1,), (0,)))


def plain_layer(
    tokens, norm_gain, w_conv_a, w_conv_gate, conv_weight, conv_gain, w_query, w_key, w_value, w_outgate,
    w_decay, decay_bias, decay_extra, head_gain, init_state, w_out_conv, w_out_gla,
):
    me = lax.axis_index("sp")

    def gather(shard):
        return lax.all_gather(shard, "sp", axis=0, tiled=True)

    widened = lax.all_gather(tokens, "tp", axis=1, tiled=True).astype(jnp.float32)
    normed = (
        widened * lax.rsqrt(jnp.mean(widened * widened, axis=-1, keepdims=True) + epsilon) * norm_gain
    ).astype(jnp.bfloat16)
    half = w_query.shape[1]
    conv_a = project(normed, gather(w_conv_a)).astype(jnp.bfloat16)
    conv_gate = project(normed, gather(w_conv_gate)).astype(jnp.bfloat16)
    full_qkd = gather(jnp.concatenate([w_query, w_key, w_decay], axis=1))
    full_v = gather(w_value)
    gated = (conv_a.astype(jnp.float32) * jax.nn.sigmoid(conv_gate.astype(jnp.float32))).astype(jnp.bfloat16)
    conv_out = conv_branch(gated, conv_weight, conv_gain)
    query_keys = project(normed, full_qkd[:, : 2 * half]).astype(jnp.bfloat16)
    decay_pre = project(normed, full_qkd[:, 2 * half :])
    values = project(normed, full_v).astype(jnp.bfloat16)
    attn, since, end, end_log = gla_local(
        query_keys[:, :half], query_keys[:, half:], values, decay_pre, decay_extra, decay_bias
    )
    packed = jnp.concatenate([end, jnp.broadcast_to(jnp.exp(end_log), (16, half))], axis=0).astype(jnp.bfloat16)
    ends = gather(packed)
    out_gate = project(normed, gather(w_outgate)).astype(jnp.bfloat16)
    gla_out = gla_finish(attn, since, out_gate, ends, init_state, head_gain, me)
    total = dot(conv_out, gather(w_out_conv.T), ((1,), (1,))) + dot(gla_out, gather(w_out_gla.T), ((1,), (1,)))
    return lax.psum_scatter(total.astype(jnp.bfloat16), "tp", scatter_dimension=0, tiled=True)


def per_device(*arrays):
    if folded(lax.axis_size("sp"), lax.axis_size("tp")):
        return fused_layer(*arrays)
    return plain_layer(*arrays)


def solution(mesh):
    placed = (
        P("sp", "tp"), P(), P("sp", "tp"), P("sp", "tp"), P(None, "tp"), P("tp"), P("sp", "tp"), P("sp", "tp"),
        P("sp", "tp"), P("sp", "tp"), P("sp", "tp"), P("tp"), P("sp", "tp"), P(), P("tp", None, None),
        P("tp", "sp"), P("tp", "sp"),
    )
    return jax.shard_map(
        per_device, mesh=mesh, in_specs=placed, out_specs=P(("sp", "tp"), None), check_vma=False
    )
```

```python
import functools

import jax
import jax.numpy as jnp
from jax import lax
from jax.experimental import pallas as pl
from jax.experimental.pallas import tpu as pltpu
from jax.sharding import PartitionSpec as P

D_CONV = 1024
HK = 64
HV = 128
BLOCK = 64

epsilon = 1e-06
gate_divisor = 16.0

MESH = pl.DeviceIdType.MESH


def dot(a, b, dims):
    return lax.dot_general(a, b, (dims, ((), ())), preferred_element_type=jnp.float32)


def folded(n_sp, n_tp):
    return n_sp == 16 and n_tp == 2


class Mover:
    def __init__(self):
        self.me = lax.axis_index("sp")
        self.tp = lax.axis_index("tp")
        self.z, self.y, self.x = self.me // 4, (self.me // 2) % 2, self.me % 2
        self.other = {"x": self.me + 1 - 2 * self.x, "y": self.me + 2 - 4 * self.y}
        self.across = self.me + 3 - 2 * self.x - 4 * self.y
        self.sent = []

    def copy(self, source, target, send, recv, place, core=None):
        core = self.tp if core is None else core
        return pltpu.make_async_remote_copy(
            src_ref=source, dst_ref=target, send_sem=send, recv_sem=recv, device_id=(place, core), device_id_type=MESH
        )

    def piece(self, j):
        z = self.z
        return (z, z + 1 - 2 * (z % 2), 2 - z // 2, 3 - 3 * (z // 2))[j]


class Flow:
    def __init__(self, mover, number, view, first, sems):
        self.m, self.number, self.view, self.first = mover, number, view, first
        self.last = {"x": "y", "y": "x"}[first]
        self.sems = sems

    def own(self, p):
        return self.view(p, self.m.y, self.m.x)

    def pair(self, p):
        every = slice(None)
        return self.view(p, self.m.y, every) if self.first == "x" else self.view(p, every, self.m.x)

    def first_copy(self, p):
        own = self.own(p)
        fs, fr = self.sems["first_send"], self.sems["first_recv"]
        return self.m.copy(own, own, fs.at[self.number, p], fr.at[self.number, p], self.m.other[self.first])

    def last_copy(self, p):
        pair = self.pair(p)
        ls, lr = self.sems["last_send"], self.sems["last_recv"]
        return self.m.copy(pair, pair, ls.at[self.number, p], lr.at[self.number, p], self.m.other[self.last])


class Line:
    def __init__(self, mover, number, view, sems):
        self.m, self.number, self.view, self.sems = mover, number, view, sems

    def up(self, p):
        return self.m.copy(
            self.view(p), self.view(p), self.sems["up_send"].at[self.number, p], self.sems["z_recv"].at[self.number, p],
            self.m.me + 4,
        )

    def down(self, p):
        return self.m.copy(
            self.view(p), self.view(p), self.sems["down_send"].at[self.number, p],
            self.sems["z_recv"].at[self.number, p], self.m.me - 4,
        )

    def start_own(self):
        z = self.m.z

        @pl.when(z < 3)
        def _():
            self.up(z).start()

        @pl.when(z > 0)
        def _():
            self.down(z).start()

    def relay(self, step, then):
        z = self.m.z

        @pl.when(z >= step)
        def _():
            p = z - step
            self.up(p).wait_recv()

            @pl.when(z < 3)
            def _():
                self.up(p).start()

            then(p)

        @pl.when(z + step <= 3)
        def _():
            p = z + step
            self.down(p).wait_recv()

            @pl.when(z > 0)
            def _():
                self.down(p).start()

            then(p)

    def drain(self):
        z = self.m.z
        for p in range(4):
            @pl.when((p <= z) & (z < 3))
            def _():
                self.up(p).wait_send()

            @pl.when((p >= z) & (z > 0))
            def _():
                self.down(p).wait_send()


def at_step(z, step, then):
    if step == 0:
        then(z)
        return

    @pl.when(z >= step)
    def _():
        then(z - step)

    @pl.when(z + step <= 3)
    def _():
        then(z + step)


def layer_kernel(
    tokens, gain, wa, wg, taps, conv_gain, wq, wk, wv, wog, wd, bias, extra_in, head_gain, init, woc, wogl, own_out, other_out,
    w1, w2, w3, wo, both, normed, acc1, acc2, acc3, extra, seq, attn, since, act, psend,
    halo_out, halo_in, stat_own, stat_in, packs, state, prefix, before,
    local, first_send, first_recv, last_send, last_recv, up_send, down_send, z_recv, misc_send, misc_recv, end_send, end_recv,
    part_send, part_recv,
):
    m = Mover()
    me, tp, z, y, x = m.me, m.tp, m.z, m.y, m.x
    rows = normed.shape[0]
    half = rows // 2
    width = both.shape[2]
    n_key = acc1.shape[1] // 5
    n_conv = 2 * n_key
    heads = n_key // HK
    sems = dict(
        first_send=first_send, first_recv=first_recv, last_send=last_send, last_recv=last_recv,
        up_send=up_send, down_send=down_send, z_recv=z_recv,
    )

    def lanes(ref, low, size):
        return lambda p, yy, xx: ref.at[p, yy, xx, :, pl.ds(low, size)]

    def depth(low, size):
        return lambda p, yy, xx: wo.at[p, yy, xx, pl.ds(low, size), :]

    mid = w1.shape[-1] // 2
    late = wo.shape[3] // 8
    early = wo.shape[3] // 2 - late
    b1 = Flow(m, 0, lanes(w1, 0, mid), "x", sems)
    b2 = Flow(m, 1, lanes(w1, mid, mid), "y", sems)
    pairs = [
        (Flow(m, 2, lanes(w2, 0, n_conv), "x", sems), Flow(m, 3, lanes(w2, n_conv, n_conv), "y", sems)),
        (Flow(m, 4, lanes(w3, 0, n_key), "x", sems), Flow(m, 5, lanes(w3, n_key, n_key), "y", sems)),
        (Flow(m, 6, depth(0, early), "x", sems), Flow(m, 7, depth(early, early), "y", sems)),
        (Flow(m, 8, depth(2 * early, late), "x", sems), Flow(m, 9, depth(2 * early + late, late), "y", sems)),
    ]
    whole = Line(m, 0, lambda p: w1.at[p, y, x], sems)
    lines = [tuple(Line(m, f.number - 1, f.pair, sems) for f in pair) for pair in pairs]

    loads = [
        (wq, w1.at[z, y, x, :, pl.ds(0, n_key)]),
        (wk, w1.at[z, y, x, :, pl.ds(n_key, n_key)]),
        (wd, w1.at[z, y, x, :, pl.ds(2 * n_key, n_key)]),
        (wv, w1.at[z, y, x, :, pl.ds(3 * n_key, n_conv)]),
        (wa, w2.at[z, y, x, :, pl.ds(0, n_conv)]),
        (wg, w2.at[z, y, x, :, pl.ds(n_conv, n_conv)]),
        (wog, w3.at[z, y, x]),
        (woc, wo.at[z, y, x, pl.ds(0, n_conv), :]),
        (wogl, wo.at[z, y, x, pl.ds(n_conv, n_conv), :]),
        (tokens, both.at[tp]),
        (extra_in, extra),
    ]
    loads = [pltpu.make_async_copy(a, b, local.at[i]) for i, (a, b) in enumerate(loads)]
    for load in loads:
        load.start()

    barrier = pltpu.get_barrier_semaphore()
    partners = [(m.other["x"], tp), (m.other["y"], tp), (m.across, tp), (me, 1 - tp)]
    partners += [((me + k) % 16, tp) for k in (4, 8, 12, 1, 15)]
    for place, core in partners:
        pl.semaphore_signal(barrier, inc=1, device_id=(place, core), device_id_type=MESH)
    pl.semaphore_wait(barrier, len(partners))

    for i in range(4):
        loads[i].wait()
    whole.start_own()
    b1.first_copy(z).start()
    b2.first_copy(z).start()
    loads[9].wait()
    swap = m.copy(both.at[tp], both.at[tp], misc_send.at[0], misc_recv.at[0], me, 1 - tp)
    swap.start()
    loads[4].wait()
    loads[5].wait()
    for f in pairs[0]:
        f.first_copy(z).start()
    loads[6].wait()
    for f in pairs[1]:
        f.first_copy(z).start()
    for i in (7, 8, 10):
        loads[i].wait()

    def head_firsts(step):
        def one(p):
            b1.first_copy(p).wait_recv()
            b1.last_copy(p).start()
            b2.first_copy(p).wait_recv()
            b2.last_copy(p).start()

        at_step(z, step, one)

    def head_line(step):
        def then(p):
            b1.first_copy(p).start()
            b2.first_copy(p).start()

        whole.relay(step, then)

    def begin(k):
        for f in pairs[k]:
            f.first_copy(z).start()

    def enter_one(k, i):
        pairs[k][i].first_copy(z).wait_recv()
        lines[k][i].start_own()

    def enter(k):
        enter_one(k, 0)
        enter_one(k, 1)

    def own_last(k):
        for f in pairs[k]:
            f.last_copy(z).start()

    def pass_on(k, step):
        for f, line in zip(pairs[k], lines[k]):
            line.relay(step, lambda p: f.last_copy(p).start())

    def arrived(flows, p):
        for f in flows:
            f.last_copy(p).wait_recv()

    def norm_tiles(low, high):
        def body(i, carry):
            at = pl.ds(pl.multiple_of(i * 128, 128), 128)
            a = both[0, at, :].astype(jnp.float32)
            b = both[1, at, :].astype(jnp.float32)
            square = jnp.sum(a * a + b * b, axis=1, keepdims=True)
            scale = lax.rsqrt(square / (2 * width) + epsilon)
            normed[at, :width] = (a * scale * gain[:, :width]).astype(jnp.bfloat16)
            normed[at, width:] = (b * scale * gain[:, width:]).astype(jnp.bfloat16)
            return carry

        lax.fori_loop(low, high, body, 0)

    def slab(acc, ref, p, first):
        size = ref.shape[1] * ref.shape[2] * ref.shape[3]

        def body(c, carry):
            at = pl.ds(pl.multiple_of(c * 256, 256), 256)
            left = normed[:, pl.ds(pl.multiple_of(p * size, size), size)]
            right = ref[p, :, :, :, at].reshape(size, 256)
            got = dot(left, right, ((1,), (0,)))
            if first:
                acc[:, at] = got
            else:
                acc[:, at] += got
            return carry

        lax.fori_loop(0, acc.shape[1] // 256, body, 0)

    swap.wait_recv()
    norm_tiles(0, 4)
    head_line(1)
    head_firsts(0)
    norm_tiles(4, 8)
    enter_one(0, 0)
    head_line(2)
    enter_one(0, 1)
    head_firsts(1)
    head_line(3)
    arrived((b1, b2), m.piece(0))
    slab(acc1, w1, m.piece(0), True)
    head_firsts(2)
    begin(2)
    begin(3)
    pass_on(0, 1)
    arrived((b1, b2), m.piece(1))
    slab(acc1, w1, m.piece(1), False)
    head_firsts(3)
    enter(1)
    own_last(0)
    pass_on(0, 2)
    arrived((b1, b2), m.piece(2))
    slab(acc1, w1, m.piece(2), False)
    pass_on(1, 1)
    enter(2)
    arrived((b1, b2), m.piece(3))
    slab(acc1, w1, m.piece(3), False)

    state[...] = jnp.zeros_like(state)
    prefix[...] = jnp.zeros_like(prefix)
    r_iota = lax.broadcasted_iota(jnp.int32, (BLOCK, BLOCK), 0)
    c_iota = lax.broadcasted_iota(jnp.int32, (BLOCK, BLOCK), 1)
    causal = r_iota >= c_iota
    lower = causal.astype(jnp.float32)

    def block(i, carry):
        at = pl.ds(pl.multiple_of(i * BLOCK, BLOCK), BLOCK)
        pre = acc1[at, 2 * n_key : 3 * n_key] + bias[...]
        logs = jax.nn.log_sigmoid(pre) / gate_divisor + extra[at, :]
        cum = lax.dot_general(
            lower, logs, (((1,), (0,)), ((), ())), precision=lax.Precision.HIGHEST, preferred_element_type=jnp.float32
        )
        total = cum[BLOCK - 1 :, :]
        middle = cum[BLOCK // 2 - 1 : BLOCK // 2, :]
        query = acc1[at, 0:n_key].astype(jnp.bfloat16).astype(jnp.float32) * HK ** (-0.5)
        keys = acc1[at, n_key : 2 * n_key].astype(jnp.bfloat16).astype(jnp.float32)
        decayed = query * jnp.exp(cum)
        since[at, :] = (decayed * jnp.exp(prefix[...])).astype(jnp.bfloat16)
        decayed = decayed.astype(jnp.bfloat16)
        query = (query * jnp.exp(cum - middle)).astype(jnp.bfloat16)
        inverse = (keys * jnp.exp(middle - cum)).astype(jnp.bfloat16)
        to_end = (keys * jnp.exp(total - cum)).astype(jnp.bfloat16)
        entering = state[...].astype(jnp.bfloat16)
        added = []
        for h in range(heads):
            ks, vs = slice(h * HK, (h + 1) * HK), slice(h * HV, (h + 1) * HV)
            values = acc1[at, 3 * n_key + h * HV : 3 * n_key + (h + 1) * HV].astype(jnp.bfloat16)
            scores = jnp.where(causal, dot(query[:, ks], inverse[:, ks], ((1,), (1,))), 0.0)
            attn[at, vs] = dot(scores.astype(jnp.bfloat16), values, ((1,), (0,))) + dot(
                decayed[:, ks], entering[:, ks], ((1,), (1,))
            )
            added.append(dot(values, to_end[:, ks], ((0,), (0,))))
        state[...] = state[...] * jnp.exp(total) + jnp.concatenate(added, axis=1)
        prefix[...] = prefix[...] + total
        return carry

    blocks = rows // BLOCK

    def attend(i, carry):
        block(i, 0)

        @pl.when(i == blocks // 2)
        def _():
            own_last(1)
            pass_on(0, 3)

        @pl.when(i == blocks - 3)
        def _():
            pass_on(1, 2)

        return carry

    lax.fori_loop(0, blocks, attend, 0)

    def pack(slot, decay, end):
        packs[slot, 0:HV, :] = end.astype(jnp.bfloat16)
        packs[slot, HV:, :] = jnp.broadcast_to(decay, (16, n_key)).astype(jnp.bfloat16)

    def read(slot):
        return packs[slot, HV : HV + 1, :].astype(jnp.float32), packs[slot, 0:HV, :].astype(jnp.float32)

    def end_copy(source, target, number, place):
        return m.copy(packs.at[source], packs.at[target], end_send.at[number], end_recv.at[target], place)

    def join(early, late):
        return early[0] * late[0], early[1] * late[0] + late[1]

    near_ends = [
        end_copy(0, 1, 0, m.other["x"]),
        end_copy(0, 2, 1, m.other["y"]),
        end_copy(0, 3, 2, m.across),
    ]
    pack(0, jnp.exp(prefix[...]), state[...])

    arrived(pairs[0], m.piece(0))
    slab(acc2, w2, m.piece(0), True)
    for end in near_ends:
        end.start()
    pass_on(2, 1)
    enter(3)
    arrived(pairs[0], m.piece(1))
    slab(acc2, w2, m.piece(1), False)
    arrived(pairs[0], m.piece(2))
    slab(acc2, w2, m.piece(2), False)
    arrived(pairs[0], m.piece(3))
    slab(acc2, w2, m.piece(3), False)
    pass_on(1, 3)
    own_last(2)

    def join_near():
        for end in near_ends:
            end.wait_recv()
        run = (jnp.ones((1, n_key), jnp.float32), jnp.zeros((HV, n_key), jnp.float32))
        pre = run
        for yy in range(2):
            for xx in range(2):
                past = yy * 2 + xx < y * 2 + x
                run = join(run, read((y + yy - 2 * y * yy) * 2 + x + xx - 2 * x * xx))
                pre = jnp.where(past, run[0], pre[0]), jnp.where(past, run[1], pre[1])
        before[0:HV, :] = pre[1]
        before[HV:, :] = jnp.broadcast_to(pre[0], (8, n_key))
        pack(4, *run)

    def far_end(k):
        return end_copy(4, 4 + k, 2 + k, me + 4 * k)

    pad = seq.shape[1] - rows

    def gate_tiles(low, high):
        def body(i, carry):
            at = pl.ds(pl.multiple_of(i * 128, 128), 128)
            for c in range(n_conv // 128):
                a = acc2[at, c * 128 : (c + 1) * 128].astype(jnp.bfloat16).astype(jnp.float32)
                g = acc2[at, n_conv + c * 128 : n_conv + (c + 1) * 128].astype(jnp.bfloat16).astype(jnp.float32)
                value = (a * jax.nn.sigmoid(g)).astype(jnp.bfloat16)
                seq[c, pl.ds(pl.multiple_of(i * 128 + pad, 32), 128), :] = value.astype(jnp.float32)
            return carry

        lax.fori_loop(low, high, body, 0)

    gate_tiles(rows // 128 - 1, rows // 128)
    for c in range(n_conv // 128):
        halo_out[:, c * 128 : (c + 1) * 128] = seq[c, rows : rows + pad, :].astype(jnp.bfloat16)
    gate_tiles(0, rows // 128 - 1)
    halo = m.copy(halo_out, halo_in, misc_send.at[1], misc_recv.at[1], me + 1)

    @pl.when(me < 15)
    def _():
        halo.start()

    n_taps = taps.shape[0]
    shift = pad - (n_taps - 1)

    def conv_chunk(i):
        base = pl.multiple_of(i * 128, 128)
        sums = jnp.zeros((128, 128), jnp.float32)
        squares = jnp.zeros((128, 128), jnp.float32)
        for c in range(n_conv // 128):
            part = seq[c, pl.ds(base, 128 + pad), :]
            total = jnp.zeros((128, 128), jnp.float32)
            for turn in range(8):
                moved = part if turn == 0 else pltpu.roll(part, 128 + pad - turn, 0)
                for tap in range(n_taps):
                    if (shift + tap) % 8 == turn:
                        start = shift + tap - turn
                        total = total + taps[tap : tap + 1, c * 128 : (c + 1) * 128] * moved[start : start + 128]
            acc2[pl.ds(base, 128), c * 128 : (c + 1) * 128] = total
            sums = sums + total
            squares = squares + total * total
        first = jnp.sum(sums, axis=1, keepdims=True)
        second = jnp.sum(squares, axis=1, keepdims=True)
        lane = lax.broadcasted_iota(jnp.int32, (128, 128), 1)
        stat_own[pl.ds(base, 128), :] = jnp.where(lane == 0, first, second)

    chunks = rows // 128

    def conv_loop(i, carry):
        conv_chunk(i)

        @pl.when(i == chunks // 2)
        def _():
            pass_on(2, 2)

        return carry

    lax.fori_loop(1, chunks, conv_loop, 0)

    @pl.when(me > 0)
    def _():
        halo.wait_recv()
        for c in range(n_conv // 128):
            seq[c, 0:pad, :] = halo_in[:, c * 128 : (c + 1) * 128].astype(jnp.float32)

    @pl.when(me == 0)
    def _():
        seq[:, 0:pad, :] = jnp.zeros((n_conv // 128, pad, 128), jnp.float32)

    lax.fori_loop(0, 1, conv_loop, 0)

    pass_on(3, 1)
    own_last(3)
    arrived(pairs[1], m.piece(0))
    slab(acc3, w3, m.piece(0), True)
    stats = m.copy(stat_own, stat_in, misc_send.at[2], misc_recv.at[2], me, 1 - tp)
    stats.start()
    join_near()
    arrived(pairs[1], m.piece(1))
    slab(acc3, w3, m.piece(1), False)
    for k in (1, 2, 3):
        @pl.when(z + k <= 3)
        def _():
            far_end(k).start()

    arrived(pairs[1], m.piece(2))
    slab(acc3, w3, m.piece(2), False)
    arrived(pairs[1], m.piece(3))
    slab(acc3, w3, m.piece(3), False)
    pass_on(2, 3)
    stats.wait_recv()

    def conv_finish(i, carry):
        at = pl.ds(pl.multiple_of(i * 128, 128), 128)
        both_stats = stat_own[at, :] + stat_in[at, :]
        mean_val = both_stats[:, 0:1] / (2 * n_conv)
        square_mean = both_stats[:, 1:2] / (2 * n_conv)
        scale = lax.rsqrt(square_mean - mean_val * mean_val + epsilon)
        value = (acc2[at, 0:n_conv] - mean_val) * scale * conv_gain[...]
        act[at, 0:n_conv] = (value * jax.nn.sigmoid(value)).astype(jnp.bfloat16)
        return carry

    lax.fori_loop(0, chunks, conv_finish, 0)
    pass_on(3, 2)
    for k in (1, 2, 3):
        @pl.when(z - k >= 0)
        def _():
            end_copy(4, 4 + k, 2 + k, me).wait_recv()
            pre = join(read(4 + k), (before[HV : HV + 1, :], before[0:HV, :]))
            before[0:HV, :] = pre[1]
            before[HV:, :] = jnp.broadcast_to(pre[0], (8, n_key))

    entry = jnp.concatenate([init[h].T for h in range(heads)], axis=1)
    state[...] = entry * before[HV : HV + 1, :] + before[0:HV, :]

    def gla_finish(i, carry):
        at = pl.ds(pl.multiple_of(i * 256, 256), 256)
        entering = state[...].astype(jnp.bfloat16)
        for h in range(heads):
            ks, vs = slice(h * HK, (h + 1) * HK), slice(h * HV, (h + 1) * HV)
            value = attn[at, vs] + dot(since[at, ks], entering[:, ks], ((1,), (1,)))
            value = value * lax.rsqrt(jnp.mean(value * value, axis=-1, keepdims=True) + epsilon) * head_gain[...]
            gate = acc3[at, vs].astype(jnp.bfloat16).astype(jnp.float32)
            act[at, n_conv + h * HV : n_conv + (h + 1) * HV] = (value * (gate * jax.nn.sigmoid(gate))).astype(jnp.bfloat16)
        return carry

    lax.fori_loop(0, rows // 256, gla_finish, 0)

    def part_copy(b):
        at = pl.ds(pl.multiple_of(b * 256, 256), 256)
        return m.copy(psend.at[b], other_out.at[:, at], part_send.at[b], part_recv.at[b], me, 1 - tp)

    def project(p, yy, core):
        weight = jnp.concatenate([wo[p, yy, 0], wo[p, yy, 1]], axis=1)
        left = act[pl.ds(pl.multiple_of(core * half, half), half), :]
        return dot(left, weight, ((1,), (0,))).astype(jnp.bfloat16)

    def out_pieces(j):
        p = m.piece(j)

        def theirs(yy, carry):
            psend[p * 2 + yy] = project(p, yy, 1 - tp)
            return carry

        def ours(yy, carry):
            part_copy(p * 2 + yy).start()
            own_out[:, pl.ds(pl.multiple_of((p * 2 + yy) * 256, 256), 256)] = project(p, yy, tp)
            return carry

        arrived(pairs[2] + pairs[3], p)
        lax.fori_loop(0, 2, theirs, 0)
        lax.fori_loop(0, 2, ours, 0)

    def rows_of(core):
        return pl.ds(pl.multiple_of(core * half, half), half)

    def last_part(yy, low, high):
        p = m.piece(3)
        weight = jnp.concatenate([wo[p, yy, 0, low:high, :], wo[p, yy, 1, low:high, :]], axis=1)
        return lambda core: dot(act[rows_of(core), low:high], weight, ((1,), (0,)))

    def last_begin():
        def body(yy, carry):
            part = last_part(yy, 0, 2 * early)
            at = pl.ds(pl.multiple_of(yy * 256, 256), 256)
            acc2[0:half, at] = part(1 - tp)
            acc2[half:, at] = part(tp)
            return carry

        arrived(pairs[2], m.piece(3))
        lax.fori_loop(0, 2, body, 0)

    def last_end():
        b = m.piece(3) * 2

        def theirs(yy, carry):
            at = pl.ds(pl.multiple_of(yy * 256, 256), 256)
            part = last_part(yy, 2 * early, 2 * early + 2 * late)
            psend[b + yy] = (acc2[0:half, at] + part(1 - tp)).astype(jnp.bfloat16)
            return carry

        def ours(yy, carry):
            part_copy(b + yy).start()
            at = pl.ds(pl.multiple_of(yy * 256, 256), 256)
            part = last_part(yy, 2 * early, 2 * early + 2 * late)
            own_out[:, pl.ds(pl.multiple_of((b + yy) * 256, 256), 256)] = (acc2[half:, at] + part(tp)).astype(jnp.bfloat16)
            return carry

        arrived(pairs[3], m.piece(3))
        lax.fori_loop(0, 2, theirs, 0)
        lax.fori_loop(0, 2, ours, 0)

    def drain_early():
        swap.wait_send()
        stats.wait_send()

        @pl.when(me < 15)
        def _():
            halo.wait_send()

        for end in near_ends:
            end.wait_send()
        for k in (1, 2, 3):
            @pl.when(z + k <= 3)
            def _():
                far_end(k).wait_send()

        for p in range(4):
            for f in (b1, b2):
                f.first_copy(p).wait_send()
                f.last_copy(p).wait_send()
            for pair in pairs[:2]:
                for f in pair:
                    f.last_copy(p).wait_send()
        for pair in pairs:
            for f in pair:
                f.first_copy(z).wait_send()
        whole.drain()
        for pair in lines:
            for line in pair:
                line.drain()
        for j in range(3):
            for yy in range(2):
                part_copy(m.piece(j) * 2 + yy).wait()

    out_pieces(0)
    out_pieces(1)
    pass_on(3, 3)
    out_pieces(2)
    last_begin()
    drain_early()
    last_end()

    for p in range(4):
        for pair in pairs[2:]:
            for f in pair:
                f.last_copy(p).wait_send()
    for yy in range(2):
        part_copy(m.piece(3) * 2 + yy).wait()


def fused_layer(
    tokens, norm_gain, w_conv_a, w_conv_gate, conv_weight, conv_gain, w_query, w_key, w_value, w_outgate,
    w_decay, decay_bias, decay_extra, head_gain, init_state, w_out_conv, w_out_gla,
):
    rows, width = tokens.shape
    depth = w_query.shape[0]
    n_key = w_query.shape[1]
    n_conv = w_conv_a.shape[1]
    cols = w_out_conv.shape[1]
    half = rows // 2
    pad = 32
    bf16, f32 = jnp.bfloat16, jnp.float32
    dma = pltpu.SemaphoreType.DMA
    vm = pl.BlockSpec(memory_space=pltpu.VMEM)
    hbm = pl.BlockSpec(memory_space=pl.ANY)
    share = pltpu.VMEM((half, 2 * width), bf16)
    own, other = pl.pallas_call(
        layer_kernel,
        out_shape=[share, share],
        in_specs=[hbm, vm, hbm, hbm, vm, vm, hbm, hbm, hbm, hbm, hbm, vm, hbm, vm, vm, hbm, hbm],
        out_specs=[vm, vm],
        scratch_shapes=[
            pltpu.VMEM((4, 2, 2, depth, 5 * n_key), bf16),
            pltpu.VMEM((4, 2, 2, depth, 2 * n_conv), bf16),
            pltpu.VMEM((4, 2, 2, depth, n_conv), bf16),
            pltpu.VMEM((4, 2, 2, 2 * n_conv, cols), bf16),
            pltpu.VMEM((2, rows, width), bf16),
            pltpu.VMEM((rows, 2 * width), bf16),
            pltpu.VMEM((rows, 5 * n_key), f32),
            pltpu.VMEM((rows, 2 * n_conv), f32),
            pltpu.VMEM((rows, n_conv), f32),
            pltpu.VMEM((rows, n_key), f32),
            pltpu.VMEM((n_conv // 128, rows + pad, 128), f32),
            pltpu.VMEM((rows, n_conv), f32),
            pltpu.VMEM((rows, n_key), bf16),
            pltpu.VMEM((rows, 2 * n_conv), bf16),
            pltpu.VMEM((8, half, 256), bf16),
            pltpu.VMEM((pad, n_conv), bf16),
            pltpu.VMEM((pad, n_conv), bf16),
            pltpu.VMEM((rows, 128), f32),
            pltpu.VMEM((rows, 128), f32),
            pltpu.VMEM((8, HV + 16, n_key), bf16),
            pltpu.VMEM((HV, n_key), f32),
            pltpu.VMEM((1, n_key), f32),
            pltpu.VMEM((HV + 8, n_key), f32),
            dma((11,)), dma((10, 4)), dma((10, 4)), dma((10, 4)), dma((10, 4)), dma((9, 4)), dma((9, 4)), dma((9, 4)),
            dma((3,)), dma((3,)), dma((6,)), dma((8,)), dma((8,)), dma((8,)),
        ],
        compiler_params=pltpu.CompilerParams(collective_id=0, has_side_effects=True, vmem_limit_bytes=56 * 2**20),
        name="layer",
    )(
        tokens, norm_gain[None, :], w_conv_a, w_conv_gate, conv_weight, conv_gain[None, :], w_query, w_key, w_value,
        w_outgate, w_decay, decay_bias[None, :], decay_extra, head_gain[None, :], init_state, w_out_conv, w_out_gla,
    )
    return (own.astype(f32) + other.astype(f32)).astype(bf16)


def local_kernel(heads, pieces, q_ref, k_ref, v_ref, pre_ref, extra_ref, bias_ref, attn_ref, since_ref, end_ref, log_ref, state, prefix):
    step = pl.program_id(0)

    @pl.when(step == 0)
    def _():
        state[...] = jnp.zeros_like(state)
        prefix[...] = jnp.zeros_like(prefix)

    rows = lax.broadcasted_iota(jnp.int32, (BLOCK, BLOCK), 0)
    columns = lax.broadcasted_iota(jnp.int32, (BLOCK, BLOCK), 1)
    causal = rows >= columns
    lower = causal.astype(jnp.float32)
    for piece in range(pieces):
        at = pl.ds(piece * BLOCK, BLOCK)
        pre = pre_ref[at, :] + bias_ref[...]
        logs = jax.nn.log_sigmoid(pre) / gate_divisor + extra_ref[at, :]
        cum = lax.dot_general(
            lower, logs, (((1,), (0,)), ((), ())), precision=lax.Precision.HIGHEST, preferred_element_type=jnp.float32
        )
        total = cum[BLOCK - 1 :, :]
        middle = cum[BLOCK // 2 - 1 : BLOCK // 2, :]
        query = q_ref[at, :].astype(jnp.float32) * HK ** (-0.5)
        keys = k_ref[at, :].astype(jnp.float32)
        decayed = query * jnp.exp(cum)
        since_ref[at, :] = (decayed * jnp.exp(prefix[...])).astype(jnp.bfloat16)
        decayed = decayed.astype(jnp.bfloat16)
        query = (query * jnp.exp(cum - middle)).astype(jnp.bfloat16)
        inverse = (keys * jnp.exp(middle - cum)).astype(jnp.bfloat16)
        to_end = (keys * jnp.exp(total - cum)).astype(jnp.bfloat16)
        entering = state[...].astype(jnp.bfloat16)
        added = []
        for h in range(heads):
            ks, vs = slice(h * HK, (h + 1) * HK), slice(h * HV, (h + 1) * HV)
            values = v_ref[at, vs]
            scores = jnp.where(causal, dot(query[:, ks], inverse[:, ks], ((1,), (1,))), 0.0)
            attn_ref[at, vs] = dot(scores.astype(jnp.bfloat16), values, ((1,), (0,))) + dot(
                decayed[:, ks], entering[:, ks], ((1,), (1,))
            )
            added.append(dot(values, to_end[:, ks], ((0,), (0,))))
        added = added[0] if heads == 1 else jnp.concatenate(added, axis=1)
        state[...] = state[...] * jnp.exp(total) + added
        prefix[...] = prefix[...] + total
    end_ref[...] = state[...]
    log_ref[...] = prefix[...]


def gla_local(query, keys, values, decay_pre, decay_extra, decay_bias):
    rows, width = query.shape
    heads = width // HK
    pieces = 4
    tile = pieces * BLOCK

    def tiled(array):
        return pl.BlockSpec((tile, array.shape[1]), lambda i: (i, 0))

    def whole(shape):
        return pl.BlockSpec(shape, lambda i: (0, 0))

    return pl.pallas_call(
        functools.partial(local_kernel, heads, pieces),
        grid=(rows // tile,),
        in_specs=[tiled(query), tiled(keys), tiled(values), tiled(decay_pre), tiled(decay_extra), whole((1, width))],
        out_specs=[tiled(values), tiled(query), whole((HV, width)), whole((1, width))],
        out_shape=[
            jax.ShapeDtypeStruct(values.shape, jnp.float32),
            jax.ShapeDtypeStruct(query.shape, jnp.bfloat16),
            jax.ShapeDtypeStruct((HV, width), jnp.float32),
            jax.ShapeDtypeStruct((1, width), jnp.float32),
        ],
        scratch_shapes=[pltpu.VMEM((HV, width), jnp.float32), pltpu.VMEM((1, width), jnp.float32)],
        cost_estimate=pl.CostEstimate(flops=10**10, bytes_accessed=10**7, transcendentals=10**6),
        name="gla_local",
    )(query, keys, values, decay_pre, decay_extra, decay_bias[None, :])


def finish_kernel(heads, size, where_ref, attn_ref, since_ref, gate_ref, ends_ref, init_ref, gain_ref, out_ref, state):
    me = where_ref[0]

    @pl.when(pl.program_id(0) == 0)
    def _():
        state[...] = init_ref[...]

        def one(device, carry):
            at = device
            decay = ends_ref[pl.ds(pl.multiple_of(at * size + HV, 16), 16), :].astype(jnp.float32)[:1]
            end = ends_ref[pl.ds(pl.multiple_of(at * size, 16), HV), :].astype(jnp.float32)
            state[...] = state[...] * decay + end
            return carry

        lax.fori_loop(0, me, one, 0)

    entering = state[...].astype(jnp.bfloat16)
    for h in range(heads):
        ks, vs = slice(h * HK, (h + 1) * HK), slice(h * HV, (h + 1) * HV)
        attn = attn_ref[:, vs] + dot(since_ref[:, ks], entering[:, ks], ((1,), (1,)))
        attn = attn * lax.rsqrt(jnp.mean(attn * attn, axis=-1, keepdims=True) + epsilon) * gain_ref[...]
        gate = gate_ref[:, vs].astype(jnp.float32)
        out_ref[:, vs] = (attn * (gate * jax.nn.sigmoid(gate))).astype(jnp.bfloat16)


def gla_finish(attn, since, out_gate, ends, init_state, head_gain, me):
    rows, width = since.shape
    heads = width // HK
    tile = 256

    def tiled(array):
        return pl.BlockSpec((tile, array.shape[1]), lambda i, w: (i, 0))

    def whole(array):
        return pl.BlockSpec(array.shape, lambda i, w: (0, 0))

    init = init_state.transpose(2, 0, 1).reshape(HV, width)
    gain = head_gain[None, :]
    return pl.pallas_call(
        functools.partial(finish_kernel, heads, HV + 16),
        grid_spec=pltpu.PrefetchScalarGridSpec(
            num_scalar_prefetch=1,
            grid=(rows // tile,),
            in_specs=[tiled(attn), tiled(since), tiled(out_gate), whole(ends), whole(init), whole(gain)],
            out_specs=tiled(attn),
            scratch_shapes=[pltpu.VMEM((HV, width), jnp.float32)],
        ),
        out_shape=jax.ShapeDtypeStruct(attn.shape, jnp.bfloat16),
        cost_estimate=pl.CostEstimate(flops=3 * 10**9, bytes_accessed=10**7, transcendentals=10**6),
        name="gla_finish",
    )(me[None], attn, since, out_gate, ends, init, gain)


def conv_branch(gated, conv_weight, conv_gain):
    taps = conv_weight.shape[0]
    row_count = gated.shape[0]
    count = lax.axis_size("sp")
    earlier = lax.ppermute(gated[row_count - taps + 1 :], "sp", [(i, i + 1) for i in range(count - 1)])
    extended = jnp.concatenate([earlier, gated], axis=0).astype(jnp.float32)
    conv_sum = jnp.zeros(gated.shape, jnp.float32)
    for tap in range(taps):
        conv_sum = conv_sum + conv_weight[tap][None, :] * extended[tap : tap + row_count]
    row_sums, row_squares = lax.psum((jnp.sum(conv_sum, axis=1), jnp.sum(conv_sum * conv_sum, axis=1)), "tp")
    mean_val = (row_sums / D_CONV)[:, None]
    square_mean = (row_squares / D_CONV)[:, None]
    conv_norm = (conv_sum - mean_val) * lax.rsqrt(square_mean - mean_val * mean_val + epsilon) * conv_gain
    return jax.nn.silu(conv_norm).astype(jnp.bfloat16)


def project(hidden, weight):
    return dot(hidden, weight, ((1,), (0,)))


def plain_layer(
    tokens, norm_gain, w_conv_a, w_conv_gate, conv_weight, conv_gain, w_query, w_key, w_value, w_outgate,
    w_decay, decay_bias, decay_extra, head_gain, init_state, w_out_conv, w_out_gla,
):
    me = lax.axis_index("sp")

    def gather(shard):
        return lax.all_gather(shard, "sp", axis=0, tiled=True)

    widened = lax.all_gather(tokens, "tp", axis=1, tiled=True).astype(jnp.float32)
    normed = (
        widened * lax.rsqrt(jnp.mean(widened * widened, axis=-1, keepdims=True) + epsilon) * norm_gain
    ).astype(jnp.bfloat16)
    half = w_query.shape[1]
    conv_a = project(normed, gather(w_conv_a)).astype(jnp.bfloat16)
    conv_gate = project(normed, gather(w_conv_gate)).astype(jnp.bfloat16)
    full_qkd = gather(jnp.concatenate([w_query, w_key, w_decay], axis=1))
    full_v = gather(w_value)
    gated = (conv_a.astype(jnp.float32) * jax.nn.sigmoid(conv_gate.astype(jnp.float32))).astype(jnp.bfloat16)
    conv_out = conv_branch(gated, conv_weight, conv_gain)
    query_keys = project(normed, full_qkd[:, : 2 * half]).astype(jnp.bfloat16)
    decay_pre = project(normed, full_qkd[:, 2 * half :])
    values = project(normed, full_v).astype(jnp.bfloat16)
    attn, since, end, end_log = gla_local(
        query_keys[:, :half], query_keys[:, half:], values, decay_pre, decay_extra, decay_bias
    )
    packed = jnp.concatenate([end, jnp.broadcast_to(jnp.exp(end_log), (16, half))], axis=0).astype(jnp.bfloat16)
    ends = gather(packed)
    out_gate = project(normed, gather(w_outgate)).astype(jnp.bfloat16)
    gla_out = gla_finish(attn, since, out_gate, ends, init_state, head_gain, me)
    total = dot(conv_out, gather(w_out_conv.T), ((1,), (1,))) + dot(gla_out, gather(w_out_gla.T), ((1,), (1,)))
    return lax.psum_scatter(total.astype(jnp.bfloat16), "tp", scatter_dimension=0, tiled=True)


def per_device(*arrays):
    if folded(lax.axis_size("sp"), lax.axis_size("tp")):
        return fused_layer(*arrays)
    return plain_layer(*arrays)


def solution(mesh):
    placed = (
        P("sp", "tp"), P(), P("sp", "tp"), P("sp", "tp"), P(None, "tp"), P("tp"), P("sp", "tp"), P("sp", "tp"),
        P("sp", "tp"), P("sp", "tp"), P("sp", "tp"), P("tp"), P("sp", "tp"), P(), P("tp", None, None),
        P("tp", "sp"), P("tp", "sp"),
    )
    return jax.shard_map(
        per_device, mesh=mesh, in_specs=placed, out_specs=P(("sp", "tp"), None), check_vma=False
    )
```

```python
import functools

import jax
import jax.numpy as jnp
from jax import lax
from jax.experimental import pallas as pl
from jax.experimental.pallas import tpu as pltpu
from jax.sharding import PartitionSpec as P

D_CONV = 1024
HK = 64
HV = 128
BLOCK = 64

epsilon = 1e-06
gate_divisor = 16.0

MESH = pl.DeviceIdType.MESH


def dot(a, b, dims):
    return lax.dot_general(a, b, (dims, ((), ())), preferred_element_type=jnp.float32)


def folded(n_sp, n_tp):
    return n_sp == 16 and n_tp == 2


class Mover:
    def __init__(self):
        self.me = lax.axis_index("sp")
        self.tp = lax.axis_index("tp")
        self.z, self.y, self.x = self.me // 4, (self.me // 2) % 2, self.me % 2
        self.other = {"x": self.me + 1 - 2 * self.x, "y": self.me + 2 - 4 * self.y}
        self.across = self.me + 3 - 2 * self.x - 4 * self.y
        self.sent = []

    def copy(self, source, target, send, recv, place, core=None):
        core = self.tp if core is None else core
        return pltpu.make_async_remote_copy(
            src_ref=source, dst_ref=target, send_sem=send, recv_sem=recv, device_id=(place, core), device_id_type=MESH
        )

    def piece(self, j):
        z = self.z
        return (z, z + 1 - 2 * (z % 2), 2 - z // 2, 3 - 3 * (z // 2))[j]


class Flow:
    def __init__(self, mover, number, view, first, sems):
        self.m, self.number, self.view, self.first = mover, number, view, first
        self.last = {"x": "y", "y": "x"}[first]
        self.sems = sems

    def own(self, p):
        return self.view(p, self.m.y, self.m.x)

    def pair(self, p):
        every = slice(None)
        return self.view(p, self.m.y, every) if self.first == "x" else self.view(p, every, self.m.x)

    def first_copy(self, p, source=None):
        own = self.own(p) if source is None else source
        slot = self.number * 4 + p if self.number < 2 else self.number + 6
        fs, fr = self.sems["first_send"], self.sems["first_recv"]
        return self.m.copy(own, own, fs.at[self.number], fr.at[slot], self.m.other[self.first])

    def last_copy(self, p, source=None):
        pair = self.pair(p) if source is None else source
        ls, lr = self.sems["last_send"], self.sems["last_recv"]
        return self.m.copy(pair, pair, ls.at[self.number], lr.at[self.number // 2, p], self.m.other[self.last])

    def drain_first(self):
        if self.number < 2:
            self.first_copy(0, self.own(slice(None))).wait_send()
        else:
            self.first_copy(self.m.z).wait_send()

    def drain_last(self):
        self.last_copy(0, self.pair(slice(None))).wait_send()


class Line:
    def __init__(self, mover, number, view, sems):
        self.m, self.number, self.view, self.sems = mover, number, view, sems

    def up(self, p):
        return self.m.copy(
            self.view(p), self.view(p), self.sems["z_send"].at[self.number, p], self.sems["z_recv"].at[self.number, p],
            self.m.me + 4,
        )

    def down(self, p):
        return self.m.copy(
            self.view(p), self.view(p), self.sems["z_send"].at[self.number, p + 1],
            self.sems["z_recv"].at[self.number, p], self.m.me - 4,
        )

    def start_own(self):
        z = self.m.z

        @pl.when(z < 3)
        def _():
            self.up(z).start()

        @pl.when(z > 0)
        def _():
            self.down(z).start()

    def relay(self, step, then):
        z = self.m.z

        @pl.when(z >= step)
        def _():
            p = z - step
            self.up(p).wait_recv()

            @pl.when(z < 3)
            def _():
                self.up(p).start()

            then(p)

        @pl.when(z + step <= 3)
        def _():
            p = z + step
            self.down(p).wait_recv()

            @pl.when(z > 0)
            def _():
                self.down(p).start()

            then(p)

    def drain(self):
        z = self.m.z
        for p in range(4):
            @pl.when((p <= z) & (z < 3))
            def _():
                self.up(p).wait_send()

            @pl.when((p >= z) & (z > 0))
            def _():
                self.down(p).wait_send()


def at_step(z, step, then):
    if step == 0:
        then(z)
        return

    @pl.when(z >= step)
    def _():
        then(z - step)

    @pl.when(z + step <= 3)
    def _():
        then(z + step)


def layer_kernel(
    tokens, gain, wa, wg, taps, conv_gain, wq, wk, wv, wog, wd, bias, extra_in, head_gain, init, woc, wogl, own_out, other_out,
    w1, w2, w3, wo, both, normed, acc1, acc2, acc3, extra, seq, attn, since, act, psend,
    halo_out, halo_in, stat_own, stat_in, packs, state, prefix, before,
    local, first_send, first_recv, last_send, last_recv, z_send, z_recv, misc_send, misc_recv, end_send, end_recv,
    part_send, part_recv,
):
    m = Mover()
    me, tp, z, y, x = m.me, m.tp, m.z, m.y, m.x
    rows = normed.shape[0]
    half = rows // 2
    width = both.shape[2]
    n_key = acc1.shape[1] // 5
    n_conv = 2 * n_key
    heads = n_key // HK
    sems = dict(
        first_send=first_send, first_recv=first_recv, last_send=last_send, last_recv=last_recv,
        z_send=z_send, z_recv=z_recv,
    )

    def lanes(ref, low, size):
        return lambda p, yy, xx: ref.at[p, yy, xx, :, pl.ds(low, size)]

    def depth(low, size):
        return lambda p, yy, xx: wo.at[p, yy, xx, pl.ds(low, size), :]

    mid = w1.shape[-1] // 2
    late = wo.shape[3] // 8
    early = wo.shape[3] // 2 - late
    b1 = Flow(m, 0, lanes(w1, 0, mid), "x", sems)
    b2 = Flow(m, 1, lanes(w1, mid, mid), "y", sems)
    pairs = [
        (Flow(m, 2, lanes(w2, 0, n_conv), "x", sems), Flow(m, 3, lanes(w2, n_conv, n_conv), "y", sems)),
        (Flow(m, 4, lanes(w3, 0, n_key), "x", sems), Flow(m, 5, lanes(w3, n_key, n_key), "y", sems)),
        (Flow(m, 6, depth(0, early), "x", sems), Flow(m, 7, depth(early, early), "y", sems)),
        (Flow(m, 8, depth(2 * early, late), "x", sems), Flow(m, 9, depth(2 * early + late, late), "y", sems)),
    ]
    whole = Line(m, 0, lambda p: w1.at[p, y, x], sems)
    lines = [tuple(Line(m, f.number - 1, f.pair, sems) for f in pair) for pair in pairs]

    loads = [
        (wq, w1.at[z, y, x, :, pl.ds(0, n_key)]),
        (wk, w1.at[z, y, x, :, pl.ds(n_key, n_key)]),
        (wd, w1.at[z, y, x, :, pl.ds(2 * n_key, n_key)]),
        (wv, w1.at[z, y, x, :, pl.ds(3 * n_key, n_conv)]),
        (wa, w2.at[z, y, x, :, pl.ds(0, n_conv)]),
        (wg, w2.at[z, y, x, :, pl.ds(n_conv, n_conv)]),
        (wog, w3.at[z, y, x]),
        (woc, wo.at[z, y, x, pl.ds(0, n_conv), :]),
        (wogl, wo.at[z, y, x, pl.ds(n_conv, n_conv), :]),
        (tokens, both.at[tp]),
        (extra_in, extra),
    ]
    loads = [pltpu.make_async_copy(a, b, local.at[i]) for i, (a, b) in enumerate(loads)]
    for load in loads:
        load.start()

    barrier = pltpu.get_barrier_semaphore()
    partners = [(m.other["x"], tp), (m.other["y"], tp), (m.across, tp), (me, 1 - tp)]
    partners += [((me + k) % 16, tp) for k in (4, 8, 12, 1, 15)]
    for place, core in partners:
        pl.semaphore_signal(barrier, inc=1, device_id=(place, core), device_id_type=MESH)
    pl.semaphore_wait(barrier, len(partners))

    for i in range(4):
        loads[i].wait()
    whole.start_own()
    b1.first_copy(z).start()
    b2.first_copy(z).start()
    loads[9].wait()
    swap = m.copy(both.at[tp], both.at[tp], misc_send.at[0], misc_recv.at[0], me, 1 - tp)
    swap.start()
    loads[4].wait()
    loads[5].wait()
    for f in pairs[0]:
        f.first_copy(z).start()
    loads[6].wait()
    for f in pairs[1]:
        f.first_copy(z).start()
    for i in (7, 8, 10):
        loads[i].wait()

    def head_firsts(step):
        def one(p):
            b1.first_copy(p).wait_recv()
            b1.last_copy(p).start()
            b2.first_copy(p).wait_recv()
            b2.last_copy(p).start()

        at_step(z, step, one)

    def head_line(step):
        def then(p):
            b1.first_copy(p).start()
            b2.first_copy(p).start()

        whole.relay(step, then)

    def begin(k):
        for f in pairs[k]:
            f.first_copy(z).start()

    def enter_one(k, i):
        pairs[k][i].first_copy(z).wait_recv()
        lines[k][i].start_own()

    def enter(k):
        enter_one(k, 0)
        enter_one(k, 1)

    def own_last(k):
        for f in pairs[k]:
            f.last_copy(z).start()

    def pass_on(k, step):
        for f, line in zip(pairs[k], lines[k]):
            line.relay(step, lambda p: f.last_copy(p).start())

    def relay_only(k, step):
        for line in lines[k]:
            line.relay(step, lambda p: None)

    def finish(k, step):
        for f in pairs[k]:
            at_step(z, step, lambda p: f.last_copy(p).start())

    def arrived(k, p):
        every = (p, slice(None), slice(None))
        both_flows = (
            w1.at[(*every, slice(None), pl.ds(0, mid))],
            w2.at[(*every, slice(None), pl.ds(0, n_conv))],
            w3.at[(*every, slice(None), pl.ds(0, n_key))],
            wo.at[(*every, pl.ds(0, early), slice(None))],
            wo.at[(*every, pl.ds(0, late), slice(None))],
        )[k]
        flow = b1 if k == 0 else pairs[k - 1][0]
        flow.last_copy(p, both_flows).wait_recv()

    def norm_tiles(low, high):
        def body(i, carry):
            at = pl.ds(pl.multiple_of(i * 128, 128), 128)
            a = both[0, at, :].astype(jnp.float32)
            b = both[1, at, :].astype(jnp.float32)
            square = jnp.sum(a * a + b * b, axis=1, keepdims=True)
            scale = lax.rsqrt(square / (2 * width) + epsilon)
            normed[at, :width] = (a * scale * gain[:, :width]).astype(jnp.bfloat16)
            normed[at, width:] = (b * scale * gain[:, width:]).astype(jnp.bfloat16)
            return carry

        lax.fori_loop(low, high, body, 0)

    def slab(acc, ref, p, first):
        size = ref.shape[1] * ref.shape[2] * ref.shape[3]

        def body(c, carry):
            at = pl.ds(pl.multiple_of(c * 256, 256), 256)
            left = normed[:, pl.ds(pl.multiple_of(p * size, size), size)]
            right = ref[p, :, :, :, at].reshape(size, 256)
            got = dot(left, right, ((1,), (0,)))
            if first:
                acc[:, at] = got
            else:
                acc[:, at] += got
            return carry

        lax.fori_loop(0, acc.shape[1] // 256, body, 0)

    swap.wait_recv()
    norm_tiles(0, 4)
    head_line(1)
    head_firsts(0)
    norm_tiles(4, 8)
    enter_one(0, 0)
    head_line(2)
    enter_one(0, 1)
    head_firsts(1)
    head_line(3)
    arrived(0, m.piece(0))
    slab(acc1, w1, m.piece(0), True)
    head_firsts(2)
    begin(2)
    begin(3)
    pass_on(0, 1)
    arrived(0, m.piece(1))
    slab(acc1, w1, m.piece(1), False)
    head_firsts(3)
    enter(1)
    own_last(0)
    pass_on(0, 2)
    arrived(0, m.piece(2))
    slab(acc1, w1, m.piece(2), False)
    pass_on(1, 1)
    enter(2)
    arrived(0, m.piece(3))
    slab(acc1, w1, m.piece(3), False)

    state[...] = jnp.zeros_like(state)
    prefix[...] = jnp.zeros_like(prefix)
    r_iota = lax.broadcasted_iota(jnp.int32, (BLOCK, BLOCK), 0)
    c_iota = lax.broadcasted_iota(jnp.int32, (BLOCK, BLOCK), 1)
    causal = r_iota >= c_iota
    lower = causal.astype(jnp.float32)

    def block(i, carry):
        at = pl.ds(pl.multiple_of(i * BLOCK, BLOCK), BLOCK)
        pre = acc1[at, 2 * n_key : 3 * n_key] + bias[...]
        logs = jax.nn.log_sigmoid(pre) / gate_divisor + extra[at, :]
        cum = lax.dot_general(
            lower, logs, (((1,), (0,)), ((), ())), precision=lax.Precision.HIGHEST, preferred_element_type=jnp.float32
        )
        total = cum[BLOCK - 1 :, :]
        middle = cum[BLOCK // 2 - 1 : BLOCK // 2, :]
        query = acc1[at, 0:n_key].astype(jnp.bfloat16).astype(jnp.float32) * HK ** (-0.5)
        keys = acc1[at, n_key : 2 * n_key].astype(jnp.bfloat16).astype(jnp.float32)
        decayed = query * jnp.exp(cum)
        since[at, :] = (decayed * jnp.exp(prefix[...])).astype(jnp.bfloat16)
        decayed = decayed.astype(jnp.bfloat16)
        query = (query * jnp.exp(cum - middle)).astype(jnp.bfloat16)
        inverse = (keys * jnp.exp(middle - cum)).astype(jnp.bfloat16)
        to_end = (keys * jnp.exp(total - cum)).astype(jnp.bfloat16)
        entering = state[...].astype(jnp.bfloat16)
        added = []
        for h in range(heads):
            ks, vs = slice(h * HK, (h + 1) * HK), slice(h * HV, (h + 1) * HV)
            values = acc1[at, 3 * n_key + h * HV : 3 * n_key + (h + 1) * HV].astype(jnp.bfloat16)
            scores = jnp.where(causal, dot(query[:, ks], inverse[:, ks], ((1,), (1,))), 0.0)
            attn[at, vs] = dot(scores.astype(jnp.bfloat16), values, ((1,), (0,))) + dot(
                decayed[:, ks], entering[:, ks], ((1,), (1,))
            )
            added.append(dot(values, to_end[:, ks], ((0,), (0,))))
        state[...] = state[...] * jnp.exp(total) + jnp.concatenate(added, axis=1)
        prefix[...] = prefix[...] + total
        return carry

    blocks = rows // BLOCK

    def attend(i, carry):
        block(i, 0)

        @pl.when(i == blocks // 2)
        def _():
            pass_on(0, 3)

        @pl.when(i == blocks - 3)
        def _():
            relay_only(1, 2)

        return carry

    lax.fori_loop(0, blocks, attend, 0)

    def pack(slot, decay, end):
        packs[slot, 0:HV, :] = end.astype(jnp.bfloat16)
        packs[slot, HV:, :] = jnp.broadcast_to(decay, (16, n_key)).astype(jnp.bfloat16)

    def read(slot):
        return packs[slot, HV : HV + 1, :].astype(jnp.float32), packs[slot, 0:HV, :].astype(jnp.float32)

    def end_copy(source, target, number, place):
        return m.copy(packs.at[source], packs.at[target], end_send.at[number], end_recv.at[target], place)

    def join(early, late):
        return early[0] * late[0], early[1] * late[0] + late[1]

    near_ends = [
        end_copy(0, 1, 0, m.other["x"]),
        end_copy(0, 2, 1, m.other["y"]),
        end_copy(0, 3, 2, m.across),
    ]
    pack(0, jnp.exp(prefix[...]), state[...])

    arrived(1, m.piece(0))
    slab(acc2, w2, m.piece(0), True)
    for end in near_ends:
        end.start()
    own_last(1)
    finish(1, 2)
    pass_on(2, 1)
    enter(3)
    arrived(1, m.piece(1))
    slab(acc2, w2, m.piece(1), False)
    arrived(1, m.piece(2))
    slab(acc2, w2, m.piece(2), False)
    arrived(1, m.piece(3))
    slab(acc2, w2, m.piece(3), False)
    pass_on(1, 3)
    own_last(2)

    def join_near():
        for end in near_ends:
            end.wait_recv()
        run = (jnp.ones((1, n_key), jnp.float32), jnp.zeros((HV, n_key), jnp.float32))
        pre = run
        for yy in range(2):
            for xx in range(2):
                past = yy * 2 + xx < y * 2 + x
                run = join(run, read((y + yy - 2 * y * yy) * 2 + x + xx - 2 * x * xx))
                pre = jnp.where(past, run[0], pre[0]), jnp.where(past, run[1], pre[1])
        before[0:HV, :] = pre[1]
        before[HV:, :] = jnp.broadcast_to(pre[0], (8, n_key))
        pack(4, *run)

    def far_end(k):
        return end_copy(4, 4 + k, 2 + k, me + 4 * k)

    pad = seq.shape[1] - rows

    def gate_tiles(low, high):
        def body(i, carry):
            at = pl.ds(pl.multiple_of(i * 128, 128), 128)
            for c in range(n_conv // 128):
                a = acc2[at, c * 128 : (c + 1) * 128].astype(jnp.bfloat16).astype(jnp.float32)
                g = acc2[at, n_conv + c * 128 : n_conv + (c + 1) * 128].astype(jnp.bfloat16).astype(jnp.float32)
                value = (a * jax.nn.sigmoid(g)).astype(jnp.bfloat16)
                seq[c, pl.ds(pl.multiple_of(i * 128 + pad, 32), 128), :] = value.astype(jnp.float32)
            return carry

        lax.fori_loop(low, high, body, 0)

    gate_tiles(rows // 128 - 1, rows // 128)
    for c in range(n_conv // 128):
        halo_out[:, c * 128 : (c + 1) * 128] = seq[c, rows : rows + pad, :].astype(jnp.bfloat16)
    gate_tiles(0, rows // 128 - 1)
    halo = m.copy(halo_out, halo_in, misc_send.at[1], misc_recv.at[1], me + 1)

    @pl.when(me < 15)
    def _():
        halo.start()

    n_taps = taps.shape[0]
    shift = pad - (n_taps - 1)

    def conv_chunk(i):
        base = pl.multiple_of(i * 128, 128)
        sums = jnp.zeros((128, 128), jnp.float32)
        squares = jnp.zeros((128, 128), jnp.float32)
        for c in range(n_conv // 128):
            part = seq[c, pl.ds(base, 128 + pad), :]
            total = jnp.zeros((128, 128), jnp.float32)
            for turn in range(8):
                moved = part if turn == 0 else pltpu.roll(part, 128 + pad - turn, 0)
                for tap in range(n_taps):
                    if (shift + tap) % 8 == turn:
                        start = shift + tap - turn
                        total = total + taps[tap : tap + 1, c * 128 : (c + 1) * 128] * moved[start : start + 128]
            acc2[pl.ds(base, 128), c * 128 : (c + 1) * 128] = total
            sums = sums + total
            squares = squares + total * total
        first = jnp.sum(sums, axis=1, keepdims=True)
        second = jnp.sum(squares, axis=1, keepdims=True)
        lane = lax.broadcasted_iota(jnp.int32, (128, 128), 1)
        stat_own[pl.ds(base, 128), :] = jnp.where(lane == 0, first, second)

    chunks = rows // 128

    def conv_loop(i, carry):
        conv_chunk(i)

        @pl.when(i == chunks // 2)
        def _():
            pass_on(2, 2)

        @pl.when(i == chunks - 3)
        def _():
            join_near()

        @pl.when(i == chunks - 1)
        def _():
            for k in (1, 2, 3):
                @pl.when(z + k <= 3)
                def _():
                    far_end(k).start()

        return carry

    lax.fori_loop(1, chunks, conv_loop, 0)

    @pl.when(me > 0)
    def _():
        halo.wait_recv()
        for c in range(n_conv // 128):
            seq[c, 0:pad, :] = halo_in[:, c * 128 : (c + 1) * 128].astype(jnp.float32)

    @pl.when(me == 0)
    def _():
        seq[:, 0:pad, :] = jnp.zeros((n_conv // 128, pad, 128), jnp.float32)

    lax.fori_loop(0, 1, conv_loop, 0)

    pass_on(3, 1)
    own_last(3)
    arrived(2, m.piece(0))
    slab(acc3, w3, m.piece(0), True)
    stats = m.copy(stat_own, stat_in, misc_send.at[2], misc_recv.at[2], me, 1 - tp)
    stats.start()
    arrived(2, m.piece(1))
    slab(acc3, w3, m.piece(1), False)
    arrived(2, m.piece(2))
    slab(acc3, w3, m.piece(2), False)
    arrived(2, m.piece(3))
    slab(acc3, w3, m.piece(3), False)
    pass_on(2, 3)
    stats.wait_recv()

    def conv_finish(i, carry):
        at = pl.ds(pl.multiple_of(i * 128, 128), 128)
        both_stats = stat_own[at, :] + stat_in[at, :]
        mean_val = both_stats[:, 0:1] / (2 * n_conv)
        square_mean = both_stats[:, 1:2] / (2 * n_conv)
        scale = lax.rsqrt(square_mean - mean_val * mean_val + epsilon)
        value = (acc2[at, 0:n_conv] - mean_val) * scale * conv_gain[...]
        act[at, 0:n_conv] = (value * jax.nn.sigmoid(value)).astype(jnp.bfloat16)
        return carry

    lax.fori_loop(0, chunks, conv_finish, 0)
    pass_on(3, 2)
    for k in (1, 2, 3):
        @pl.when(z - k >= 0)
        def _():
            end_copy(4, 4 + k, 2 + k, me).wait_recv()
            pre = join(read(4 + k), (before[HV : HV + 1, :], before[0:HV, :]))
            before[0:HV, :] = pre[1]
            before[HV:, :] = jnp.broadcast_to(pre[0], (8, n_key))

    entry = jnp.concatenate([init[h].T for h in range(heads)], axis=1)
    state[...] = entry * before[HV : HV + 1, :] + before[0:HV, :]

    def gla_finish(i, carry):
        at = pl.ds(pl.multiple_of(i * 256, 256), 256)
        entering = state[...].astype(jnp.bfloat16)
        for h in range(heads):
            ks, vs = slice(h * HK, (h + 1) * HK), slice(h * HV, (h + 1) * HV)
            value = attn[at, vs] + dot(since[at, ks], entering[:, ks], ((1,), (1,)))
            value = value * lax.rsqrt(jnp.mean(value * value, axis=-1, keepdims=True) + epsilon) * head_gain[...]
            gate = acc3[at, vs].astype(jnp.bfloat16).astype(jnp.float32)
            act[at, n_conv + h * HV : n_conv + (h + 1) * HV] = (value * (gate * jax.nn.sigmoid(gate))).astype(jnp.bfloat16)
        return carry

    lax.fori_loop(0, rows // 256, gla_finish, 0)

    def part_copy(b):
        at = pl.ds(pl.multiple_of(b * 256, 256), 256)
        return m.copy(psend.at[b], other_out.at[:, at], part_send, part_recv, me, 1 - tp)

    def project(p, yy, core):
        weight = jnp.concatenate([wo[p, yy, 0], wo[p, yy, 1]], axis=1)
        left = act[pl.ds(pl.multiple_of(core * half, half), half), :]
        return dot(left, weight, ((1,), (0,))).astype(jnp.bfloat16)

    def out_pieces(j):
        p = m.piece(j)

        def theirs(yy, carry):
            psend[p * 2 + yy] = project(p, yy, 1 - tp)
            return carry

        def ours(yy, carry):
            part_copy(p * 2 + yy).start()
            own_out[:, pl.ds(pl.multiple_of((p * 2 + yy) * 256, 256), 256)] = project(p, yy, tp)
            return carry

        arrived(3, p)
        arrived(4, p)
        lax.fori_loop(0, 2, theirs, 0)
        lax.fori_loop(0, 2, ours, 0)

    def rows_of(core):
        return pl.ds(pl.multiple_of(core * half, half), half)

    def last_part(yy, low, high):
        p = m.piece(3)
        weight = jnp.concatenate([wo[p, yy, 0, low:high, :], wo[p, yy, 1, low:high, :]], axis=1)
        return lambda core: dot(act[rows_of(core), low:high], weight, ((1,), (0,)))

    def last_begin():
        def body(yy, carry):
            part = last_part(yy, 0, 2 * early)
            at = pl.ds(pl.multiple_of(yy * 256, 256), 256)
            acc2[0:half, at] = part(1 - tp)
            acc2[half:, at] = part(tp)
            return carry

        arrived(3, m.piece(3))
        lax.fori_loop(0, 2, body, 0)

    def last_end():
        b = m.piece(3) * 2

        def theirs(yy, carry):
            at = pl.ds(pl.multiple_of(yy * 256, 256), 256)
            part = last_part(yy, 2 * early, 2 * early + 2 * late)
            psend[b + yy] = (acc2[0:half, at] + part(1 - tp)).astype(jnp.bfloat16)
            return carry

        def ours(yy, carry):
            part_copy(b + yy).start()
            at = pl.ds(pl.multiple_of(yy * 256, 256), 256)
            part = last_part(yy, 2 * early, 2 * early + 2 * late)
            own_out[:, pl.ds(pl.multiple_of((b + yy) * 256, 256), 256)] = (acc2[half:, at] + part(tp)).astype(jnp.bfloat16)
            return carry

        arrived(4, m.piece(3))
        lax.fori_loop(0, 2, theirs, 0)
        lax.fori_loop(0, 2, ours, 0)

    def drain_early():
        swap.wait_send()
        stats.wait_send()

        @pl.when(me < 15)
        def _():
            halo.wait_send()

        for end in near_ends:
            end.wait_send()
        for k in (1, 2, 3):
            @pl.when(z + k <= 3)
            def _():
                far_end(k).wait_send()

        for f in (b1, b2, *pairs[0], *pairs[1]):
            f.drain_first()
            f.drain_last()
        for f in (*pairs[2], *pairs[3]):
            f.drain_first()
        whole.drain()
        for pair in lines:
            for line in pair:
                line.drain()

    out_pieces(0)
    pass_on(3, 3)
    out_pieces(1)
    out_pieces(2)
    last_begin()
    drain_early()
    last_end()

    for f in (*pairs[2], *pairs[3]):
        f.drain_last()
    m.copy(psend, psend, part_send, part_recv, me, 1 - tp).wait_send()
    m.copy(other_out, other_out, part_send, part_recv, me, 1 - tp).wait_recv()


def fused_layer(
    tokens, norm_gain, w_conv_a, w_conv_gate, conv_weight, conv_gain, w_query, w_key, w_value, w_outgate,
    w_decay, decay_bias, decay_extra, head_gain, init_state, w_out_conv, w_out_gla,
):
    rows, width = tokens.shape
    depth = w_query.shape[0]
    n_key = w_query.shape[1]
    n_conv = w_conv_a.shape[1]
    cols = w_out_conv.shape[1]
    half = rows // 2
    pad = 32
    bf16, f32 = jnp.bfloat16, jnp.float32
    dma = pltpu.SemaphoreType.DMA
    vm = pl.BlockSpec(memory_space=pltpu.VMEM)
    hbm = pl.BlockSpec(memory_space=pl.ANY)
    share = pltpu.VMEM((half, 2 * width), bf16)
    own, other = pl.pallas_call(
        layer_kernel,
        out_shape=[share, share],
        in_specs=[hbm, vm, hbm, hbm, vm, vm, hbm, hbm, hbm, hbm, hbm, vm, hbm, vm, vm, hbm, hbm],
        out_specs=[vm, vm],
        scratch_shapes=[
            pltpu.VMEM((4, 2, 2, depth, 5 * n_key), bf16),
            pltpu.VMEM((4, 2, 2, depth, 2 * n_conv), bf16),
            pltpu.VMEM((4, 2, 2, depth, n_conv), bf16),
            pltpu.VMEM((4, 2, 2, 2 * n_conv, cols), bf16),
            pltpu.VMEM((2, rows, width), bf16),
            pltpu.VMEM((rows, 2 * width), bf16),
            pltpu.VMEM((rows, 5 * n_key), f32),
            pltpu.VMEM((rows, 2 * n_conv), f32),
            pltpu.VMEM((rows, n_conv), f32),
            pltpu.VMEM((rows, n_key), f32),
            pltpu.VMEM((n_conv // 128, rows + pad, 128), f32),
            pltpu.VMEM((rows, n_conv), f32),
            pltpu.VMEM((rows, n_key), bf16),
            pltpu.VMEM((rows, 2 * n_conv), bf16),
            pltpu.VMEM((8, half, 256), bf16),
            pltpu.VMEM((pad, n_conv), bf16),
            pltpu.VMEM((pad, n_conv), bf16),
            pltpu.VMEM((rows, 128), f32),
            pltpu.VMEM((rows, 128), f32),
            pltpu.VMEM((8, HV + 16, n_key), bf16),
            pltpu.VMEM((HV, n_key), f32),
            pltpu.VMEM((1, n_key), f32),
            pltpu.VMEM((HV + 8, n_key), f32),
            dma((11,)), dma((10,)), dma((16,)), dma((10,)), dma((5, 4)), dma((9, 5)), dma((9, 4)),
            dma((3,)), dma((3,)), dma((6,)), dma((8,)), dma(()), dma(()),
        ],
        compiler_params=pltpu.CompilerParams(collective_id=0, has_side_effects=True, vmem_limit_bytes=56 * 2**20),
        name="layer",
    )(
        tokens, norm_gain[None, :], w_conv_a, w_conv_gate, conv_weight, conv_gain[None, :], w_query, w_key, w_value,
        w_outgate, w_decay, decay_bias[None, :], decay_extra, head_gain[None, :], init_state, w_out_conv, w_out_gla,
    )
    return (own.astype(f32) + other.astype(f32)).astype(bf16)


def local_kernel(heads, pieces, q_ref, k_ref, v_ref, pre_ref, extra_ref, bias_ref, attn_ref, since_ref, end_ref, log_ref, state, prefix):
    step = pl.program_id(0)

    @pl.when(step == 0)
    def _():
        state[...] = jnp.zeros_like(state)
        prefix[...] = jnp.zeros_like(prefix)

    rows = lax.broadcasted_iota(jnp.int32, (BLOCK, BLOCK), 0)
    columns = lax.broadcasted_iota(jnp.int32, (BLOCK, BLOCK), 1)
    causal = rows >= columns
    lower = causal.astype(jnp.float32)
    for piece in range(pieces):
        at = pl.ds(piece * BLOCK, BLOCK)
        pre = pre_ref[at, :] + bias_ref[...]
        logs = jax.nn.log_sigmoid(pre) / gate_divisor + extra_ref[at, :]
        cum = lax.dot_general(
            lower, logs, (((1,), (0,)), ((), ())), precision=lax.Precision.HIGHEST, preferred_element_type=jnp.float32
        )
        total = cum[BLOCK - 1 :, :]
        middle = cum[BLOCK // 2 - 1 : BLOCK // 2, :]
        query = q_ref[at, :].astype(jnp.float32) * HK ** (-0.5)
        keys = k_ref[at, :].astype(jnp.float32)
        decayed = query * jnp.exp(cum)
        since_ref[at, :] = (decayed * jnp.exp(prefix[...])).astype(jnp.bfloat16)
        decayed = decayed.astype(jnp.bfloat16)
        query = (query * jnp.exp(cum - middle)).astype(jnp.bfloat16)
        inverse = (keys * jnp.exp(middle - cum)).astype(jnp.bfloat16)
        to_end = (keys * jnp.exp(total - cum)).astype(jnp.bfloat16)
        entering = state[...].astype(jnp.bfloat16)
        added = []
        for h in range(heads):
            ks, vs = slice(h * HK, (h + 1) * HK), slice(h * HV, (h + 1) * HV)
            values = v_ref[at, vs]
            scores = jnp.where(causal, dot(query[:, ks], inverse[:, ks], ((1,), (1,))), 0.0)
            attn_ref[at, vs] = dot(scores.astype(jnp.bfloat16), values, ((1,), (0,))) + dot(
                decayed[:, ks], entering[:, ks], ((1,), (1,))
            )
            added.append(dot(values, to_end[:, ks], ((0,), (0,))))
        added = added[0] if heads == 1 else jnp.concatenate(added, axis=1)
        state[...] = state[...] * jnp.exp(total) + added
        prefix[...] = prefix[...] + total
    end_ref[...] = state[...]
    log_ref[...] = prefix[...]


def gla_local(query, keys, values, decay_pre, decay_extra, decay_bias):
    rows, width = query.shape
    heads = width // HK
    pieces = 4
    tile = pieces * BLOCK

    def tiled(array):
        return pl.BlockSpec((tile, array.shape[1]), lambda i: (i, 0))

    def whole(shape):
        return pl.BlockSpec(shape, lambda i: (0, 0))

    return pl.pallas_call(
        functools.partial(local_kernel, heads, pieces),
        grid=(rows // tile,),
        in_specs=[tiled(query), tiled(keys), tiled(values), tiled(decay_pre), tiled(decay_extra), whole((1, width))],
        out_specs=[tiled(values), tiled(query), whole((HV, width)), whole((1, width))],
        out_shape=[
            jax.ShapeDtypeStruct(values.shape, jnp.float32),
            jax.ShapeDtypeStruct(query.shape, jnp.bfloat16),
            jax.ShapeDtypeStruct((HV, width), jnp.float32),
            jax.ShapeDtypeStruct((1, width), jnp.float32),
        ],
        scratch_shapes=[pltpu.VMEM((HV, width), jnp.float32), pltpu.VMEM((1, width), jnp.float32)],
        cost_estimate=pl.CostEstimate(flops=10**10, bytes_accessed=10**7, transcendentals=10**6),
        name="gla_local",
    )(query, keys, values, decay_pre, decay_extra, decay_bias[None, :])


def finish_kernel(heads, size, where_ref, attn_ref, since_ref, gate_ref, ends_ref, init_ref, gain_ref, out_ref, state):
    me = where_ref[0]

    @pl.when(pl.program_id(0) == 0)
    def _():
        state[...] = init_ref[...]

        def one(device, carry):
            at = device
            decay = ends_ref[pl.ds(pl.multiple_of(at * size + HV, 16), 16), :].astype(jnp.float32)[:1]
            end = ends_ref[pl.ds(pl.multiple_of(at * size, 16), HV), :].astype(jnp.float32)
            state[...] = state[...] * decay + end
            return carry

        lax.fori_loop(0, me, one, 0)

    entering = state[...].astype(jnp.bfloat16)
    for h in range(heads):
        ks, vs = slice(h * HK, (h + 1) * HK), slice(h * HV, (h + 1) * HV)
        attn = attn_ref[:, vs] + dot(since_ref[:, ks], entering[:, ks], ((1,), (1,)))
        attn = attn * lax.rsqrt(jnp.mean(attn * attn, axis=-1, keepdims=True) + epsilon) * gain_ref[...]
        gate = gate_ref[:, vs].astype(jnp.float32)
        out_ref[:, vs] = (attn * (gate * jax.nn.sigmoid(gate))).astype(jnp.bfloat16)


def gla_finish(attn, since, out_gate, ends, init_state, head_gain, me):
    rows, width = since.shape
    heads = width // HK
    tile = 256

    def tiled(array):
        return pl.BlockSpec((tile, array.shape[1]), lambda i, w: (i, 0))

    def whole(array):
        return pl.BlockSpec(array.shape, lambda i, w: (0, 0))

    init = init_state.transpose(2, 0, 1).reshape(HV, width)
    gain = head_gain[None, :]
    return pl.pallas_call(
        functools.partial(finish_kernel, heads, HV + 16),
        grid_spec=pltpu.PrefetchScalarGridSpec(
            num_scalar_prefetch=1,
            grid=(rows // tile,),
            in_specs=[tiled(attn), tiled(since), tiled(out_gate), whole(ends), whole(init), whole(gain)],
            out_specs=tiled(attn),
            scratch_shapes=[pltpu.VMEM((HV, width), jnp.float32)],
        ),
        out_shape=jax.ShapeDtypeStruct(attn.shape, jnp.bfloat16),
        cost_estimate=pl.CostEstimate(flops=3 * 10**9, bytes_accessed=10**7, transcendentals=10**6),
        name="gla_finish",
    )(me[None], attn, since, out_gate, ends, init, gain)


def conv_branch(gated, conv_weight, conv_gain):
    taps = conv_weight.shape[0]
    row_count = gated.shape[0]
    count = lax.axis_size("sp")
    earlier = lax.ppermute(gated[row_count - taps + 1 :], "sp", [(i, i + 1) for i in range(count - 1)])
    extended = jnp.concatenate([earlier, gated], axis=0).astype(jnp.float32)
    conv_sum = jnp.zeros(gated.shape, jnp.float32)
    for tap in range(taps):
        conv_sum = conv_sum + conv_weight[tap][None, :] * extended[tap : tap + row_count]
    row_sums, row_squares = lax.psum((jnp.sum(conv_sum, axis=1), jnp.sum(conv_sum * conv_sum, axis=1)), "tp")
    mean_val = (row_sums / D_CONV)[:, None]
    square_mean = (row_squares / D_CONV)[:, None]
    conv_norm = (conv_sum - mean_val) * lax.rsqrt(square_mean - mean_val * mean_val + epsilon) * conv_gain
    return jax.nn.silu(conv_norm).astype(jnp.bfloat16)


def project(hidden, weight):
    return dot(hidden, weight, ((1,), (0,)))


def plain_layer(
    tokens, norm_gain, w_conv_a, w_conv_gate, conv_weight, conv_gain, w_query, w_key, w_value, w_outgate,
    w_decay, decay_bias, decay_extra, head_gain, init_state, w_out_conv, w_out_gla,
):
    me = lax.axis_index("sp")

    def gather(shard):
        return lax.all_gather(shard, "sp", axis=0, tiled=True)

    widened = lax.all_gather(tokens, "tp", axis=1, tiled=True).astype(jnp.float32)
    normed = (
        widened * lax.rsqrt(jnp.mean(widened * widened, axis=-1, keepdims=True) + epsilon) * norm_gain
    ).astype(jnp.bfloat16)
    half = w_query.shape[1]
    conv_a = project(normed, gather(w_conv_a)).astype(jnp.bfloat16)
    conv_gate = project(normed, gather(w_conv_gate)).astype(jnp.bfloat16)
    full_qkd = gather(jnp.concatenate([w_query, w_key, w_decay], axis=1))
    full_v = gather(w_value)
    gated = (conv_a.astype(jnp.float32) * jax.nn.sigmoid(conv_gate.astype(jnp.float32))).astype(jnp.bfloat16)
    conv_out = conv_branch(gated, conv_weight, conv_gain)
    query_keys = project(normed, full_qkd[:, : 2 * half]).astype(jnp.bfloat16)
    decay_pre = project(normed, full_qkd[:, 2 * half :])
    values = project(normed, full_v).astype(jnp.bfloat16)
    attn, since, end, end_log = gla_local(
        query_keys[:, :half], query_keys[:, half:], values, decay_pre, decay_extra, decay_bias
    )
    packed = jnp.concatenate([end, jnp.broadcast_to(jnp.exp(end_log), (16, half))], axis=0).astype(jnp.bfloat16)
    ends = gather(packed)
    out_gate = project(normed, gather(w_outgate)).astype(jnp.bfloat16)
    gla_out = gla_finish(attn, since, out_gate, ends, init_state, head_gain, me)
    total = dot(conv_out, gather(w_out_conv.T), ((1,), (1,))) + dot(gla_out, gather(w_out_gla.T), ((1,), (1,)))
    return lax.psum_scatter(total.astype(jnp.bfloat16), "tp", scatter_dimension=0, tiled=True)


def per_device(*arrays):
    if folded(lax.axis_size("sp"), lax.axis_size("tp")):
        return fused_layer(*arrays)
    return plain_layer(*arrays)


def solution(mesh):
    placed = (
        P("sp", "tp"), P(), P("sp", "tp"), P("sp", "tp"), P(None, "tp"), P("tp"), P("sp", "tp"), P("sp", "tp"),
        P("sp", "tp"), P("sp", "tp"), P("sp", "tp"), P("tp"), P("sp", "tp"), P(), P("tp", None, None),
        P("tp", "sp"), P("tp", "sp"),
    )
    return jax.shard_map(
        per_device, mesh=mesh, in_specs=placed, out_specs=P(("sp", "tp"), None), check_vma=False
    )
```

```python
import functools

import jax
import jax.numpy as jnp
from jax import lax
from jax.experimental import pallas as pl
from jax.experimental.pallas import tpu as pltpu
from jax.sharding import PartitionSpec as P

D_CONV = 1024
HK = 64
HV = 128
BLOCK = 64

epsilon = 1e-06
gate_divisor = 16.0

MESH = pl.DeviceIdType.MESH


def dot(a, b, dims):
    return lax.dot_general(a, b, (dims, ((), ())), preferred_element_type=jnp.float32)


def folded(n_sp, n_tp):
    return n_sp == 16 and n_tp == 2


class Mover:
    def __init__(self):
        self.me = lax.axis_index("sp")
        self.tp = lax.axis_index("tp")
        self.z, self.y, self.x = self.me // 4, (self.me // 2) % 2, self.me % 2
        self.other = {"x": self.me + 1 - 2 * self.x, "y": self.me + 2 - 4 * self.y}
        self.across = self.me + 3 - 2 * self.x - 4 * self.y
        self.sent = []

    def copy(self, source, target, send, recv, place, core=None):
        core = self.tp if core is None else core
        return pltpu.make_async_remote_copy(
            src_ref=source, dst_ref=target, send_sem=send, recv_sem=recv, device_id=(place, core), device_id_type=MESH
        )

    def piece(self, j):
        z = self.z
        return (z, z + 1 - 2 * (z % 2), 2 - z // 2, 3 - 3 * (z // 2))[j]


class Flow:
    def __init__(self, mover, number, view, first, sems):
        self.m, self.number, self.view, self.first = mover, number, view, first
        self.last = {"x": "y", "y": "x"}[first]
        self.sems = sems

    def own(self, p):
        return self.view(p, self.m.y, self.m.x)

    def pair(self, p):
        every = slice(None)
        return self.view(p, self.m.y, every) if self.first == "x" else self.view(p, every, self.m.x)

    def first_copy(self, p, source=None):
        own = self.own(p) if source is None else source
        slot = self.number * 4 + p if self.number < 2 else self.number + 6
        fs, fr = self.sems["first_send"], self.sems["first_recv"]
        return self.m.copy(own, own, fs.at[self.number], fr.at[slot], self.m.other[self.first])

    def last_copy(self, p, source=None):
        pair = self.pair(p) if source is None else source
        ls, lr = self.sems["last_send"], self.sems["last_recv"]
        return self.m.copy(pair, pair, ls.at[self.number], lr.at[self.number // 2, p], self.m.other[self.last])

    def drain_first(self):
        if self.number < 2:
            self.first_copy(0, self.own(slice(None))).wait_send()
        else:
            self.first_copy(self.m.z).wait_send()

    def drain_last(self):
        self.last_copy(0, self.pair(slice(None))).wait_send()


class Line:
    def __init__(self, mover, number, view, sems):
        self.m, self.number, self.view, self.sems = mover, number, view, sems

    def up(self, p):
        return self.m.copy(
            self.view(p), self.view(p), self.sems["z_send"].at[self.number, p], self.sems["z_recv"].at[self.number, p],
            self.m.me + 4,
        )

    def down(self, p):
        return self.m.copy(
            self.view(p), self.view(p), self.sems["z_send"].at[self.number, p + 1],
            self.sems["z_recv"].at[self.number, p], self.m.me - 4,
        )

    def start_own(self):
        z = self.m.z

        @pl.when(z < 3)
        def _():
            self.up(z).start()

        @pl.when(z > 0)
        def _():
            self.down(z).start()

    def relay(self, step, then):
        z = self.m.z

        @pl.when(z >= step)
        def _():
            p = z - step
            self.up(p).wait_recv()

            @pl.when(z < 3)
            def _():
                self.up(p).start()

            then(p)

        @pl.when(z + step <= 3)
        def _():
            p = z + step
            self.down(p).wait_recv()

            @pl.when(z > 0)
            def _():
                self.down(p).start()

            then(p)

    def drain(self):
        z = self.m.z
        for p in range(4):
            @pl.when((p <= z) & (z < 3))
            def _():
                self.up(p).wait_send()

            @pl.when((p >= z) & (z > 0))
            def _():
                self.down(p).wait_send()


def at_step(z, step, then):
    if step == 0:
        then(z)
        return

    @pl.when(z >= step)
    def _():
        then(z - step)

    @pl.when(z + step <= 3)
    def _():
        then(z + step)


def layer_kernel(
    tokens, gain, wa, wg, taps, conv_gain, wq, wk, wv, wog, wd, bias, extra_in, head_gain, init, woc, wogl, own_out, other_out,
    w1, w2, w3, wo, both, normed, acc1, acc2, acc3, extra, seq, attn, since, act, psend,
    halo_out, halo_in, stat_own, stat_in, packs, state, prefix, before,
    local, first_send, first_recv, last_send, last_recv, z_send, z_recv, misc_send, misc_recv, end_send, end_recv,
    part_send, part_recv,
):
    m = Mover()
    me, tp, z, y, x = m.me, m.tp, m.z, m.y, m.x
    rows = normed.shape[0]
    half = rows // 2
    width = both.shape[2]
    n_key = acc1.shape[1] // 5
    n_conv = 2 * n_key
    heads = n_key // HK
    sems = dict(
        first_send=first_send, first_recv=first_recv, last_send=last_send, last_recv=last_recv,
        z_send=z_send, z_recv=z_recv,
    )

    def lanes(ref, low, size):
        return lambda p, yy, xx: ref.at[p, yy, xx, :, pl.ds(low, size)]

    def depth(low, size):
        return lambda p, yy, xx: wo.at[p, yy, xx, pl.ds(low, size), :]

    mid = w1.shape[-1] // 2
    late = wo.shape[3] // 8
    early = wo.shape[3] // 2 - late
    b1 = Flow(m, 0, lanes(w1, 0, mid), "x", sems)
    b2 = Flow(m, 1, lanes(w1, mid, mid), "y", sems)
    pairs = [
        (Flow(m, 2, lanes(w2, 0, n_conv), "x", sems), Flow(m, 3, lanes(w2, n_conv, n_conv), "y", sems)),
        (Flow(m, 4, lanes(w3, 0, n_key), "x", sems), Flow(m, 5, lanes(w3, n_key, n_key), "y", sems)),
        (Flow(m, 6, depth(0, early), "x", sems), Flow(m, 7, depth(early, early), "y", sems)),
        (Flow(m, 8, depth(2 * early, late), "x", sems), Flow(m, 9, depth(2 * early + late, late), "y", sems)),
    ]
    whole = Line(m, 0, lambda p: w1.at[p, y, x], sems)
    lines = [tuple(Line(m, f.number - 1, f.pair, sems) for f in pair) for pair in pairs]

    loads = [
        (wq, w1.at[z, y, x, :, pl.ds(0, n_key)]),
        (wk, w1.at[z, y, x, :, pl.ds(n_key, n_key)]),
        (wd, w1.at[z, y, x, :, pl.ds(2 * n_key, n_key)]),
        (wv, w1.at[z, y, x, :, pl.ds(3 * n_key, n_conv)]),
        (wa, w2.at[z, y, x, :, pl.ds(0, n_conv)]),
        (wg, w2.at[z, y, x, :, pl.ds(n_conv, n_conv)]),
        (wog, w3.at[z, y, x]),
        (woc, wo.at[z, y, x, pl.ds(0, n_conv), :]),
        (wogl, wo.at[z, y, x, pl.ds(n_conv, n_conv), :]),
        (tokens, both.at[tp]),
        (extra_in, extra),
    ]
    loads = [pltpu.make_async_copy(a, b, local.at[i]) for i, (a, b) in enumerate(loads)]
    for load in loads:
        load.start()

    barrier = pltpu.get_barrier_semaphore()
    def greet(place, core):
        pl.semaphore_signal(barrier, inc=1, device_id=(place, core), device_id_type=MESH)

    for place, core in ((m.other["x"], tp), (m.other["y"], tp), (me, 1 - tp)):
        greet(place, core)

    @pl.when(z < 3)
    def _():
        greet(me + 4, tp)

    @pl.when(z > 0)
    def _():
        greet(me - 4, tp)

    at_end = (z == 0) | (z == 3)

    @pl.when(at_end)
    def _():
        pl.semaphore_wait(barrier, 4)

    @pl.when(jnp.logical_not(at_end))
    def _():
        pl.semaphore_wait(barrier, 5)

    for i in range(4):
        loads[i].wait()
    whole.start_own()
    b1.first_copy(z).start()
    b2.first_copy(z).start()
    loads[9].wait()
    swap = m.copy(both.at[tp], both.at[tp], misc_send.at[0], misc_recv.at[0], me, 1 - tp)
    swap.start()
    loads[4].wait()
    loads[5].wait()
    for f in pairs[0]:
        f.first_copy(z).start()
    loads[6].wait()
    for f in pairs[1]:
        f.first_copy(z).start()
    for i in (7, 8, 10):
        loads[i].wait()

    def head_firsts(step):
        def one(p):
            b1.first_copy(p).wait_recv()
            b1.last_copy(p).start()
            b2.first_copy(p).wait_recv()
            b2.last_copy(p).start()

        at_step(z, step, one)

    def head_line(step):
        def then(p):
            b1.first_copy(p).start()
            b2.first_copy(p).start()

        whole.relay(step, then)

    def begin(k):
        for f in pairs[k]:
            f.first_copy(z).start()

    def enter_one(k, i):
        pairs[k][i].first_copy(z).wait_recv()
        lines[k][i].start_own()

    def enter(k):
        enter_one(k, 0)
        enter_one(k, 1)

    def own_last(k):
        for f in pairs[k]:
            f.last_copy(z).start()

    def pass_on(k, step):
        for f, line in zip(pairs[k], lines[k]):
            line.relay(step, lambda p: f.last_copy(p).start())

    def relay_only(k, step):
        for line in lines[k]:
            line.relay(step, lambda p: None)

    def finish(k, step):
        for f in pairs[k]:
            at_step(z, step, lambda p: f.last_copy(p).start())

    def arrived(k, p):
        every = (p, slice(None), slice(None))
        both_flows = (
            w1.at[(*every, slice(None), pl.ds(0, mid))],
            w2.at[(*every, slice(None), pl.ds(0, n_conv))],
            w3.at[(*every, slice(None), pl.ds(0, n_key))],
            wo.at[(*every, pl.ds(0, early), slice(None))],
            wo.at[(*every, pl.ds(0, late), slice(None))],
        )[k]
        flow = b1 if k == 0 else pairs[k - 1][0]
        flow.last_copy(p, both_flows).wait_recv()

    def norm_tiles(low, high):
        def body(i, carry):
            at = pl.ds(pl.multiple_of(i * 128, 128), 128)
            a = both[0, at, :].astype(jnp.float32)
            b = both[1, at, :].astype(jnp.float32)
            square = jnp.sum(a * a + b * b, axis=1, keepdims=True)
            scale = lax.rsqrt(square / (2 * width) + epsilon)
            normed[at, :width] = (a * scale * gain[:, :width]).astype(jnp.bfloat16)
            normed[at, width:] = (b * scale * gain[:, width:]).astype(jnp.bfloat16)
            return carry

        lax.fori_loop(low, high, body, 0)

    def slab(acc, ref, p, first):
        size = ref.shape[1] * ref.shape[2] * ref.shape[3]

        def body(c, carry):
            at = pl.ds(pl.multiple_of(c * 256, 256), 256)
            left = normed[:, pl.ds(pl.multiple_of(p * size, size), size)]
            right = ref[p, :, :, :, at].reshape(size, 256)
            got = dot(left, right, ((1,), (0,)))
            if first:
                acc[:, at] = got
            else:
                acc[:, at] += got
            return carry

        lax.fori_loop(0, acc.shape[1] // 256, body, 0)

    swap.wait_recv()
    norm_tiles(0, 4)
    head_line(1)
    head_firsts(0)
    norm_tiles(4, 8)
    enter_one(0, 0)
    head_line(2)
    enter_one(0, 1)
    head_firsts(1)
    head_line(3)
    arrived(0, m.piece(0))
    slab(acc1, w1, m.piece(0), True)
    head_firsts(2)
    begin(2)
    begin(3)
    pass_on(0, 1)
    arrived(0, m.piece(1))
    slab(acc1, w1, m.piece(1), False)
    head_firsts(3)
    enter(1)
    own_last(0)
    pass_on(0, 2)
    arrived(0, m.piece(2))
    slab(acc1, w1, m.piece(2), False)
    pass_on(1, 1)
    enter(2)
    arrived(0, m.piece(3))
    slab(acc1, w1, m.piece(3), False)

    state[...] = jnp.zeros_like(state)
    prefix[...] = jnp.zeros_like(prefix)
    r_iota = lax.broadcasted_iota(jnp.int32, (BLOCK, BLOCK), 0)
    c_iota = lax.broadcasted_iota(jnp.int32, (BLOCK, BLOCK), 1)
    causal = r_iota >= c_iota
    lower = causal.astype(jnp.float32)

    def block(i, carry):
        at = pl.ds(pl.multiple_of(i * BLOCK, BLOCK), BLOCK)
        pre = acc1[at, 2 * n_key : 3 * n_key] + bias[...]
        logs = jax.nn.log_sigmoid(pre) / gate_divisor + extra[at, :]
        cum = lax.dot_general(
            lower, logs, (((1,), (0,)), ((), ())), precision=lax.Precision.HIGHEST, preferred_element_type=jnp.float32
        )
        total = cum[BLOCK - 1 :, :]
        middle = cum[BLOCK // 2 - 1 : BLOCK // 2, :]
        query = acc1[at, 0:n_key].astype(jnp.bfloat16).astype(jnp.float32) * HK ** (-0.5)
        keys = acc1[at, n_key : 2 * n_key].astype(jnp.bfloat16).astype(jnp.float32)
        decayed = query * jnp.exp(cum)
        since[at, :] = (decayed * jnp.exp(prefix[...])).astype(jnp.bfloat16)
        decayed = decayed.astype(jnp.bfloat16)
        query = (query * jnp.exp(cum - middle)).astype(jnp.bfloat16)
        inverse = (keys * jnp.exp(middle - cum)).astype(jnp.bfloat16)
        to_end = (keys * jnp.exp(total - cum)).astype(jnp.bfloat16)
        entering = state[...].astype(jnp.bfloat16)
        added = []
        for h in range(heads):
            ks, vs = slice(h * HK, (h + 1) * HK), slice(h * HV, (h + 1) * HV)
            values = acc1[at, 3 * n_key + h * HV : 3 * n_key + (h + 1) * HV].astype(jnp.bfloat16)
            scores = jnp.where(causal, dot(query[:, ks], inverse[:, ks], ((1,), (1,))), 0.0)
            attn[at, vs] = dot(scores.astype(jnp.bfloat16), values, ((1,), (0,))) + dot(
                decayed[:, ks], entering[:, ks], ((1,), (1,))
            )
            added.append(dot(values, to_end[:, ks], ((0,), (0,))))
        state[...] = state[...] * jnp.exp(total) + jnp.concatenate(added, axis=1)
        prefix[...] = prefix[...] + total
        return carry

    blocks = rows // BLOCK

    def attend(i, carry):
        block(i, 0)

        @pl.when(i == blocks // 2)
        def _():
            pass_on(0, 3)

        @pl.when(i == blocks - 3)
        def _():
            relay_only(1, 2)

        return carry

    lax.fori_loop(0, blocks, attend, 0)

    def pack(slot, decay, end):
        packs[slot, 0:HV, :] = end.astype(jnp.bfloat16)
        packs[slot, HV:, :] = jnp.broadcast_to(decay, (16, n_key)).astype(jnp.bfloat16)

    def read(slot):
        return packs[slot, HV : HV + 1, :].astype(jnp.float32), packs[slot, 0:HV, :].astype(jnp.float32)

    def end_copy(source, target, number, place):
        return m.copy(packs.at[source], packs.at[target], end_send.at[number], end_recv.at[target], place)

    def join(early, late):
        return early[0] * late[0], early[1] * late[0] + late[1]

    near_ends = [
        end_copy(0, 1, 0, m.other["x"]),
        end_copy(0, 2, 1, m.other["y"]),
        end_copy(0, 3, 2, m.across),
    ]
    pack(0, jnp.exp(prefix[...]), state[...])

    arrived(1, m.piece(0))
    slab(acc2, w2, m.piece(0), True)
    for end in near_ends:
        end.start()
    own_last(1)
    finish(1, 2)
    pass_on(2, 1)
    enter(3)
    arrived(1, m.piece(1))
    slab(acc2, w2, m.piece(1), False)
    arrived(1, m.piece(2))
    slab(acc2, w2, m.piece(2), False)
    arrived(1, m.piece(3))
    slab(acc2, w2, m.piece(3), False)
    pass_on(1, 3)
    own_last(2)

    def join_near():
        for end in near_ends:
            end.wait_recv()
        run = (jnp.ones((1, n_key), jnp.float32), jnp.zeros((HV, n_key), jnp.float32))
        pre = run
        for yy in range(2):
            for xx in range(2):
                past = yy * 2 + xx < y * 2 + x
                run = join(run, read((y + yy - 2 * y * yy) * 2 + x + xx - 2 * x * xx))
                pre = jnp.where(past, run[0], pre[0]), jnp.where(past, run[1], pre[1])
        before[0:HV, :] = pre[1]
        before[HV:, :] = jnp.broadcast_to(pre[0], (8, n_key))
        pack(4, *run)

    def far_end(k):
        return end_copy(4, 4 + k, 2 + k, me + 4 * k)

    pad = seq.shape[1] - rows

    def gate_tiles(low, high):
        def body(i, carry):
            at = pl.ds(pl.multiple_of(i * 128, 128), 128)
            for c in range(n_conv // 128):
                a = acc2[at, c * 128 : (c + 1) * 128].astype(jnp.bfloat16).astype(jnp.float32)
                g = acc2[at, n_conv + c * 128 : n_conv + (c + 1) * 128].astype(jnp.bfloat16).astype(jnp.float32)
                value = (a * jax.nn.sigmoid(g)).astype(jnp.bfloat16)
                seq[c, pl.ds(pl.multiple_of(i * 128 + pad, 32), 128), :] = value.astype(jnp.float32)
            return carry

        lax.fori_loop(low, high, body, 0)

    gate_tiles(rows // 128 - 1, rows // 128)
    for c in range(n_conv // 128):
        halo_out[:, c * 128 : (c + 1) * 128] = seq[c, rows : rows + pad, :].astype(jnp.bfloat16)
    gate_tiles(0, rows // 128 - 1)
    halo = m.copy(halo_out, halo_in, misc_send.at[1], misc_recv.at[1], me + 1)

    @pl.when(me < 15)
    def _():
        halo.start()

    n_taps = taps.shape[0]
    shift = pad - (n_taps - 1)

    def conv_chunk(i):
        base = pl.multiple_of(i * 128, 128)
        sums = jnp.zeros((128, 128), jnp.float32)
        squares = jnp.zeros((128, 128), jnp.float32)
        for c in range(n_conv // 128):
            part = seq[c, pl.ds(base, 128 + pad), :]
            total = jnp.zeros((128, 128), jnp.float32)
            for turn in range(8):
                moved = part if turn == 0 else pltpu.roll(part, 128 + pad - turn, 0)
                for tap in range(n_taps):
                    if (shift + tap) % 8 == turn:
                        start = shift + tap - turn
                        total = total + taps[tap : tap + 1, c * 128 : (c + 1) * 128] * moved[start : start + 128]
            acc2[pl.ds(base, 128), c * 128 : (c + 1) * 128] = total
            sums = sums + total
            squares = squares + total * total
        first = jnp.sum(sums, axis=1, keepdims=True)
        second = jnp.sum(squares, axis=1, keepdims=True)
        lane = lax.broadcasted_iota(jnp.int32, (128, 128), 1)
        stat_own[pl.ds(base, 128), :] = jnp.where(lane == 0, first, second)

    chunks = rows // 128

    def conv_loop(i, carry):
        conv_chunk(i)

        @pl.when(i == chunks // 2)
        def _():
            pass_on(2, 2)

        @pl.when(i == chunks - 3)
        def _():
            join_near()

        @pl.when(i == chunks - 1)
        def _():
            for k in (1, 2, 3):
                @pl.when(z + k <= 3)
                def _():
                    far_end(k).start()

        return carry

    lax.fori_loop(1, chunks, conv_loop, 0)

    @pl.when(me > 0)
    def _():
        halo.wait_recv()
        for c in range(n_conv // 128):
            seq[c, 0:pad, :] = halo_in[:, c * 128 : (c + 1) * 128].astype(jnp.float32)

    @pl.when(me == 0)
    def _():
        seq[:, 0:pad, :] = jnp.zeros((n_conv // 128, pad, 128), jnp.float32)

    lax.fori_loop(0, 1, conv_loop, 0)

    pass_on(3, 1)
    own_last(3)
    arrived(2, m.piece(0))
    slab(acc3, w3, m.piece(0), True)
    stats = m.copy(stat_own, stat_in, misc_send.at[2], misc_recv.at[2], me, 1 - tp)
    stats.start()
    arrived(2, m.piece(1))
    slab(acc3, w3, m.piece(1), False)
    arrived(2, m.piece(2))
    slab(acc3, w3, m.piece(2), False)
    arrived(2, m.piece(3))
    slab(acc3, w3, m.piece(3), False)
    pass_on(2, 3)
    stats.wait_recv()

    def conv_finish(i, carry):
        at = pl.ds(pl.multiple_of(i * 128, 128), 128)
        both_stats = stat_own[at, :] + stat_in[at, :]
        mean_val = both_stats[:, 0:1] / (2 * n_conv)
        square_mean = both_stats[:, 1:2] / (2 * n_conv)
        scale = lax.rsqrt(square_mean - mean_val * mean_val + epsilon)
        value = (acc2[at, 0:n_conv] - mean_val) * scale * conv_gain[...]
        act[at, 0:n_conv] = (value * jax.nn.sigmoid(value)).astype(jnp.bfloat16)
        return carry

    lax.fori_loop(0, chunks, conv_finish, 0)
    pass_on(3, 2)
    for k in (1, 2, 3):
        @pl.when(z - k >= 0)
        def _():
            end_copy(4, 4 + k, 2 + k, me).wait_recv()
            pre = join(read(4 + k), (before[HV : HV + 1, :], before[0:HV, :]))
            before[0:HV, :] = pre[1]
            before[HV:, :] = jnp.broadcast_to(pre[0], (8, n_key))

    entry = jnp.concatenate([init[h].T for h in range(heads)], axis=1)
    state[...] = entry * before[HV : HV + 1, :] + before[0:HV, :]

    def gla_finish(i, carry):
        at = pl.ds(pl.multiple_of(i * 256, 256), 256)
        entering = state[...].astype(jnp.bfloat16)
        for h in range(heads):
            ks, vs = slice(h * HK, (h + 1) * HK), slice(h * HV, (h + 1) * HV)
            value = attn[at, vs] + dot(since[at, ks], entering[:, ks], ((1,), (1,)))
            value = value * lax.rsqrt(jnp.mean(value * value, axis=-1, keepdims=True) + epsilon) * head_gain[...]
            gate = acc3[at, vs].astype(jnp.bfloat16).astype(jnp.float32)
            act[at, n_conv + h * HV : n_conv + (h + 1) * HV] = (value * (gate * jax.nn.sigmoid(gate))).astype(jnp.bfloat16)
        return carry

    lax.fori_loop(0, rows // 256, gla_finish, 0)

    def part_copy(b):
        at = pl.ds(pl.multiple_of(b * 256, 256), 256)
        return m.copy(psend.at[b], other_out.at[:, at], part_send, part_recv, me, 1 - tp)

    def project(p, yy, core):
        weight = jnp.concatenate([wo[p, yy, 0], wo[p, yy, 1]], axis=1)
        left = act[pl.ds(pl.multiple_of(core * half, half), half), :]
        return dot(left, weight, ((1,), (0,))).astype(jnp.bfloat16)

    def out_pieces(j):
        p = m.piece(j)

        def theirs(yy, carry):
            psend[p * 2 + yy] = project(p, yy, 1 - tp)
            return carry

        def ours(yy, carry):
            part_copy(p * 2 + yy).start()
            own_out[:, pl.ds(pl.multiple_of((p * 2 + yy) * 256, 256), 256)] = project(p, yy, tp)
            return carry

        arrived(3, p)
        arrived(4, p)
        lax.fori_loop(0, 2, theirs, 0)
        lax.fori_loop(0, 2, ours, 0)

    def rows_of(core):
        return pl.ds(pl.multiple_of(core * half, half), half)

    def last_part(yy, low, high):
        p = m.piece(3)
        weight = jnp.concatenate([wo[p, yy, 0, low:high, :], wo[p, yy, 1, low:high, :]], axis=1)
        return lambda core: dot(act[rows_of(core), low:high], weight, ((1,), (0,)))

    def last_begin():
        def body(yy, carry):
            part = last_part(yy, 0, 2 * early)
            at = pl.ds(pl.multiple_of(yy * 256, 256), 256)
            acc2[0:half, at] = part(1 - tp)
            acc2[half:, at] = part(tp)
            return carry

        arrived(3, m.piece(3))
        lax.fori_loop(0, 2, body, 0)

    def last_end():
        b = m.piece(3) * 2

        def theirs(yy, carry):
            at = pl.ds(pl.multiple_of(yy * 256, 256), 256)
            part = last_part(yy, 2 * early, 2 * early + 2 * late)
            psend[b + yy] = (acc2[0:half, at] + part(1 - tp)).astype(jnp.bfloat16)
            return carry

        def ours(yy, carry):
            part_copy(b + yy).start()
            at = pl.ds(pl.multiple_of(yy * 256, 256), 256)
            part = last_part(yy, 2 * early, 2 * early + 2 * late)
            own_out[:, pl.ds(pl.multiple_of((b + yy) * 256, 256), 256)] = (acc2[half:, at] + part(tp)).astype(jnp.bfloat16)
            return carry

        arrived(4, m.piece(3))
        lax.fori_loop(0, 2, theirs, 0)
        lax.fori_loop(0, 2, ours, 0)

    def drain_early():
        swap.wait_send()
        stats.wait_send()

        @pl.when(me < 15)
        def _():
            halo.wait_send()

        for end in near_ends:
            end.wait_send()
        for k in (1, 2, 3):
            @pl.when(z + k <= 3)
            def _():
                far_end(k).wait_send()

        for f in (b1, b2, *pairs[0], *pairs[1]):
            f.drain_first()
            f.drain_last()
        for f in (*pairs[2], *pairs[3]):
            f.drain_first()
        whole.drain()
        for pair in lines:
            for line in pair:
                line.drain()

    out_pieces(0)
    pass_on(3, 3)
    out_pieces(1)
    out_pieces(2)
    last_begin()
    drain_early()
    last_end()

    for f in (*pairs[2], *pairs[3]):
        f.drain_last()
    m.copy(psend, psend, part_send, part_recv, me, 1 - tp).wait_send()
    m.copy(other_out, other_out, part_send, part_recv, me, 1 - tp).wait_recv()


def fused_layer(
    tokens, norm_gain, w_conv_a, w_conv_gate, conv_weight, conv_gain, w_query, w_key, w_value, w_outgate,
    w_decay, decay_bias, decay_extra, head_gain, init_state, w_out_conv, w_out_gla,
):
    rows, width = tokens.shape
    depth = w_query.shape[0]
    n_key = w_query.shape[1]
    n_conv = w_conv_a.shape[1]
    cols = w_out_conv.shape[1]
    half = rows // 2
    pad = 32
    bf16, f32 = jnp.bfloat16, jnp.float32
    dma = pltpu.SemaphoreType.DMA
    vm = pl.BlockSpec(memory_space=pltpu.VMEM)
    hbm = pl.BlockSpec(memory_space=pl.ANY)
    share = pltpu.VMEM((half, 2 * width), bf16)
    own, other = pl.pallas_call(
        layer_kernel,
        out_shape=[share, share],
        in_specs=[hbm, vm, hbm, hbm, vm, vm, hbm, hbm, hbm, hbm, hbm, vm, hbm, vm, vm, hbm, hbm],
        out_specs=[vm, vm],
        scratch_shapes=[
            pltpu.VMEM((4, 2, 2, depth, 5 * n_key), bf16),
            pltpu.VMEM((4, 2, 2, depth, 2 * n_conv), bf16),
            pltpu.VMEM((4, 2, 2, depth, n_conv), bf16),
            pltpu.VMEM((4, 2, 2, 2 * n_conv, cols), bf16),
            pltpu.VMEM((2, rows, width), bf16),
            pltpu.VMEM((rows, 2 * width), bf16),
            pltpu.VMEM((rows, 5 * n_key), f32),
            pltpu.VMEM((rows, 2 * n_conv), f32),
            pltpu.VMEM((rows, n_conv), f32),
            pltpu.VMEM((rows, n_key), f32),
            pltpu.VMEM((n_conv // 128, rows + pad, 128), f32),
            pltpu.VMEM((rows, n_conv), f32),
            pltpu.VMEM((rows, n_key), bf16),
            pltpu.VMEM((rows, 2 * n_conv), bf16),
            pltpu.VMEM((8, half, 256), bf16),
            pltpu.VMEM((pad, n_conv), bf16),
            pltpu.VMEM((pad, n_conv), bf16),
            pltpu.VMEM((rows, 128), f32),
            pltpu.VMEM((rows, 128), f32),
            pltpu.VMEM((8, HV + 16, n_key), bf16),
            pltpu.VMEM((HV, n_key), f32),
            pltpu.VMEM((1, n_key), f32),
            pltpu.VMEM((HV + 8, n_key), f32),
            dma((11,)), dma((10,)), dma((16,)), dma((10,)), dma((5, 4)), dma((9, 5)), dma((9, 4)),
            dma((3,)), dma((3,)), dma((6,)), dma((8,)), dma(()), dma(()),
        ],
        compiler_params=pltpu.CompilerParams(collective_id=0, has_side_effects=True, vmem_limit_bytes=56 * 2**20),
        name="layer",
    )(
        tokens, norm_gain[None, :], w_conv_a, w_conv_gate, conv_weight, conv_gain[None, :], w_query, w_key, w_value,
        w_outgate, w_decay, decay_bias[None, :], decay_extra, head_gain[None, :], init_state, w_out_conv, w_out_gla,
    )
    return (own.astype(f32) + other.astype(f32)).astype(bf16)


def local_kernel(heads, pieces, q_ref, k_ref, v_ref, pre_ref, extra_ref, bias_ref, attn_ref, since_ref, end_ref, log_ref, state, prefix):
    step = pl.program_id(0)

    @pl.when(step == 0)
    def _():
        state[...] = jnp.zeros_like(state)
        prefix[...] = jnp.zeros_like(prefix)

    rows = lax.broadcasted_iota(jnp.int32, (BLOCK, BLOCK), 0)
    columns = lax.broadcasted_iota(jnp.int32, (BLOCK, BLOCK), 1)
    causal = rows >= columns
    lower = causal.astype(jnp.float32)
    for piece in range(pieces):
        at = pl.ds(piece * BLOCK, BLOCK)
        pre = pre_ref[at, :] + bias_ref[...]
        logs = jax.nn.log_sigmoid(pre) / gate_divisor + extra_ref[at, :]
        cum = lax.dot_general(
            lower, logs, (((1,), (0,)), ((), ())), precision=lax.Precision.HIGHEST, preferred_element_type=jnp.float32
        )
        total = cum[BLOCK - 1 :, :]
        middle = cum[BLOCK // 2 - 1 : BLOCK // 2, :]
        query = q_ref[at, :].astype(jnp.float32) * HK ** (-0.5)
        keys = k_ref[at, :].astype(jnp.float32)
        decayed = query * jnp.exp(cum)
        since_ref[at, :] = (decayed * jnp.exp(prefix[...])).astype(jnp.bfloat16)
        decayed = decayed.astype(jnp.bfloat16)
        query = (query * jnp.exp(cum - middle)).astype(jnp.bfloat16)
        inverse = (keys * jnp.exp(middle - cum)).astype(jnp.bfloat16)
        to_end = (keys * jnp.exp(total - cum)).astype(jnp.bfloat16)
        entering = state[...].astype(jnp.bfloat16)
        added = []
        for h in range(heads):
            ks, vs = slice(h * HK, (h + 1) * HK), slice(h * HV, (h + 1) * HV)
            values = v_ref[at, vs]
            scores = jnp.where(causal, dot(query[:, ks], inverse[:, ks], ((1,), (1,))), 0.0)
            attn_ref[at, vs] = dot(scores.astype(jnp.bfloat16), values, ((1,), (0,))) + dot(
                decayed[:, ks], entering[:, ks], ((1,), (1,))
            )
            added.append(dot(values, to_end[:, ks], ((0,), (0,))))
        added = added[0] if heads == 1 else jnp.concatenate(added, axis=1)
        state[...] = state[...] * jnp.exp(total) + added
        prefix[...] = prefix[...] + total
    end_ref[...] = state[...]
    log_ref[...] = prefix[...]


def gla_local(query, keys, values, decay_pre, decay_extra, decay_bias):
    rows, width = query.shape
    heads = width // HK
    pieces = 4
    tile = pieces * BLOCK

    def tiled(array):
        return pl.BlockSpec((tile, array.shape[1]), lambda i: (i, 0))

    def whole(shape):
        return pl.BlockSpec(shape, lambda i: (0, 0))

    return pl.pallas_call(
        functools.partial(local_kernel, heads, pieces),
        grid=(rows // tile,),
        in_specs=[tiled(query), tiled(keys), tiled(values), tiled(decay_pre), tiled(decay_extra), whole((1, width))],
        out_specs=[tiled(values), tiled(query), whole((HV, width)), whole((1, width))],
        out_shape=[
            jax.ShapeDtypeStruct(values.shape, jnp.float32),
            jax.ShapeDtypeStruct(query.shape, jnp.bfloat16),
            jax.ShapeDtypeStruct((HV, width), jnp.float32),
            jax.ShapeDtypeStruct((1, width), jnp.float32),
        ],
        scratch_shapes=[pltpu.VMEM((HV, width), jnp.float32), pltpu.VMEM((1, width), jnp.float32)],
        cost_estimate=pl.CostEstimate(flops=10**10, bytes_accessed=10**7, transcendentals=10**6),
        name="gla_local",
    )(query, keys, values, decay_pre, decay_extra, decay_bias[None, :])


def finish_kernel(heads, size, where_ref, attn_ref, since_ref, gate_ref, ends_ref, init_ref, gain_ref, out_ref, state):
    me = where_ref[0]

    @pl.when(pl.program_id(0) == 0)
    def _():
        state[...] = init_ref[...]

        def one(device, carry):
            at = device
            decay = ends_ref[pl.ds(pl.multiple_of(at * size + HV, 16), 16), :].astype(jnp.float32)[:1]
            end = ends_ref[pl.ds(pl.multiple_of(at * size, 16), HV), :].astype(jnp.float32)
            state[...] = state[...] * decay + end
            return carry

        lax.fori_loop(0, me, one, 0)

    entering = state[...].astype(jnp.bfloat16)
    for h in range(heads):
        ks, vs = slice(h * HK, (h + 1) * HK), slice(h * HV, (h + 1) * HV)
        attn = attn_ref[:, vs] + dot(since_ref[:, ks], entering[:, ks], ((1,), (1,)))
        attn = attn * lax.rsqrt(jnp.mean(attn * attn, axis=-1, keepdims=True) + epsilon) * gain_ref[...]
        gate = gate_ref[:, vs].astype(jnp.float32)
        out_ref[:, vs] = (attn * (gate * jax.nn.sigmoid(gate))).astype(jnp.bfloat16)


def gla_finish(attn, since, out_gate, ends, init_state, head_gain, me):
    rows, width = since.shape
    heads = width // HK
    tile = 256

    def tiled(array):
        return pl.BlockSpec((tile, array.shape[1]), lambda i, w: (i, 0))

    def whole(array):
        return pl.BlockSpec(array.shape, lambda i, w: (0, 0))

    init = init_state.transpose(2, 0, 1).reshape(HV, width)
    gain = head_gain[None, :]
    return pl.pallas_call(
        functools.partial(finish_kernel, heads, HV + 16),
        grid_spec=pltpu.PrefetchScalarGridSpec(
            num_scalar_prefetch=1,
            grid=(rows // tile,),
            in_specs=[tiled(attn), tiled(since), tiled(out_gate), whole(ends), whole(init), whole(gain)],
            out_specs=tiled(attn),
            scratch_shapes=[pltpu.VMEM((HV, width), jnp.float32)],
        ),
        out_shape=jax.ShapeDtypeStruct(attn.shape, jnp.bfloat16),
        cost_estimate=pl.CostEstimate(flops=3 * 10**9, bytes_accessed=10**7, transcendentals=10**6),
        name="gla_finish",
    )(me[None], attn, since, out_gate, ends, init, gain)


def conv_branch(gated, conv_weight, conv_gain):
    taps = conv_weight.shape[0]
    row_count = gated.shape[0]
    count = lax.axis_size("sp")
    earlier = lax.ppermute(gated[row_count - taps + 1 :], "sp", [(i, i + 1) for i in range(count - 1)])
    extended = jnp.concatenate([earlier, gated], axis=0).astype(jnp.float32)
    conv_sum = jnp.zeros(gated.shape, jnp.float32)
    for tap in range(taps):
        conv_sum = conv_sum + conv_weight[tap][None, :] * extended[tap : tap + row_count]
    row_sums, row_squares = lax.psum((jnp.sum(conv_sum, axis=1), jnp.sum(conv_sum * conv_sum, axis=1)), "tp")
    mean_val = (row_sums / D_CONV)[:, None]
    square_mean = (row_squares / D_CONV)[:, None]
    conv_norm = (conv_sum - mean_val) * lax.rsqrt(square_mean - mean_val * mean_val + epsilon) * conv_gain
    return jax.nn.silu(conv_norm).astype(jnp.bfloat16)


def project(hidden, weight):
    return dot(hidden, weight, ((1,), (0,)))


def plain_layer(
    tokens, norm_gain, w_conv_a, w_conv_gate, conv_weight, conv_gain, w_query, w_key, w_value, w_outgate,
    w_decay, decay_bias, decay_extra, head_gain, init_state, w_out_conv, w_out_gla,
):
    me = lax.axis_index("sp")

    def gather(shard):
        return lax.all_gather(shard, "sp", axis=0, tiled=True)

    widened = lax.all_gather(tokens, "tp", axis=1, tiled=True).astype(jnp.float32)
    normed = (
        widened * lax.rsqrt(jnp.mean(widened * widened, axis=-1, keepdims=True) + epsilon) * norm_gain
    ).astype(jnp.bfloat16)
    half = w_query.shape[1]
    conv_a = project(normed, gather(w_conv_a)).astype(jnp.bfloat16)
    conv_gate = project(normed, gather(w_conv_gate)).astype(jnp.bfloat16)
    full_qkd = gather(jnp.concatenate([w_query, w_key, w_decay], axis=1))
    full_v = gather(w_value)
    gated = (conv_a.astype(jnp.float32) * jax.nn.sigmoid(conv_gate.astype(jnp.float32))).astype(jnp.bfloat16)
    conv_out = conv_branch(gated, conv_weight, conv_gain)
    query_keys = project(normed, full_qkd[:, : 2 * half]).astype(jnp.bfloat16)
    decay_pre = project(normed, full_qkd[:, 2 * half :])
    values = project(normed, full_v).astype(jnp.bfloat16)
    attn, since, end, end_log = gla_local(
        query_keys[:, :half], query_keys[:, half:], values, decay_pre, decay_extra, decay_bias
    )
    packed = jnp.concatenate([end, jnp.broadcast_to(jnp.exp(end_log), (16, half))], axis=0).astype(jnp.bfloat16)
    ends = gather(packed)
    out_gate = project(normed, gather(w_outgate)).astype(jnp.bfloat16)
    gla_out = gla_finish(attn, since, out_gate, ends, init_state, head_gain, me)
    total = dot(conv_out, gather(w_out_conv.T), ((1,), (1,))) + dot(gla_out, gather(w_out_gla.T), ((1,), (1,)))
    return lax.psum_scatter(total.astype(jnp.bfloat16), "tp", scatter_dimension=0, tiled=True)


def per_device(*arrays):
    if folded(lax.axis_size("sp"), lax.axis_size("tp")):
        return fused_layer(*arrays)
    return plain_layer(*arrays)


def solution(mesh):
    placed = (
        P("sp", "tp"), P(), P("sp", "tp"), P("sp", "tp"), P(None, "tp"), P("tp"), P("sp", "tp"), P("sp", "tp"),
        P("sp", "tp"), P("sp", "tp"), P("sp", "tp"), P("tp"), P("sp", "tp"), P(), P("tp", None, None),
        P("tp", "sp"), P("tp", "sp"),
    )
    return jax.shard_map(
        per_device, mesh=mesh, in_specs=placed, out_specs=P(("sp", "tp"), None), check_vma=False
    )
```

```python
import functools

import jax
import jax.numpy as jnp
from jax import lax
from jax.experimental import pallas as pl
from jax.experimental.pallas import tpu as pltpu
from jax.sharding import PartitionSpec as P

D_CONV = 1024
HK = 64
HV = 128
BLOCK = 64

epsilon = 1e-06
gate_divisor = 16.0

MESH = pl.DeviceIdType.MESH


def dot(a, b, dims):
    return lax.dot_general(a, b, (dims, ((), ())), preferred_element_type=jnp.float32)


def folded(n_sp, n_tp):
    return n_sp == 16 and n_tp == 2


class Mover:
    def __init__(self):
        self.me = lax.axis_index("sp")
        self.tp = lax.axis_index("tp")
        self.z, self.y, self.x = self.me // 4, (self.me // 2) % 2, self.me % 2
        self.other = {"x": self.me + 1 - 2 * self.x, "y": self.me + 2 - 4 * self.y}
        self.across = self.me + 3 - 2 * self.x - 4 * self.y
        self.sent = []

    def copy(self, source, target, send, recv, place, core=None):
        core = self.tp if core is None else core
        return pltpu.make_async_remote_copy(
            src_ref=source, dst_ref=target, send_sem=send, recv_sem=recv, device_id=(place, core), device_id_type=MESH
        )

    def piece(self, j):
        z = self.z
        return (z, z + 1 - 2 * (z % 2), 2 - z // 2, 3 - 3 * (z // 2))[j]


class Flow:
    def __init__(self, mover, number, view, first, sems):
        self.m, self.number, self.view, self.first = mover, number, view, first
        self.last = {"x": "y", "y": "x"}[first]
        self.sems = sems

    def own(self, p):
        return self.view(p, self.m.y, self.m.x)

    def pair(self, p):
        every = slice(None)
        return self.view(p, self.m.y, every) if self.first == "x" else self.view(p, every, self.m.x)

    def first_copy(self, p, source=None):
        own = self.own(p) if source is None else source
        slot = self.number * 4 + p if self.number < 2 else self.number + 6
        fs, fr = self.sems["first_send"], self.sems["first_recv"]
        return self.m.copy(own, own, fs.at[self.number], fr.at[slot], self.m.other[self.first])

    def last_copy(self, p, source=None):
        pair = self.pair(p) if source is None else source
        ls, lr = self.sems["last_send"], self.sems["last_recv"]
        return self.m.copy(pair, pair, ls.at[self.number], lr.at[self.number // 2, p], self.m.other[self.last])

    def drain_first(self):
        if self.number < 2:
            self.first_copy(0, self.own(slice(None))).wait_send()
        else:
            self.first_copy(self.m.z).wait_send()

    def drain_last(self):
        self.last_copy(0, self.pair(slice(None))).wait_send()


class Line:
    def __init__(self, mover, number, view, sems):
        self.m, self.number, self.view, self.sems = mover, number, view, sems

    def up(self, p):
        return self.m.copy(
            self.view(p), self.view(p), self.sems["z_send"].at[self.number, p], self.sems["z_recv"].at[self.number, p],
            self.m.me + 4,
        )

    def down(self, p):
        return self.m.copy(
            self.view(p), self.view(p), self.sems["z_send"].at[self.number, p + 1],
            self.sems["z_recv"].at[self.number, p], self.m.me - 4,
        )

    def start_own(self):
        z = self.m.z

        @pl.when(z < 3)
        def _():
            self.up(z).start()

        @pl.when(z > 0)
        def _():
            self.down(z).start()

    def relay(self, step, then):
        z = self.m.z

        @pl.when(z >= step)
        def _():
            p = z - step
            self.up(p).wait_recv()

            @pl.when(z < 3)
            def _():
                self.up(p).start()

            then(p)

        @pl.when(z + step <= 3)
        def _():
            p = z + step
            self.down(p).wait_recv()

            @pl.when(z > 0)
            def _():
                self.down(p).start()

            then(p)

    def drain(self):
        z = self.m.z
        for p in range(4):
            @pl.when((p <= z) & (z < 3))
            def _():
                self.up(p).wait_send()

            @pl.when((p >= z) & (z > 0))
            def _():
                self.down(p).wait_send()


def at_step(z, step, then):
    if step == 0:
        then(z)
        return

    @pl.when(z >= step)
    def _():
        then(z - step)

    @pl.when(z + step <= 3)
    def _():
        then(z + step)


def layer_kernel(
    tokens, gain, wa, wg, taps, conv_gain, wq, wk, wv, wog, wd, bias, extra_in, head_gain, init, woc, wogl, own_out, other_out,
    w1, w2, w3, wo, both, normed, acc1, acc2, acc3, extra, seq, attn, since, act, psend,
    halo_out, halo_in, stat_own, stat_in, packs, state, prefix, before,
    local, first_send, first_recv, last_send, last_recv, z_send, z_recv, misc_send, misc_recv, end_send, end_recv,
    part_send, part_recv,
):
    m = Mover()
    me, tp, z, y, x = m.me, m.tp, m.z, m.y, m.x
    rows = normed.shape[0]
    half = rows // 2
    width = both.shape[2]
    n_key = acc1.shape[1] // 5
    n_conv = 2 * n_key
    heads = n_key // HK
    sems = dict(
        first_send=first_send, first_recv=first_recv, last_send=last_send, last_recv=last_recv,
        z_send=z_send, z_recv=z_recv,
    )

    def lanes(ref, low, size):
        return lambda p, yy, xx: ref.at[p, yy, xx, :, pl.ds(low, size)]

    def depth(low, size):
        return lambda p, yy, xx: wo.at[p, yy, xx, pl.ds(low, size), :]

    mid = w1.shape[-1] // 2
    late = wo.shape[3] // 8
    early = wo.shape[3] // 2 - late
    b1 = Flow(m, 0, lanes(w1, 0, mid), "x", sems)
    b2 = Flow(m, 1, lanes(w1, mid, mid), "y", sems)
    pairs = [
        (Flow(m, 2, lanes(w2, 0, n_conv), "x", sems), Flow(m, 3, lanes(w2, n_conv, n_conv), "y", sems)),
        (Flow(m, 4, lanes(w3, 0, n_key), "x", sems), Flow(m, 5, lanes(w3, n_key, n_key), "y", sems)),
        (Flow(m, 6, depth(0, early), "x", sems), Flow(m, 7, depth(early, early), "y", sems)),
        (Flow(m, 8, depth(2 * early, late), "x", sems), Flow(m, 9, depth(2 * early + late, late), "y", sems)),
    ]
    whole = Line(m, 0, lambda p: w1.at[p, y, x], sems)
    lines = [tuple(Line(m, f.number - 1, f.pair, sems) for f in pair) for pair in pairs]

    loads = [
        (wq, w1.at[z, y, x, :, pl.ds(0, n_key)]),
        (wk, w1.at[z, y, x, :, pl.ds(n_key, n_key)]),
        (wd, w1.at[z, y, x, :, pl.ds(2 * n_key, n_key)]),
        (wv, w1.at[z, y, x, :, pl.ds(3 * n_key, n_conv)]),
        (wa, w2.at[z, y, x, :, pl.ds(0, n_conv)]),
        (wg, w2.at[z, y, x, :, pl.ds(n_conv, n_conv)]),
        (wog, w3.at[z, y, x]),
        (woc, wo.at[z, y, x, pl.ds(0, n_conv), :]),
        (wogl, wo.at[z, y, x, pl.ds(n_conv, n_conv), :]),
        (tokens, both.at[tp]),
        (extra_in, extra),
    ]
    loads = [pltpu.make_async_copy(a, b, local.at[i]) for i, (a, b) in enumerate(loads)]
    for load in loads:
        load.start()

    barrier = pltpu.get_barrier_semaphore()
    def greet(place, core):
        pl.semaphore_signal(barrier, inc=1, device_id=(place, core), device_id_type=MESH)

    for place, core in ((m.other["x"], tp), (m.other["y"], tp), (me, 1 - tp)):
        greet(place, core)

    @pl.when(z < 3)
    def _():
        greet(me + 4, tp)

    @pl.when(z > 0)
    def _():
        greet(me - 4, tp)

    at_end = (z == 0) | (z == 3)

    @pl.when(at_end)
    def _():
        pl.semaphore_wait(barrier, 4)

    @pl.when(jnp.logical_not(at_end))
    def _():
        pl.semaphore_wait(barrier, 5)

    for i in range(4):
        loads[i].wait()
    whole.start_own()
    b1.first_copy(z).start()
    b2.first_copy(z).start()
    loads[9].wait()
    swap = m.copy(both.at[tp], both.at[tp], misc_send.at[0], misc_recv.at[0], me, 1 - tp)
    swap.start()
    loads[4].wait()
    loads[5].wait()
    for f in pairs[0]:
        f.first_copy(z).start()
    loads[6].wait()
    for f in pairs[1]:
        f.first_copy(z).start()
    for i in (7, 8, 10):
        loads[i].wait()

    def head_firsts(step):
        def one(p):
            b1.first_copy(p).wait_recv()
            b1.last_copy(p).start()
            b2.first_copy(p).wait_recv()
            b2.last_copy(p).start()

        at_step(z, step, one)

    def head_line(step):
        def then(p):
            b1.first_copy(p).start()
            b2.first_copy(p).start()

        whole.relay(step, then)

    def begin(k):
        for f in pairs[k]:
            f.first_copy(z).start()

    def enter_one(k, i):
        pairs[k][i].first_copy(z).wait_recv()
        lines[k][i].start_own()

    def enter(k):
        enter_one(k, 0)
        enter_one(k, 1)

    def own_last(k):
        for f in pairs[k]:
            f.last_copy(z).start()

    def pass_on(k, step):
        for f, line in zip(pairs[k], lines[k]):
            line.relay(step, lambda p: f.last_copy(p).start())

    def relay_only(k, step):
        for line in lines[k]:
            line.relay(step, lambda p: None)

    def finish(k, step):
        for f in pairs[k]:
            at_step(z, step, lambda p: f.last_copy(p).start())

    def arrived(k, p):
        every = (p, slice(None), slice(None))
        both_flows = (
            w1.at[(*every, slice(None), pl.ds(0, mid))],
            w2.at[(*every, slice(None), pl.ds(0, n_conv))],
            w3.at[(*every, slice(None), pl.ds(0, n_key))],
            wo.at[(*every, pl.ds(0, early), slice(None))],
            wo.at[(*every, pl.ds(0, late), slice(None))],
        )[k]
        flow = b1 if k == 0 else pairs[k - 1][0]
        flow.last_copy(p, both_flows).wait_recv()

    def norm_tiles(low, high):
        def body(i, carry):
            at = pl.ds(pl.multiple_of(i * 128, 128), 128)
            a = both[0, at, :].astype(jnp.float32)
            b = both[1, at, :].astype(jnp.float32)
            square = jnp.sum(a * a + b * b, axis=1, keepdims=True)
            scale = lax.rsqrt(square / (2 * width) + epsilon)
            normed[at, :width] = (a * scale * gain[:, :width]).astype(jnp.bfloat16)
            normed[at, width:] = (b * scale * gain[:, width:]).astype(jnp.bfloat16)
            return carry

        lax.fori_loop(low, high, body, 0)

    def slab(acc, ref, p, first):
        size = ref.shape[1] * ref.shape[2] * ref.shape[3]

        def body(c, carry):
            at = pl.ds(pl.multiple_of(c * 256, 256), 256)
            left = normed[:, pl.ds(pl.multiple_of(p * size, size), size)]
            right = ref[p, :, :, :, at].reshape(size, 256)
            got = dot(left, right, ((1,), (0,)))
            if first:
                acc[:, at] = got
            else:
                acc[:, at] += got
            return carry

        lax.fori_loop(0, acc.shape[1] // 256, body, 0)

    swap.wait_recv()
    norm_tiles(0, 4)
    head_line(1)
    head_firsts(0)
    norm_tiles(4, 8)
    enter_one(0, 0)
    head_line(2)
    enter_one(0, 1)
    head_firsts(1)
    head_line(3)
    arrived(0, m.piece(0))
    slab(acc1, w1, m.piece(0), True)
    head_firsts(2)
    begin(2)
    begin(3)
    pass_on(0, 1)
    arrived(0, m.piece(1))
    slab(acc1, w1, m.piece(1), False)
    head_firsts(3)
    enter(1)
    own_last(0)
    pass_on(0, 2)
    arrived(0, m.piece(2))
    slab(acc1, w1, m.piece(2), False)
    pass_on(1, 1)
    enter(2)
    arrived(0, m.piece(3))
    slab(acc1, w1, m.piece(3), False)

    state[...] = jnp.zeros_like(state)
    prefix[...] = jnp.zeros_like(prefix)
    r_iota = lax.broadcasted_iota(jnp.int32, (BLOCK, BLOCK), 0)
    c_iota = lax.broadcasted_iota(jnp.int32, (BLOCK, BLOCK), 1)
    causal = r_iota >= c_iota
    lower = causal.astype(jnp.float32)

    def block(i, carry):
        at = pl.ds(pl.multiple_of(i * BLOCK, BLOCK), BLOCK)
        pre = acc1[at, 2 * n_key : 3 * n_key] + bias[...]
        logs = jax.nn.log_sigmoid(pre) / gate_divisor + extra[at, :]
        cum = lax.dot_general(
            lower, logs, (((1,), (0,)), ((), ())), precision=lax.Precision.HIGHEST, preferred_element_type=jnp.float32
        )
        total = cum[BLOCK - 1 :, :]
        middle = cum[BLOCK // 2 - 1 : BLOCK // 2, :]
        query = acc1[at, 0:n_key].astype(jnp.bfloat16).astype(jnp.float32) * HK ** (-0.5)
        keys = acc1[at, n_key : 2 * n_key].astype(jnp.bfloat16).astype(jnp.float32)
        decayed = query * jnp.exp(cum)
        since[at, :] = (decayed * jnp.exp(prefix[...])).astype(jnp.bfloat16)
        decayed = decayed.astype(jnp.bfloat16)
        query = (query * jnp.exp(cum - middle)).astype(jnp.bfloat16)
        inverse = (keys * jnp.exp(middle - cum)).astype(jnp.bfloat16)
        to_end = (keys * jnp.exp(total - cum)).astype(jnp.bfloat16)
        entering = state[...].astype(jnp.bfloat16)
        added = []
        for h in range(heads):
            ks, vs = slice(h * HK, (h + 1) * HK), slice(h * HV, (h + 1) * HV)
            values = acc1[at, 3 * n_key + h * HV : 3 * n_key + (h + 1) * HV].astype(jnp.bfloat16)
            scores = jnp.where(causal, dot(query[:, ks], inverse[:, ks], ((1,), (1,))), 0.0)
            attn[at, vs] = dot(scores.astype(jnp.bfloat16), values, ((1,), (0,))) + dot(
                decayed[:, ks], entering[:, ks], ((1,), (1,))
            )
            added.append(dot(values, to_end[:, ks], ((0,), (0,))))
        state[...] = state[...] * jnp.exp(total) + jnp.concatenate(added, axis=1)
        prefix[...] = prefix[...] + total
        return carry

    blocks = rows // BLOCK

    def attend(i, carry):
        block(i, 0)

        @pl.when(i == blocks // 2)
        def _():
            pass_on(0, 3)

        @pl.when(i == blocks - 3)
        def _():
            relay_only(1, 2)

        return carry

    lax.fori_loop(0, blocks, attend, 0)

    def pack(slot, decay, end):
        packs[slot, 0:HV, :] = end.astype(jnp.bfloat16)
        packs[slot, HV:, :] = jnp.broadcast_to(decay, (16, n_key)).astype(jnp.bfloat16)

    def read(slot):
        return packs[slot, HV : HV + 1, :].astype(jnp.float32), packs[slot, 0:HV, :].astype(jnp.float32)

    def end_copy(source, target, number, place):
        return m.copy(packs.at[source], packs.at[target], end_send.at[number], end_recv.at[target], place)

    def join(early, late):
        return early[0] * late[0], early[1] * late[0] + late[1]

    near_ends = [
        end_copy(0, 1, 0, m.other["x"]),
        end_copy(0, 2, 1, m.other["y"]),
        end_copy(0, 3, 2, m.across),
    ]
    pack(0, jnp.exp(prefix[...]), state[...])

    arrived(1, m.piece(0))
    slab(acc2, w2, m.piece(0), True)
    for end in near_ends:
        end.start()
    own_last(1)
    finish(1, 2)
    pass_on(2, 1)
    enter(3)
    arrived(1, m.piece(1))
    slab(acc2, w2, m.piece(1), False)
    arrived(1, m.piece(2))
    slab(acc2, w2, m.piece(2), False)
    arrived(1, m.piece(3))
    slab(acc2, w2, m.piece(3), False)
    pass_on(1, 3)
    own_last(2)

    def join_near():
        for end in near_ends:
            end.wait_recv()
        run = (jnp.ones((1, n_key), jnp.float32), jnp.zeros((HV, n_key), jnp.float32))
        pre = run
        for yy in range(2):
            for xx in range(2):
                past = yy * 2 + xx < y * 2 + x
                run = join(run, read((y + yy - 2 * y * yy) * 2 + x + xx - 2 * x * xx))
                pre = jnp.where(past, run[0], pre[0]), jnp.where(past, run[1], pre[1])
        before[0:HV, :] = pre[1]
        before[HV:, :] = jnp.broadcast_to(pre[0], (8, n_key))
        pack(4, *run)

    def far_end(k):
        return end_copy(4, 4 + k, 2 + k, me + 4 * k)

    pad = seq.shape[1] - rows

    def gate_tiles(low, high):
        def body(i, carry):
            at = pl.ds(pl.multiple_of(i * 128, 128), 128)
            for c in range(n_conv // 128):
                a = acc2[at, c * 128 : (c + 1) * 128].astype(jnp.bfloat16).astype(jnp.float32)
                g = acc2[at, n_conv + c * 128 : n_conv + (c + 1) * 128].astype(jnp.bfloat16).astype(jnp.float32)
                value = (a * jax.nn.sigmoid(g)).astype(jnp.bfloat16)
                seq[c, pl.ds(pl.multiple_of(i * 128 + pad, 32), 128), :] = value.astype(jnp.float32)
            return carry

        lax.fori_loop(low, high, body, 0)

    gate_tiles(rows // 128 - 1, rows // 128)
    for c in range(n_conv // 128):
        halo_out[:, c * 128 : (c + 1) * 128] = seq[c, rows : rows + pad, :].astype(jnp.bfloat16)
    gate_tiles(0, rows // 128 - 1)
    halo = m.copy(halo_out, halo_in, misc_send.at[1], misc_recv.at[1], me + 1)

    @pl.when(me < 15)
    def _():
        halo.start()

    n_taps = taps.shape[0]
    shift = pad - (n_taps - 1)

    def conv_chunk(i):
        base = pl.multiple_of(i * 128, 128)
        sums = jnp.zeros((128, 128), jnp.float32)
        squares = jnp.zeros((128, 128), jnp.float32)
        for c in range(n_conv // 128):
            part = seq[c, pl.ds(base, 128 + pad), :]
            total = jnp.zeros((128, 128), jnp.float32)
            for turn in range(8):
                moved = part if turn == 0 else pltpu.roll(part, 128 + pad - turn, 0)
                for tap in range(n_taps):
                    if (shift + tap) % 8 == turn:
                        start = shift + tap - turn
                        total = total + taps[tap : tap + 1, c * 128 : (c + 1) * 128] * moved[start : start + 128]
            acc2[pl.ds(base, 128), c * 128 : (c + 1) * 128] = total
            sums = sums + total
            squares = squares + total * total
        first = jnp.sum(sums, axis=1, keepdims=True)
        second = jnp.sum(squares, axis=1, keepdims=True)
        lane = lax.broadcasted_iota(jnp.int32, (128, 128), 1)
        stat_own[pl.ds(base, 128), :] = jnp.where(lane == 0, first, second)

    chunks = rows // 128

    def conv_loop(i, carry):
        conv_chunk(i)

        @pl.when((i == chunks // 2) & jnp.logical_not(at_end))
        def _():
            pass_on(2, 2)

        @pl.when(i == chunks - 3)
        def _():
            join_near()

        @pl.when(i == chunks - 1)
        def _():
            for k in (1, 2, 3):
                @pl.when(z + k <= 3)
                def _():
                    far_end(k).start()

        return carry

    lax.fori_loop(1, chunks, conv_loop, 0)

    @pl.when(at_end)
    def _():
        pass_on(2, 2)

    arrived(2, m.piece(0))
    slab(acc3, w3, m.piece(0), True)
    pass_on(3, 1)
    own_last(3)
    arrived(2, m.piece(1))
    slab(acc3, w3, m.piece(1), False)
    arrived(2, m.piece(2))
    slab(acc3, w3, m.piece(2), False)
    arrived(2, m.piece(3))
    slab(acc3, w3, m.piece(3), False)
    @pl.when(me > 0)
    def _():
        halo.wait_recv()
        for c in range(n_conv // 128):
            seq[c, 0:pad, :] = halo_in[:, c * 128 : (c + 1) * 128].astype(jnp.float32)

    @pl.when(me == 0)
    def _():
        seq[:, 0:pad, :] = jnp.zeros((n_conv // 128, pad, 128), jnp.float32)

    lax.fori_loop(0, 1, conv_loop, 0)

    stats = m.copy(stat_own, stat_in, misc_send.at[2], misc_recv.at[2], me, 1 - tp)

    def conv_finish(i, carry):
        at = pl.ds(pl.multiple_of(i * 128, 128), 128)
        both_stats = stat_own[at, :] + stat_in[at, :]
        mean_val = both_stats[:, 0:1] / (2 * n_conv)
        square_mean = both_stats[:, 1:2] / (2 * n_conv)
        scale = lax.rsqrt(square_mean - mean_val * mean_val + epsilon)
        value = (acc2[at, 0:n_conv] - mean_val) * scale * conv_gain[...]
        act[at, 0:n_conv] = (value * jax.nn.sigmoid(value)).astype(jnp.bfloat16)
        return carry

    stats.start()

    @pl.when(jnp.logical_not(at_end))
    def _():
        pass_on(3, 2)

    stats.wait_recv()
    lax.fori_loop(0, chunks, conv_finish, 0)
    pass_on(2, 3)

    for k in (1, 2, 3):
        @pl.when(z - k >= 0)
        def _():
            end_copy(4, 4 + k, 2 + k, me).wait_recv()
            pre = join(read(4 + k), (before[HV : HV + 1, :], before[0:HV, :]))
            before[0:HV, :] = pre[1]
            before[HV:, :] = jnp.broadcast_to(pre[0], (8, n_key))

    entry = jnp.concatenate([init[h].T for h in range(heads)], axis=1)
    state[...] = entry * before[HV : HV + 1, :] + before[0:HV, :]

    def gla_finish(i, carry):
        at = pl.ds(pl.multiple_of(i * 256, 256), 256)
        entering = state[...].astype(jnp.bfloat16)
        for h in range(heads):
            ks, vs = slice(h * HK, (h + 1) * HK), slice(h * HV, (h + 1) * HV)
            value = attn[at, vs] + dot(since[at, ks], entering[:, ks], ((1,), (1,)))
            value = value * lax.rsqrt(jnp.mean(value * value, axis=-1, keepdims=True) + epsilon) * head_gain[...]
            gate = acc3[at, vs].astype(jnp.bfloat16).astype(jnp.float32)
            act[at, n_conv + h * HV : n_conv + (h + 1) * HV] = (value * (gate * jax.nn.sigmoid(gate))).astype(jnp.bfloat16)
        return carry

    lax.fori_loop(0, rows // 256, gla_finish, 0)

    def part_copy(b):
        at = pl.ds(pl.multiple_of(b * 256, 256), 256)
        return m.copy(psend.at[b], other_out.at[:, at], part_send, part_recv, me, 1 - tp)

    def project(p, yy, core):
        weight = jnp.concatenate([wo[p, yy, 0], wo[p, yy, 1]], axis=1)
        left = act[pl.ds(pl.multiple_of(core * half, half), half), :]
        return dot(left, weight, ((1,), (0,))).astype(jnp.bfloat16)

    def out_pieces(j):
        p = m.piece(j)

        def theirs(yy, carry):
            psend[p * 2 + yy] = project(p, yy, 1 - tp)
            return carry

        def ours(yy, carry):
            part_copy(p * 2 + yy).start()
            own_out[:, pl.ds(pl.multiple_of((p * 2 + yy) * 256, 256), 256)] = project(p, yy, tp)
            return carry

        arrived(3, p)
        arrived(4, p)
        lax.fori_loop(0, 2, theirs, 0)
        lax.fori_loop(0, 2, ours, 0)

    def rows_of(core):
        return pl.ds(pl.multiple_of(core * half, half), half)

    def last_part(yy, low, high):
        p = m.piece(3)
        weight = jnp.concatenate([wo[p, yy, 0, low:high, :], wo[p, yy, 1, low:high, :]], axis=1)
        return lambda core: dot(act[rows_of(core), low:high], weight, ((1,), (0,)))

    def last_begin():
        def body(yy, carry):
            part = last_part(yy, 0, 2 * early)
            at = pl.ds(pl.multiple_of(yy * 256, 256), 256)
            acc2[0:half, at] = part(1 - tp)
            acc2[half:, at] = part(tp)
            return carry

        arrived(3, m.piece(3))
        lax.fori_loop(0, 2, body, 0)

    def last_end():
        b = m.piece(3) * 2

        def theirs(yy, carry):
            at = pl.ds(pl.multiple_of(yy * 256, 256), 256)
            part = last_part(yy, 2 * early, 2 * early + 2 * late)
            psend[b + yy] = (acc2[0:half, at] + part(1 - tp)).astype(jnp.bfloat16)
            return carry

        def ours(yy, carry):
            part_copy(b + yy).start()
            at = pl.ds(pl.multiple_of(yy * 256, 256), 256)
            part = last_part(yy, 2 * early, 2 * early + 2 * late)
            own_out[:, pl.ds(pl.multiple_of((b + yy) * 256, 256), 256)] = (acc2[half:, at] + part(tp)).astype(jnp.bfloat16)
            return carry

        arrived(4, m.piece(3))
        lax.fori_loop(0, 2, theirs, 0)
        lax.fori_loop(0, 2, ours, 0)

    def drain_early():
        swap.wait_send()
        stats.wait_send()

        @pl.when(me < 15)
        def _():
            halo.wait_send()

        for end in near_ends:
            end.wait_send()
        for k in (1, 2, 3):
            @pl.when(z + k <= 3)
            def _():
                far_end(k).wait_send()

        for f in (b1, b2, *pairs[0], *pairs[1]):
            f.drain_first()
            f.drain_last()
        for f in (*pairs[2], *pairs[3]):
            f.drain_first()
        whole.drain()
        for pair in lines:
            for line in pair:
                line.drain()

    out_pieces(0)

    @pl.when(at_end)
    def _():
        pass_on(3, 2)

    out_pieces(1)
    pass_on(3, 3)
    last_begin()
    out_pieces(2)
    drain_early()
    last_end()

    for f in (*pairs[2], *pairs[3]):
        f.drain_last()
    m.copy(psend, psend, part_send, part_recv, me, 1 - tp).wait_send()
    m.copy(other_out, other_out, part_send, part_recv, me, 1 - tp).wait_recv()


def fused_layer(
    tokens, norm_gain, w_conv_a, w_conv_gate, conv_weight, conv_gain, w_query, w_key, w_value, w_outgate,
    w_decay, decay_bias, decay_extra, head_gain, init_state, w_out_conv, w_out_gla,
):
    rows, width = tokens.shape
    depth = w_query.shape[0]
    n_key = w_query.shape[1]
    n_conv = w_conv_a.shape[1]
    cols = w_out_conv.shape[1]
    half = rows // 2
    pad = 32
    bf16, f32 = jnp.bfloat16, jnp.float32
    dma = pltpu.SemaphoreType.DMA
    vm = pl.BlockSpec(memory_space=pltpu.VMEM)
    hbm = pl.BlockSpec(memory_space=pl.ANY)
    share = pltpu.VMEM((half, 2 * width), bf16)
    own, other = pl.pallas_call(
        layer_kernel,
        out_shape=[share, share],
        in_specs=[hbm, vm, hbm, hbm, vm, vm, hbm, hbm, hbm, hbm, hbm, vm, hbm, vm, vm, hbm, hbm],
        out_specs=[vm, vm],
        scratch_shapes=[
            pltpu.VMEM((4, 2, 2, depth, 5 * n_key), bf16),
            pltpu.VMEM((4, 2, 2, depth, 2 * n_conv), bf16),
            pltpu.VMEM((4, 2, 2, depth, n_conv), bf16),
            pltpu.VMEM((4, 2, 2, 2 * n_conv, cols), bf16),
            pltpu.VMEM((2, rows, width), bf16),
            pltpu.VMEM((rows, 2 * width), bf16),
            pltpu.VMEM((rows, 5 * n_key), f32),
            pltpu.VMEM((rows, 2 * n_conv), f32),
            pltpu.VMEM((rows, n_conv), f32),
            pltpu.VMEM((rows, n_key), f32),
            pltpu.VMEM((n_conv // 128, rows + pad, 128), f32),
            pltpu.VMEM((rows, n_conv), f32),
            pltpu.VMEM((rows, n_key), bf16),
            pltpu.VMEM((rows, 2 * n_conv), bf16),
            pltpu.VMEM((8, half, 256), bf16),
            pltpu.VMEM((pad, n_conv), bf16),
            pltpu.VMEM((pad, n_conv), bf16),
            pltpu.VMEM((rows, 128), f32),
            pltpu.VMEM((rows, 128), f32),
            pltpu.VMEM((8, HV + 16, n_key), bf16),
            pltpu.VMEM((HV, n_key), f32),
            pltpu.VMEM((1, n_key), f32),
            pltpu.VMEM((HV + 8, n_key), f32),
            dma((11,)), dma((10,)), dma((16,)), dma((10,)), dma((5, 4)), dma((9, 5)), dma((9, 4)),
            dma((3,)), dma((3,)), dma((6,)), dma((8,)), dma(()), dma(()),
        ],
        compiler_params=pltpu.CompilerParams(collective_id=0, has_side_effects=True, vmem_limit_bytes=56 * 2**20),
        name="layer",
    )(
        tokens, norm_gain[None, :], w_conv_a, w_conv_gate, conv_weight, conv_gain[None, :], w_query, w_key, w_value,
        w_outgate, w_decay, decay_bias[None, :], decay_extra, head_gain[None, :], init_state, w_out_conv, w_out_gla,
    )
    return (own.astype(f32) + other.astype(f32)).astype(bf16)


def local_kernel(heads, pieces, q_ref, k_ref, v_ref, pre_ref, extra_ref, bias_ref, attn_ref, since_ref, end_ref, log_ref, state, prefix):
    step = pl.program_id(0)

    @pl.when(step == 0)
    def _():
        state[...] = jnp.zeros_like(state)
        prefix[...] = jnp.zeros_like(prefix)

    rows = lax.broadcasted_iota(jnp.int32, (BLOCK, BLOCK), 0)
    columns = lax.broadcasted_iota(jnp.int32, (BLOCK, BLOCK), 1)
    causal = rows >= columns
    lower = causal.astype(jnp.float32)
    for piece in range(pieces):
        at = pl.ds(piece * BLOCK, BLOCK)
        pre = pre_ref[at, :] + bias_ref[...]
        logs = jax.nn.log_sigmoid(pre) / gate_divisor + extra_ref[at, :]
        cum = lax.dot_general(
            lower, logs, (((1,), (0,)), ((), ())), precision=lax.Precision.HIGHEST, preferred_element_type=jnp.float32
        )
        total = cum[BLOCK - 1 :, :]
        middle = cum[BLOCK // 2 - 1 : BLOCK // 2, :]
        query = q_ref[at, :].astype(jnp.float32) * HK ** (-0.5)
        keys = k_ref[at, :].astype(jnp.float32)
        decayed = query * jnp.exp(cum)
        since_ref[at, :] = (decayed * jnp.exp(prefix[...])).astype(jnp.bfloat16)
        decayed = decayed.astype(jnp.bfloat16)
        query = (query * jnp.exp(cum - middle)).astype(jnp.bfloat16)
        inverse = (keys * jnp.exp(middle - cum)).astype(jnp.bfloat16)
        to_end = (keys * jnp.exp(total - cum)).astype(jnp.bfloat16)
        entering = state[...].astype(jnp.bfloat16)
        added = []
        for h in range(heads):
            ks, vs = slice(h * HK, (h + 1) * HK), slice(h * HV, (h + 1) * HV)
            values = v_ref[at, vs]
            scores = jnp.where(causal, dot(query[:, ks], inverse[:, ks], ((1,), (1,))), 0.0)
            attn_ref[at, vs] = dot(scores.astype(jnp.bfloat16), values, ((1,), (0,))) + dot(
                decayed[:, ks], entering[:, ks], ((1,), (1,))
            )
            added.append(dot(values, to_end[:, ks], ((0,), (0,))))
        added = added[0] if heads == 1 else jnp.concatenate(added, axis=1)
        state[...] = state[...] * jnp.exp(total) + added
        prefix[...] = prefix[...] + total
    end_ref[...] = state[...]
    log_ref[...] = prefix[...]


def gla_local(query, keys, values, decay_pre, decay_extra, decay_bias):
    rows, width = query.shape
    heads = width // HK
    pieces = 4
    tile = pieces * BLOCK

    def tiled(array):
        return pl.BlockSpec((tile, array.shape[1]), lambda i: (i, 0))

    def whole(shape):
        return pl.BlockSpec(shape, lambda i: (0, 0))

    return pl.pallas_call(
        functools.partial(local_kernel, heads, pieces),
        grid=(rows // tile,),
        in_specs=[tiled(query), tiled(keys), tiled(values), tiled(decay_pre), tiled(decay_extra), whole((1, width))],
        out_specs=[tiled(values), tiled(query), whole((HV, width)), whole((1, width))],
        out_shape=[
            jax.ShapeDtypeStruct(values.shape, jnp.float32),
            jax.ShapeDtypeStruct(query.shape, jnp.bfloat16),
            jax.ShapeDtypeStruct((HV, width), jnp.float32),
            jax.ShapeDtypeStruct((1, width), jnp.float32),
        ],
        scratch_shapes=[pltpu.VMEM((HV, width), jnp.float32), pltpu.VMEM((1, width), jnp.float32)],
        cost_estimate=pl.CostEstimate(flops=10**10, bytes_accessed=10**7, transcendentals=10**6),
        name="gla_local",
    )(query, keys, values, decay_pre, decay_extra, decay_bias[None, :])


def finish_kernel(heads, size, where_ref, attn_ref, since_ref, gate_ref, ends_ref, init_ref, gain_ref, out_ref, state):
    me = where_ref[0]

    @pl.when(pl.program_id(0) == 0)
    def _():
        state[...] = init_ref[...]

        def one(device, carry):
            at = device
            decay = ends_ref[pl.ds(pl.multiple_of(at * size + HV, 16), 16), :].astype(jnp.float32)[:1]
            end = ends_ref[pl.ds(pl.multiple_of(at * size, 16), HV), :].astype(jnp.float32)
            state[...] = state[...] * decay + end
            return carry

        lax.fori_loop(0, me, one, 0)

    entering = state[...].astype(jnp.bfloat16)
    for h in range(heads):
        ks, vs = slice(h * HK, (h + 1) * HK), slice(h * HV, (h + 1) * HV)
        attn = attn_ref[:, vs] + dot(since_ref[:, ks], entering[:, ks], ((1,), (1,)))
        attn = attn * lax.rsqrt(jnp.mean(attn * attn, axis=-1, keepdims=True) + epsilon) * gain_ref[...]
        gate = gate_ref[:, vs].astype(jnp.float32)
        out_ref[:, vs] = (attn * (gate * jax.nn.sigmoid(gate))).astype(jnp.bfloat16)


def gla_finish(attn, since, out_gate, ends, init_state, head_gain, me):
    rows, width = since.shape
    heads = width // HK
    tile = 256

    def tiled(array):
        return pl.BlockSpec((tile, array.shape[1]), lambda i, w: (i, 0))

    def whole(array):
        return pl.BlockSpec(array.shape, lambda i, w: (0, 0))

    init = init_state.transpose(2, 0, 1).reshape(HV, width)
    gain = head_gain[None, :]
    return pl.pallas_call(
        functools.partial(finish_kernel, heads, HV + 16),
        grid_spec=pltpu.PrefetchScalarGridSpec(
            num_scalar_prefetch=1,
            grid=(rows // tile,),
            in_specs=[tiled(attn), tiled(since), tiled(out_gate), whole(ends), whole(init), whole(gain)],
            out_specs=tiled(attn),
            scratch_shapes=[pltpu.VMEM((HV, width), jnp.float32)],
        ),
        out_shape=jax.ShapeDtypeStruct(attn.shape, jnp.bfloat16),
        cost_estimate=pl.CostEstimate(flops=3 * 10**9, bytes_accessed=10**7, transcendentals=10**6),
        name="gla_finish",
    )(me[None], attn, since, out_gate, ends, init, gain)


def conv_branch(gated, conv_weight, conv_gain):
    taps = conv_weight.shape[0]
    row_count = gated.shape[0]
    count = lax.axis_size("sp")
    earlier = lax.ppermute(gated[row_count - taps + 1 :], "sp", [(i, i + 1) for i in range(count - 1)])
    extended = jnp.concatenate([earlier, gated], axis=0).astype(jnp.float32)
    conv_sum = jnp.zeros(gated.shape, jnp.float32)
    for tap in range(taps):
        conv_sum = conv_sum + conv_weight[tap][None, :] * extended[tap : tap + row_count]
    row_sums, row_squares = lax.psum((jnp.sum(conv_sum, axis=1), jnp.sum(conv_sum * conv_sum, axis=1)), "tp")
    mean_val = (row_sums / D_CONV)[:, None]
    square_mean = (row_squares / D_CONV)[:, None]
    conv_norm = (conv_sum - mean_val) * lax.rsqrt(square_mean - mean_val * mean_val + epsilon) * conv_gain
    return jax.nn.silu(conv_norm).astype(jnp.bfloat16)


def project(hidden, weight):
    return dot(hidden, weight, ((1,), (0,)))


def plain_layer(
    tokens, norm_gain, w_conv_a, w_conv_gate, conv_weight, conv_gain, w_query, w_key, w_value, w_outgate,
    w_decay, decay_bias, decay_extra, head_gain, init_state, w_out_conv, w_out_gla,
):
    me = lax.axis_index("sp")

    def gather(shard):
        return lax.all_gather(shard, "sp", axis=0, tiled=True)

    widened = lax.all_gather(tokens, "tp", axis=1, tiled=True).astype(jnp.float32)
    normed = (
        widened * lax.rsqrt(jnp.mean(widened * widened, axis=-1, keepdims=True) + epsilon) * norm_gain
    ).astype(jnp.bfloat16)
    half = w_query.shape[1]
    conv_a = project(normed, gather(w_conv_a)).astype(jnp.bfloat16)
    conv_gate = project(normed, gather(w_conv_gate)).astype(jnp.bfloat16)
    full_qkd = gather(jnp.concatenate([w_query, w_key, w_decay], axis=1))
    full_v = gather(w_value)
    gated = (conv_a.astype(jnp.float32) * jax.nn.sigmoid(conv_gate.astype(jnp.float32))).astype(jnp.bfloat16)
    conv_out = conv_branch(gated, conv_weight, conv_gain)
    query_keys = project(normed, full_qkd[:, : 2 * half]).astype(jnp.bfloat16)
    decay_pre = project(normed, full_qkd[:, 2 * half :])
    values = project(normed, full_v).astype(jnp.bfloat16)
    attn, since, end, end_log = gla_local(
        query_keys[:, :half], query_keys[:, half:], values, decay_pre, decay_extra, decay_bias
    )
    packed = jnp.concatenate([end, jnp.broadcast_to(jnp.exp(end_log), (16, half))], axis=0).astype(jnp.bfloat16)
    ends = gather(packed)
    out_gate = project(normed, gather(w_outgate)).astype(jnp.bfloat16)
    gla_out = gla_finish(attn, since, out_gate, ends, init_state, head_gain, me)
    total = dot(conv_out, gather(w_out_conv.T), ((1,), (1,))) + dot(gla_out, gather(w_out_gla.T), ((1,), (1,)))
    return lax.psum_scatter(total.astype(jnp.bfloat16), "tp", scatter_dimension=0, tiled=True)


def per_device(*arrays):
    if folded(lax.axis_size("sp"), lax.axis_size("tp")):
        return fused_layer(*arrays)
    return plain_layer(*arrays)


def solution(mesh):
    placed = (
        P("sp", "tp"), P(), P("sp", "tp"), P("sp", "tp"), P(None, "tp"), P("tp"), P("sp", "tp"), P("sp", "tp"),
        P("sp", "tp"), P("sp", "tp"), P("sp", "tp"), P("tp"), P("sp", "tp"), P(), P("tp", None, None),
        P("tp", "sp"), P("tp", "sp"),
    )
    return jax.shard_map(
        per_device, mesh=mesh, in_specs=placed, out_specs=P(("sp", "tp"), None), check_vma=False
    )
```

```python
import functools

import jax
import jax.numpy as jnp
from jax import lax
from jax.experimental import pallas as pl
from jax.experimental.pallas import tpu as pltpu
from jax.sharding import PartitionSpec as P

D_CONV = 1024
HK = 64
HV = 128
BLOCK = 64

epsilon = 1e-06
gate_divisor = 16.0

MESH = pl.DeviceIdType.MESH


def dot(a, b, dims):
    return lax.dot_general(a, b, (dims, ((), ())), preferred_element_type=jnp.float32)


def folded(n_sp, n_tp):
    return n_sp == 16 and n_tp == 2


class Mover:
    def __init__(self):
        self.me = lax.axis_index("sp")
        self.tp = lax.axis_index("tp")
        self.z, self.y, self.x = self.me // 4, (self.me // 2) % 2, self.me % 2
        self.other = {"x": self.me + 1 - 2 * self.x, "y": self.me + 2 - 4 * self.y}
        self.across = self.me + 3 - 2 * self.x - 4 * self.y
        self.sent = []

    def copy(self, source, target, send, recv, place, core=None):
        core = self.tp if core is None else core
        return pltpu.make_async_remote_copy(
            src_ref=source, dst_ref=target, send_sem=send, recv_sem=recv, device_id=(place, core), device_id_type=MESH
        )

    def piece(self, j):
        z = self.z
        return (z, z + 1 - 2 * (z % 2), 2 - z // 2, 3 - 3 * (z // 2))[j]


class Flow:
    def __init__(self, mover, number, view, first, sems):
        self.m, self.number, self.view, self.first = mover, number, view, first
        self.last = {"x": "y", "y": "x"}[first]
        self.sems = sems

    def own(self, p):
        return self.view(p, self.m.y, self.m.x)

    def pair(self, p):
        every = slice(None)
        return self.view(p, self.m.y, every) if self.first == "x" else self.view(p, every, self.m.x)

    def first_copy(self, p, source=None):
        own = self.own(p) if source is None else source
        slot = self.number * 4 + p if self.number < 2 else self.number + 6
        fs, fr = self.sems["first_send"], self.sems["first_recv"]
        return self.m.copy(own, own, fs.at[self.number], fr.at[slot], self.m.other[self.first])

    def last_copy(self, p, source=None):
        pair = self.pair(p) if source is None else source
        ls, lr = self.sems["last_send"], self.sems["last_recv"]
        return self.m.copy(pair, pair, ls.at[self.number], lr.at[self.number // 2, p], self.m.other[self.last])

    def drain_first(self):
        if self.number < 2:
            self.first_copy(0, self.own(slice(None))).wait_send()
        else:
            self.first_copy(self.m.z).wait_send()

    def drain_last(self):
        self.last_copy(0, self.pair(slice(None))).wait_send()


class Line:
    def __init__(self, mover, number, view, sems):
        self.m, self.number, self.view, self.sems = mover, number, view, sems

    def up(self, p):
        return self.m.copy(
            self.view(p), self.view(p), self.sems["z_send"].at[self.number, p], self.sems["z_recv"].at[self.number, p],
            self.m.me + 4,
        )

    def down(self, p):
        return self.m.copy(
            self.view(p), self.view(p), self.sems["z_send"].at[self.number, p + 1],
            self.sems["z_recv"].at[self.number, p], self.m.me - 4,
        )

    def start_own(self):
        z = self.m.z

        @pl.when(z < 3)
        def _():
            self.up(z).start()

        @pl.when(z > 0)
        def _():
            self.down(z).start()

    def relay(self, step, then):
        z = self.m.z

        @pl.when(z >= step)
        def _():
            p = z - step
            self.up(p).wait_recv()

            @pl.when(z < 3)
            def _():
                self.up(p).start()

            then(p)

        @pl.when(z + step <= 3)
        def _():
            p = z + step
            self.down(p).wait_recv()

            @pl.when(z > 0)
            def _():
                self.down(p).start()

            then(p)

    def drain(self):
        z = self.m.z
        for p in range(4):
            @pl.when((p <= z) & (z < 3))
            def _():
                self.up(p).wait_send()

            @pl.when((p >= z) & (z > 0))
            def _():
                self.down(p).wait_send()


def at_step(z, step, then):
    if step == 0:
        then(z)
        return

    @pl.when(z >= step)
    def _():
        then(z - step)

    @pl.when(z + step <= 3)
    def _():
        then(z + step)


def layer_kernel(
    tokens, gain, wa, wg, taps, conv_gain, wq, wk, wv, wog, wd, bias, extra_in, head_gain, init, woc, wogl, own_out, other_out,
    w1, w2, w3, wo, both, normed, acc1, acc2, acc3, extra, seq, attn, since, act, psend,
    halo_out, halo_in, stat_own, stat_in, packs, state, prefix, before,
    local, first_send, first_recv, last_send, last_recv, z_send, z_recv, misc_send, misc_recv, end_send, end_recv,
    part_send, part_recv,
):
    m = Mover()
    me, tp, z, y, x = m.me, m.tp, m.z, m.y, m.x
    rows = normed.shape[0]
    half = rows // 2
    width = both.shape[2]
    n_key = acc1.shape[1] // 5
    n_conv = 2 * n_key
    heads = n_key // HK
    sems = dict(
        first_send=first_send, first_recv=first_recv, last_send=last_send, last_recv=last_recv,
        z_send=z_send, z_recv=z_recv,
    )

    def lanes(ref, low, size):
        return lambda p, yy, xx: ref.at[p, yy, xx, :, pl.ds(low, size)]

    def depth(low, size):
        return lambda p, yy, xx: wo.at[p, yy, xx, pl.ds(low, size), :]

    mid = w1.shape[-1] // 2
    late = wo.shape[3] // 4
    early = wo.shape[3] // 2 - late
    b1 = Flow(m, 0, lanes(w1, 0, mid), "x", sems)
    b2 = Flow(m, 1, lanes(w1, mid, mid), "y", sems)
    pairs = [
        (Flow(m, 2, lanes(w2, 0, n_conv), "x", sems), Flow(m, 3, lanes(w2, n_conv, n_conv), "y", sems)),
        (Flow(m, 4, lanes(w3, 0, n_key), "x", sems), Flow(m, 5, lanes(w3, n_key, n_key), "y", sems)),
        (Flow(m, 6, depth(0, early), "x", sems), Flow(m, 7, depth(early, early), "y", sems)),
        (Flow(m, 8, depth(2 * early, late), "x", sems), Flow(m, 9, depth(2 * early + late, late), "y", sems)),
    ]
    whole = Line(m, 0, lambda p: w1.at[p, y, x], sems)
    lines = [tuple(Line(m, f.number - 1, f.pair, sems) for f in pair) for pair in pairs]

    loads = [
        (wq, w1.at[z, y, x, :, pl.ds(0, n_key)]),
        (wk, w1.at[z, y, x, :, pl.ds(n_key, n_key)]),
        (wd, w1.at[z, y, x, :, pl.ds(2 * n_key, n_key)]),
        (wv, w1.at[z, y, x, :, pl.ds(3 * n_key, n_conv)]),
        (wa, w2.at[z, y, x, :, pl.ds(0, n_conv)]),
        (wg, w2.at[z, y, x, :, pl.ds(n_conv, n_conv)]),
        (wog, w3.at[z, y, x]),
        (woc, wo.at[z, y, x, pl.ds(0, n_conv), :]),
        (wogl, wo.at[z, y, x, pl.ds(n_conv, n_conv), :]),
        (tokens, both.at[tp]),
        (extra_in, extra),
    ]
    loads = [pltpu.make_async_copy(a, b, local.at[i]) for i, (a, b) in enumerate(loads)]
    for load in loads:
        load.start()

    barrier = pltpu.get_barrier_semaphore()
    def greet(place, core):
        pl.semaphore_signal(barrier, inc=1, device_id=(place, core), device_id_type=MESH)

    for place, core in ((m.other["x"], tp), (m.other["y"], tp), (me, 1 - tp)):
        greet(place, core)

    @pl.when(z < 3)
    def _():
        greet(me + 4, tp)

    @pl.when(z > 0)
    def _():
        greet(me - 4, tp)

    at_end = (z == 0) | (z == 3)

    @pl.when(at_end)
    def _():
        pl.semaphore_wait(barrier, 4)

    @pl.when(jnp.logical_not(at_end))
    def _():
        pl.semaphore_wait(barrier, 5)

    for i in range(4):
        loads[i].wait()
    whole.start_own()
    b1.first_copy(z).start()
    b2.first_copy(z).start()
    loads[9].wait()
    swap = m.copy(both.at[tp], both.at[tp], misc_send.at[0], misc_recv.at[0], me, 1 - tp)
    swap.start()
    loads[4].wait()
    loads[5].wait()
    for f in pairs[0]:
        f.first_copy(z).start()
    loads[6].wait()
    for f in pairs[1]:
        f.first_copy(z).start()
    for i in (7, 8, 10):
        loads[i].wait()

    def head_firsts(step):
        def one(p):
            b1.first_copy(p).wait_recv()
            b1.last_copy(p).start()
            b2.first_copy(p).wait_recv()
            b2.last_copy(p).start()

        at_step(z, step, one)

    def head_line(step):
        def then(p):
            b1.first_copy(p).start()
            b2.first_copy(p).start()

        whole.relay(step, then)

    def begin(k):
        for f in pairs[k]:
            f.first_copy(z).start()

    def enter_one(k, i):
        pairs[k][i].first_copy(z).wait_recv()
        lines[k][i].start_own()

    def enter(k):
        enter_one(k, 0)
        enter_one(k, 1)

    def own_last(k):
        for f in pairs[k]:
            f.last_copy(z).start()

    def pass_on(k, step):
        for f, line in zip(pairs[k], lines[k]):
            line.relay(step, lambda p: f.last_copy(p).start())

    def relay_only(k, step):
        for line in lines[k]:
            line.relay(step, lambda p: None)

    def finish(k, step):
        for f in pairs[k]:
            at_step(z, step, lambda p: f.last_copy(p).start())

    def arrived(k, p):
        every = (p, slice(None), slice(None))
        both_flows = (
            w1.at[(*every, slice(None), pl.ds(0, mid))],
            w2.at[(*every, slice(None), pl.ds(0, n_conv))],
            w3.at[(*every, slice(None), pl.ds(0, n_key))],
            wo.at[(*every, pl.ds(0, early), slice(None))],
            wo.at[(*every, pl.ds(0, late), slice(None))],
        )[k]
        flow = b1 if k == 0 else pairs[k - 1][0]
        flow.last_copy(p, both_flows).wait_recv()

    def norm_tiles(low, high):
        def body(i, carry):
            at = pl.ds(pl.multiple_of(i * 128, 128), 128)
            a = both[0, at, :].astype(jnp.float32)
            b = both[1, at, :].astype(jnp.float32)
            square = jnp.sum(a * a + b * b, axis=1, keepdims=True)
            scale = lax.rsqrt(square / (2 * width) + epsilon)
            normed[at, :width] = (a * scale * gain[:, :width]).astype(jnp.bfloat16)
            normed[at, width:] = (b * scale * gain[:, width:]).astype(jnp.bfloat16)
            return carry

        lax.fori_loop(low, high, body, 0)

    def slab(acc, ref, p, first):
        size = ref.shape[1] * ref.shape[2] * ref.shape[3]

        def body(c, carry):
            at = pl.ds(pl.multiple_of(c * 256, 256), 256)
            left = normed[:, pl.ds(pl.multiple_of(p * size, size), size)]
            right = ref[p, :, :, :, at].reshape(size, 256)
            got = dot(left, right, ((1,), (0,)))
            if first:
                acc[:, at] = got
            else:
                acc[:, at] += got
            return carry

        lax.fori_loop(0, acc.shape[1] // 256, body, 0)

    swap.wait_recv()
    norm_tiles(0, 4)
    head_line(1)
    head_firsts(0)
    norm_tiles(4, 8)
    enter_one(0, 0)
    head_line(2)
    enter_one(0, 1)
    head_firsts(1)
    head_line(3)
    arrived(0, m.piece(0))
    slab(acc1, w1, m.piece(0), True)
    head_firsts(2)
    begin(2)
    begin(3)
    pass_on(0, 1)
    arrived(0, m.piece(1))
    slab(acc1, w1, m.piece(1), False)
    head_firsts(3)
    enter(1)
    own_last(0)
    pass_on(0, 2)
    arrived(0, m.piece(2))
    slab(acc1, w1, m.piece(2), False)
    pass_on(1, 1)
    enter(2)
    arrived(0, m.piece(3))
    slab(acc1, w1, m.piece(3), False)

    state[...] = jnp.zeros_like(state)
    prefix[...] = jnp.zeros_like(prefix)
    r_iota = lax.broadcasted_iota(jnp.int32, (BLOCK, BLOCK), 0)
    c_iota = lax.broadcasted_iota(jnp.int32, (BLOCK, BLOCK), 1)
    causal = r_iota >= c_iota
    lower = causal.astype(jnp.float32)

    def block(i, carry):
        at = pl.ds(pl.multiple_of(i * BLOCK, BLOCK), BLOCK)
        pre = acc1[at, 2 * n_key : 3 * n_key] + bias[...]
        logs = jax.nn.log_sigmoid(pre) / gate_divisor + extra[at, :]
        cum = lax.dot_general(
            lower, logs, (((1,), (0,)), ((), ())), precision=lax.Precision.HIGHEST, preferred_element_type=jnp.float32
        )
        total = cum[BLOCK - 1 :, :]
        middle = cum[BLOCK // 2 - 1 : BLOCK // 2, :]
        query = acc1[at, 0:n_key].astype(jnp.bfloat16).astype(jnp.float32) * HK ** (-0.5)
        keys = acc1[at, n_key : 2 * n_key].astype(jnp.bfloat16).astype(jnp.float32)
        decayed = query * jnp.exp(cum)
        since[at, :] = (decayed * jnp.exp(prefix[...])).astype(jnp.bfloat16)
        decayed = decayed.astype(jnp.bfloat16)
        query = (query * jnp.exp(cum - middle)).astype(jnp.bfloat16)
        inverse = (keys * jnp.exp(middle - cum)).astype(jnp.bfloat16)
        to_end = (keys * jnp.exp(total - cum)).astype(jnp.bfloat16)
        entering = state[...].astype(jnp.bfloat16)
        added = []
        for h in range(heads):
            ks, vs = slice(h * HK, (h + 1) * HK), slice(h * HV, (h + 1) * HV)
            values = acc1[at, 3 * n_key + h * HV : 3 * n_key + (h + 1) * HV].astype(jnp.bfloat16)
            scores = jnp.where(causal, dot(query[:, ks], inverse[:, ks], ((1,), (1,))), 0.0)
            attn[at, vs] = dot(scores.astype(jnp.bfloat16), values, ((1,), (0,))) + dot(
                decayed[:, ks], entering[:, ks], ((1,), (1,))
            )
            added.append(dot(values, to_end[:, ks], ((0,), (0,))))
        state[...] = state[...] * jnp.exp(total) + jnp.concatenate(added, axis=1)
        prefix[...] = prefix[...] + total
        return carry

    blocks = rows // BLOCK

    def attend(i, carry):
        block(i, 0)

        @pl.when(i == blocks // 2)
        def _():
            pass_on(0, 3)

        @pl.when(i == blocks - 3)
        def _():
            relay_only(1, 2)

        return carry

    lax.fori_loop(0, blocks, attend, 0)

    def pack(slot, decay, end):
        packs[slot, 0:HV, :] = end.astype(jnp.bfloat16)
        packs[slot, HV:, :] = jnp.broadcast_to(decay, (16, n_key)).astype(jnp.bfloat16)

    def read(slot):
        return packs[slot, HV : HV + 1, :].astype(jnp.float32), packs[slot, 0:HV, :].astype(jnp.float32)

    def end_copy(source, target, number, place):
        return m.copy(packs.at[source], packs.at[target], end_send.at[number], end_recv.at[target], place)

    def join(early, late):
        return early[0] * late[0], early[1] * late[0] + late[1]

    near_ends = [
        end_copy(0, 1, 0, m.other["x"]),
        end_copy(0, 2, 1, m.other["y"]),
        end_copy(0, 3, 2, m.across),
    ]
    pack(0, jnp.exp(prefix[...]), state[...])

    arrived(1, m.piece(0))
    slab(acc2, w2, m.piece(0), True)
    for end in near_ends:
        end.start()
    own_last(1)
    finish(1, 2)
    pass_on(2, 1)
    enter(3)
    arrived(1, m.piece(1))
    slab(acc2, w2, m.piece(1), False)
    arrived(1, m.piece(2))
    slab(acc2, w2, m.piece(2), False)
    arrived(1, m.piece(3))
    slab(acc2, w2, m.piece(3), False)
    pass_on(1, 3)
    own_last(2)

    def join_near():
        for end in near_ends:
            end.wait_recv()
        run = (jnp.ones((1, n_key), jnp.float32), jnp.zeros((HV, n_key), jnp.float32))
        pre = run
        for yy in range(2):
            for xx in range(2):
                past = yy * 2 + xx < y * 2 + x
                run = join(run, read((y + yy - 2 * y * yy) * 2 + x + xx - 2 * x * xx))
                pre = jnp.where(past, run[0], pre[0]), jnp.where(past, run[1], pre[1])
        before[0:HV, :] = pre[1]
        before[HV:, :] = jnp.broadcast_to(pre[0], (8, n_key))
        pack(4, *run)

    def far_end(k):
        return end_copy(4, 4 + k, 2 + k, me + 4 * k)

    pad = seq.shape[1] - rows

    def gate_tiles(low, high):
        def body(i, carry):
            at = pl.ds(pl.multiple_of(i * 128, 128), 128)
            for c in range(n_conv // 128):
                a = acc2[at, c * 128 : (c + 1) * 128].astype(jnp.bfloat16).astype(jnp.float32)
                g = acc2[at, n_conv + c * 128 : n_conv + (c + 1) * 128].astype(jnp.bfloat16).astype(jnp.float32)
                value = (a * jax.nn.sigmoid(g)).astype(jnp.bfloat16)
                seq[c, pl.ds(pl.multiple_of(i * 128 + pad, 32), 128), :] = value.astype(jnp.float32)
            return carry

        lax.fori_loop(low, high, body, 0)

    gate_tiles(rows // 128 - 1, rows // 128)
    for c in range(n_conv // 128):
        halo_out[:, c * 128 : (c + 1) * 128] = seq[c, rows : rows + pad, :].astype(jnp.bfloat16)
    gate_tiles(0, rows // 128 - 1)
    halo = m.copy(halo_out, halo_in, misc_send.at[1], misc_recv.at[1], me + 1)

    @pl.when(me < 15)
    def _():
        halo.start()

    n_taps = taps.shape[0]
    shift = pad - (n_taps - 1)

    def conv_chunk(i):
        base = pl.multiple_of(i * 128, 128)
        sums = jnp.zeros((128, 128), jnp.float32)
        squares = jnp.zeros((128, 128), jnp.float32)
        for c in range(n_conv // 128):
            part = seq[c, pl.ds(base, 128 + pad), :]
            total = jnp.zeros((128, 128), jnp.float32)
            for turn in range(8):
                moved = part if turn == 0 else pltpu.roll(part, 128 + pad - turn, 0)
                for tap in range(n_taps):
                    if (shift + tap) % 8 == turn:
                        start = shift + tap - turn
                        total = total + taps[tap : tap + 1, c * 128 : (c + 1) * 128] * moved[start : start + 128]
            acc2[pl.ds(base, 128), c * 128 : (c + 1) * 128] = total
            sums = sums + total
            squares = squares + total * total
        first = jnp.sum(sums, axis=1, keepdims=True)
        second = jnp.sum(squares, axis=1, keepdims=True)
        lane = lax.broadcasted_iota(jnp.int32, (128, 128), 1)
        stat_own[pl.ds(base, 128), :] = jnp.where(lane == 0, first, second)

    chunks = rows // 128

    def conv_loop(i, carry):
        conv_chunk(i)

        @pl.when((i == chunks // 2) & jnp.logical_not(at_end))
        def _():
            pass_on(2, 2)

        @pl.when(i == chunks - 3)
        def _():
            join_near()

        @pl.when(i == chunks - 1)
        def _():
            for k in (1, 2, 3):
                @pl.when(z + k <= 3)
                def _():
                    far_end(k).start()

        return carry

    lax.fori_loop(1, chunks, conv_loop, 0)

    @pl.when(at_end)
    def _():
        pass_on(2, 2)

    arrived(2, m.piece(0))
    slab(acc3, w3, m.piece(0), True)
    pass_on(3, 1)
    own_last(3)
    arrived(2, m.piece(1))
    slab(acc3, w3, m.piece(1), False)
    arrived(2, m.piece(2))
    slab(acc3, w3, m.piece(2), False)
    arrived(2, m.piece(3))
    slab(acc3, w3, m.piece(3), False)
    @pl.when(me > 0)
    def _():
        halo.wait_recv()
        for c in range(n_conv // 128):
            seq[c, 0:pad, :] = halo_in[:, c * 128 : (c + 1) * 128].astype(jnp.float32)

    @pl.when(me == 0)
    def _():
        seq[:, 0:pad, :] = jnp.zeros((n_conv // 128, pad, 128), jnp.float32)

    lax.fori_loop(0, 1, conv_loop, 0)

    stats = m.copy(stat_own, stat_in, misc_send.at[2], misc_recv.at[2], me, 1 - tp)

    def conv_finish(i, carry):
        at = pl.ds(pl.multiple_of(i * 128, 128), 128)
        both_stats = stat_own[at, :] + stat_in[at, :]
        mean_val = both_stats[:, 0:1] / (2 * n_conv)
        square_mean = both_stats[:, 1:2] / (2 * n_conv)
        scale = lax.rsqrt(square_mean - mean_val * mean_val + epsilon)
        value = (acc2[at, 0:n_conv] - mean_val) * scale * conv_gain[...]
        act[at, 0:n_conv] = (value * jax.nn.sigmoid(value)).astype(jnp.bfloat16)
        return carry

    stats.start()

    @pl.when(jnp.logical_not(at_end))
    def _():
        pass_on(3, 2)

    stats.wait_recv()
    lax.fori_loop(0, chunks, conv_finish, 0)
    pass_on(2, 3)

    for k in (1, 2, 3):
        @pl.when(z - k >= 0)
        def _():
            end_copy(4, 4 + k, 2 + k, me).wait_recv()
            pre = join(read(4 + k), (before[HV : HV + 1, :], before[0:HV, :]))
            before[0:HV, :] = pre[1]
            before[HV:, :] = jnp.broadcast_to(pre[0], (8, n_key))

    entry = jnp.concatenate([init[h].T for h in range(heads)], axis=1)
    state[...] = entry * before[HV : HV + 1, :] + before[0:HV, :]

    def gla_finish(i, carry):
        at = pl.ds(pl.multiple_of(i * 256, 256), 256)
        entering = state[...].astype(jnp.bfloat16)
        for h in range(heads):
            ks, vs = slice(h * HK, (h + 1) * HK), slice(h * HV, (h + 1) * HV)
            value = attn[at, vs] + dot(since[at, ks], entering[:, ks], ((1,), (1,)))
            value = value * lax.rsqrt(jnp.mean(value * value, axis=-1, keepdims=True) + epsilon) * head_gain[...]
            gate = acc3[at, vs].astype(jnp.bfloat16).astype(jnp.float32)
            act[at, n_conv + h * HV : n_conv + (h + 1) * HV] = (value * (gate * jax.nn.sigmoid(gate))).astype(jnp.bfloat16)
        return carry

    lax.fori_loop(0, rows // 256, gla_finish, 0)

    def part_copy(b):
        at = pl.ds(pl.multiple_of(b * 256, 256), 256)
        return m.copy(psend.at[b], other_out.at[:, at], part_send, part_recv, me, 1 - tp)

    def project(p, yy, core):
        weight = jnp.concatenate([wo[p, yy, 0], wo[p, yy, 1]], axis=1)
        left = act[pl.ds(pl.multiple_of(core * half, half), half), :]
        return dot(left, weight, ((1,), (0,))).astype(jnp.bfloat16)

    def out_pieces(j):
        p = m.piece(j)

        def theirs(yy, carry):
            psend[p * 2 + yy] = project(p, yy, 1 - tp)
            return carry

        def ours(yy, carry):
            part_copy(p * 2 + yy).start()
            own_out[:, pl.ds(pl.multiple_of((p * 2 + yy) * 256, 256), 256)] = project(p, yy, tp)
            return carry

        arrived(3, p)
        arrived(4, p)
        lax.fori_loop(0, 2, theirs, 0)
        lax.fori_loop(0, 2, ours, 0)

    def rows_of(core):
        return pl.ds(pl.multiple_of(core * half, half), half)

    def last_part(yy, low, high):
        p = m.piece(3)
        weight = jnp.concatenate([wo[p, yy, 0, low:high, :], wo[p, yy, 1, low:high, :]], axis=1)
        return lambda core: dot(act[rows_of(core), low:high], weight, ((1,), (0,)))

    def last_begin():
        def body(yy, carry):
            part = last_part(yy, 0, 2 * early)
            at = pl.ds(pl.multiple_of(yy * 256, 256), 256)
            acc2[0:half, at] = part(1 - tp)
            acc2[half:, at] = part(tp)
            return carry

        arrived(3, m.piece(3))
        lax.fori_loop(0, 2, body, 0)

    def last_end():
        b = m.piece(3) * 2

        def theirs(yy, carry):
            at = pl.ds(pl.multiple_of(yy * 256, 256), 256)
            part = last_part(yy, 2 * early, 2 * early + 2 * late)
            psend[b + yy] = (acc2[0:half, at] + part(1 - tp)).astype(jnp.bfloat16)
            return carry

        def ours(yy, carry):
            part_copy(b + yy).start()
            at = pl.ds(pl.multiple_of(yy * 256, 256), 256)
            part = last_part(yy, 2 * early, 2 * early + 2 * late)
            own_out[:, pl.ds(pl.multiple_of((b + yy) * 256, 256), 256)] = (acc2[half:, at] + part(tp)).astype(jnp.bfloat16)
            return carry

        arrived(4, m.piece(3))
        lax.fori_loop(0, 2, theirs, 0)
        lax.fori_loop(0, 2, ours, 0)

    def drain_early():
        swap.wait_send()
        stats.wait_send()

        @pl.when(me < 15)
        def _():
            halo.wait_send()

        for end in near_ends:
            end.wait_send()
        for k in (1, 2, 3):
            @pl.when(z + k <= 3)
            def _():
                far_end(k).wait_send()

        for f in (b1, b2, *pairs[0], *pairs[1]):
            f.drain_first()
            f.drain_last()
        for f in (*pairs[2], *pairs[3]):
            f.drain_first()
        whole.drain()
        for pair in lines:
            for line in pair:
                line.drain()

    out_pieces(0)

    @pl.when(at_end)
    def _():
        pass_on(3, 2)

    out_pieces(1)
    pass_on(3, 3)
    last_begin()
    out_pieces(2)
    drain_early()
    last_end()

    for f in (*pairs[2], *pairs[3]):
        f.drain_last()
    m.copy(psend, psend, part_send, part_recv, me, 1 - tp).wait_send()
    m.copy(other_out, other_out, part_send, part_recv, me, 1 - tp).wait_recv()


def fused_layer(
    tokens, norm_gain, w_conv_a, w_conv_gate, conv_weight, conv_gain, w_query, w_key, w_value, w_outgate,
    w_decay, decay_bias, decay_extra, head_gain, init_state, w_out_conv, w_out_gla,
):
    rows, width = tokens.shape
    depth = w_query.shape[0]
    n_key = w_query.shape[1]
    n_conv = w_conv_a.shape[1]
    cols = w_out_conv.shape[1]
    half = rows // 2
    pad = 32
    bf16, f32 = jnp.bfloat16, jnp.float32
    dma = pltpu.SemaphoreType.DMA
    vm = pl.BlockSpec(memory_space=pltpu.VMEM)
    hbm = pl.BlockSpec(memory_space=pl.ANY)
    share = pltpu.VMEM((half, 2 * width), bf16)
    own, other = pl.pallas_call(
        layer_kernel,
        out_shape=[share, share],
        in_specs=[hbm, vm, hbm, hbm, vm, vm, hbm, hbm, hbm, hbm, hbm, vm, hbm, vm, vm, hbm, hbm],
        out_specs=[vm, vm],
        scratch_shapes=[
            pltpu.VMEM((4, 2, 2, depth, 5 * n_key), bf16),
            pltpu.VMEM((4, 2, 2, depth, 2 * n_conv), bf16),
            pltpu.VMEM((4, 2, 2, depth, n_conv), bf16),
            pltpu.VMEM((4, 2, 2, 2 * n_conv, cols), bf16),
            pltpu.VMEM((2, rows, width), bf16),
            pltpu.VMEM((rows, 2 * width), bf16),
            pltpu.VMEM((rows, 5 * n_key), f32),
            pltpu.VMEM((rows, 2 * n_conv), f32),
            pltpu.VMEM((rows, n_conv), f32),
            pltpu.VMEM((rows, n_key), f32),
            pltpu.VMEM((n_conv // 128, rows + pad, 128), f32),
            pltpu.VMEM((rows, n_conv), f32),
            pltpu.VMEM((rows, n_key), bf16),
            pltpu.VMEM((rows, 2 * n_conv), bf16),
            pltpu.VMEM((8, half, 256), bf16),
            pltpu.VMEM((pad, n_conv), bf16),
            pltpu.VMEM((pad, n_conv), bf16),
            pltpu.VMEM((rows, 128), f32),
            pltpu.VMEM((rows, 128), f32),
            pltpu.VMEM((8, HV + 16, n_key), bf16),
            pltpu.VMEM((HV, n_key), f32),
            pltpu.VMEM((1, n_key), f32),
            pltpu.VMEM((HV + 8, n_key), f32),
            dma((11,)), dma((10,)), dma((16,)), dma((10,)), dma((5, 4)), dma((9, 5)), dma((9, 4)),
            dma((3,)), dma((3,)), dma((6,)), dma((8,)), dma(()), dma(()),
        ],
        compiler_params=pltpu.CompilerParams(collective_id=0, has_side_effects=True, vmem_limit_bytes=56 * 2**20),
        name="layer",
    )(
        tokens, norm_gain[None, :], w_conv_a, w_conv_gate, conv_weight, conv_gain[None, :], w_query, w_key, w_value,
        w_outgate, w_decay, decay_bias[None, :], decay_extra, head_gain[None, :], init_state, w_out_conv, w_out_gla,
    )
    return (own.astype(f32) + other.astype(f32)).astype(bf16)


def local_kernel(heads, pieces, q_ref, k_ref, v_ref, pre_ref, extra_ref, bias_ref, attn_ref, since_ref, end_ref, log_ref, state, prefix):
    step = pl.program_id(0)

    @pl.when(step == 0)
    def _():
        state[...] = jnp.zeros_like(state)
        prefix[...] = jnp.zeros_like(prefix)

    rows = lax.broadcasted_iota(jnp.int32, (BLOCK, BLOCK), 0)
    columns = lax.broadcasted_iota(jnp.int32, (BLOCK, BLOCK), 1)
    causal = rows >= columns
    lower = causal.astype(jnp.float32)
    for piece in range(pieces):
        at = pl.ds(piece * BLOCK, BLOCK)
        pre = pre_ref[at, :] + bias_ref[...]
        logs = jax.nn.log_sigmoid(pre) / gate_divisor + extra_ref[at, :]
        cum = lax.dot_general(
            lower, logs, (((1,), (0,)), ((), ())), precision=lax.Precision.HIGHEST, preferred_element_type=jnp.float32
        )
        total = cum[BLOCK - 1 :, :]
        middle = cum[BLOCK // 2 - 1 : BLOCK // 2, :]
        query = q_ref[at, :].astype(jnp.float32) * HK ** (-0.5)
        keys = k_ref[at, :].astype(jnp.float32)
        decayed = query * jnp.exp(cum)
        since_ref[at, :] = (decayed * jnp.exp(prefix[...])).astype(jnp.bfloat16)
        decayed = decayed.astype(jnp.bfloat16)
        query = (query * jnp.exp(cum - middle)).astype(jnp.bfloat16)
        inverse = (keys * jnp.exp(middle - cum)).astype(jnp.bfloat16)
        to_end = (keys * jnp.exp(total - cum)).astype(jnp.bfloat16)
        entering = state[...].astype(jnp.bfloat16)
        added = []
        for h in range(heads):
            ks, vs = slice(h * HK, (h + 1) * HK), slice(h * HV, (h + 1) * HV)
            values = v_ref[at, vs]
            scores = jnp.where(causal, dot(query[:, ks], inverse[:, ks], ((1,), (1,))), 0.0)
            attn_ref[at, vs] = dot(scores.astype(jnp.bfloat16), values, ((1,), (0,))) + dot(
                decayed[:, ks], entering[:, ks], ((1,), (1,))
            )
            added.append(dot(values, to_end[:, ks], ((0,), (0,))))
        added = added[0] if heads == 1 else jnp.concatenate(added, axis=1)
        state[...] = state[...] * jnp.exp(total) + added
        prefix[...] = prefix[...] + total
    end_ref[...] = state[...]
    log_ref[...] = prefix[...]


def gla_local(query, keys, values, decay_pre, decay_extra, decay_bias):
    rows, width = query.shape
    heads = width // HK
    pieces = 4
    tile = pieces * BLOCK

    def tiled(array):
        return pl.BlockSpec((tile, array.shape[1]), lambda i: (i, 0))

    def whole(shape):
        return pl.BlockSpec(shape, lambda i: (0, 0))

    return pl.pallas_call(
        functools.partial(local_kernel, heads, pieces),
        grid=(rows // tile,),
        in_specs=[tiled(query), tiled(keys), tiled(values), tiled(decay_pre), tiled(decay_extra), whole((1, width))],
        out_specs=[tiled(values), tiled(query), whole((HV, width)), whole((1, width))],
        out_shape=[
            jax.ShapeDtypeStruct(values.shape, jnp.float32),
            jax.ShapeDtypeStruct(query.shape, jnp.bfloat16),
            jax.ShapeDtypeStruct((HV, width), jnp.float32),
            jax.ShapeDtypeStruct((1, width), jnp.float32),
        ],
        scratch_shapes=[pltpu.VMEM((HV, width), jnp.float32), pltpu.VMEM((1, width), jnp.float32)],
        cost_estimate=pl.CostEstimate(flops=10**10, bytes_accessed=10**7, transcendentals=10**6),
        name="gla_local",
    )(query, keys, values, decay_pre, decay_extra, decay_bias[None, :])


def finish_kernel(heads, size, where_ref, attn_ref, since_ref, gate_ref, ends_ref, init_ref, gain_ref, out_ref, state):
    me = where_ref[0]

    @pl.when(pl.program_id(0) == 0)
    def _():
        state[...] = init_ref[...]

        def one(device, carry):
            at = device
            decay = ends_ref[pl.ds(pl.multiple_of(at * size + HV, 16), 16), :].astype(jnp.float32)[:1]
            end = ends_ref[pl.ds(pl.multiple_of(at * size, 16), HV), :].astype(jnp.float32)
            state[...] = state[...] * decay + end
            return carry

        lax.fori_loop(0, me, one, 0)

    entering = state[...].astype(jnp.bfloat16)
    for h in range(heads):
        ks, vs = slice(h * HK, (h + 1) * HK), slice(h * HV, (h + 1) * HV)
        attn = attn_ref[:, vs] + dot(since_ref[:, ks], entering[:, ks], ((1,), (1,)))
        attn = attn * lax.rsqrt(jnp.mean(attn * attn, axis=-1, keepdims=True) + epsilon) * gain_ref[...]
        gate = gate_ref[:, vs].astype(jnp.float32)
        out_ref[:, vs] = (attn * (gate * jax.nn.sigmoid(gate))).astype(jnp.bfloat16)


def gla_finish(attn, since, out_gate, ends, init_state, head_gain, me):
    rows, width = since.shape
    heads = width // HK
    tile = 256

    def tiled(array):
        return pl.BlockSpec((tile, array.shape[1]), lambda i, w: (i, 0))

    def whole(array):
        return pl.BlockSpec(array.shape, lambda i, w: (0, 0))

    init = init_state.transpose(2, 0, 1).reshape(HV, width)
    gain = head_gain[None, :]
    return pl.pallas_call(
        functools.partial(finish_kernel, heads, HV + 16),
        grid_spec=pltpu.PrefetchScalarGridSpec(
            num_scalar_prefetch=1,
            grid=(rows // tile,),
            in_specs=[tiled(attn), tiled(since), tiled(out_gate), whole(ends), whole(init), whole(gain)],
            out_specs=tiled(attn),
            scratch_shapes=[pltpu.VMEM((HV, width), jnp.float32)],
        ),
        out_shape=jax.ShapeDtypeStruct(attn.shape, jnp.bfloat16),
        cost_estimate=pl.CostEstimate(flops=3 * 10**9, bytes_accessed=10**7, transcendentals=10**6),
        name="gla_finish",
    )(me[None], attn, since, out_gate, ends, init, gain)


def conv_branch(gated, conv_weight, conv_gain):
    taps = conv_weight.shape[0]
    row_count = gated.shape[0]
    count = lax.axis_size("sp")
    earlier = lax.ppermute(gated[row_count - taps + 1 :], "sp", [(i, i + 1) for i in range(count - 1)])
    extended = jnp.concatenate([earlier, gated], axis=0).astype(jnp.float32)
    conv_sum = jnp.zeros(gated.shape, jnp.float32)
    for tap in range(taps):
        conv_sum = conv_sum + conv_weight[tap][None, :] * extended[tap : tap + row_count]
    row_sums, row_squares = lax.psum((jnp.sum(conv_sum, axis=1), jnp.sum(conv_sum * conv_sum, axis=1)), "tp")
    mean_val = (row_sums / D_CONV)[:, None]
    square_mean = (row_squares / D_CONV)[:, None]
    conv_norm = (conv_sum - mean_val) * lax.rsqrt(square_mean - mean_val * mean_val + epsilon) * conv_gain
    return jax.nn.silu(conv_norm).astype(jnp.bfloat16)


def project(hidden, weight):
    return dot(hidden, weight, ((1,), (0,)))


def plain_layer(
    tokens, norm_gain, w_conv_a, w_conv_gate, conv_weight, conv_gain, w_query, w_key, w_value, w_outgate,
    w_decay, decay_bias, decay_extra, head_gain, init_state, w_out_conv, w_out_gla,
):
    me = lax.axis_index("sp")

    def gather(shard):
        return lax.all_gather(shard, "sp", axis=0, tiled=True)

    widened = lax.all_gather(tokens, "tp", axis=1, tiled=True).astype(jnp.float32)
    normed = (
        widened * lax.rsqrt(jnp.mean(widened * widened, axis=-1, keepdims=True) + epsilon) * norm_gain
    ).astype(jnp.bfloat16)
    half = w_query.shape[1]
    conv_a = project(normed, gather(w_conv_a)).astype(jnp.bfloat16)
    conv_gate = project(normed, gather(w_conv_gate)).astype(jnp.bfloat16)
    full_qkd = gather(jnp.concatenate([w_query, w_key, w_decay], axis=1))
    full_v = gather(w_value)
    gated = (conv_a.astype(jnp.float32) * jax.nn.sigmoid(conv_gate.astype(jnp.float32))).astype(jnp.bfloat16)
    conv_out = conv_branch(gated, conv_weight, conv_gain)
    query_keys = project(normed, full_qkd[:, : 2 * half]).astype(jnp.bfloat16)
    decay_pre = project(normed, full_qkd[:, 2 * half :])
    values = project(normed, full_v).astype(jnp.bfloat16)
    attn, since, end, end_log = gla_local(
        query_keys[:, :half], query_keys[:, half:], values, decay_pre, decay_extra, decay_bias
    )
    packed = jnp.concatenate([end, jnp.broadcast_to(jnp.exp(end_log), (16, half))], axis=0).astype(jnp.bfloat16)
    ends = gather(packed)
    out_gate = project(normed, gather(w_outgate)).astype(jnp.bfloat16)
    gla_out = gla_finish(attn, since, out_gate, ends, init_state, head_gain, me)
    total = dot(conv_out, gather(w_out_conv.T), ((1,), (1,))) + dot(gla_out, gather(w_out_gla.T), ((1,), (1,)))
    return lax.psum_scatter(total.astype(jnp.bfloat16), "tp", scatter_dimension=0, tiled=True)


def per_device(*arrays):
    if folded(lax.axis_size("sp"), lax.axis_size("tp")):
        return fused_layer(*arrays)
    return plain_layer(*arrays)


def solution(mesh):
    placed = (
        P("sp", "tp"), P(), P("sp", "tp"), P("sp", "tp"), P(None, "tp"), P("tp"), P("sp", "tp"), P("sp", "tp"),
        P("sp", "tp"), P("sp", "tp"), P("sp", "tp"), P("tp"), P("sp", "tp"), P(), P("tp", None, None),
        P("tp", "sp"), P("tp", "sp"),
    )
    return jax.shard_map(
        per_device, mesh=mesh, in_specs=placed, out_specs=P(("sp", "tp"), None), check_vma=False
    )
```

```python
import functools

import jax
import jax.numpy as jnp
from jax import lax
from jax.experimental import pallas as pl
from jax.experimental.pallas import tpu as pltpu
from jax.sharding import PartitionSpec as P

D_CONV = 1024
HK = 64
HV = 128
BLOCK = 64

epsilon = 1e-06
gate_divisor = 16.0

MESH = pl.DeviceIdType.MESH


def dot(a, b, dims):
    return lax.dot_general(a, b, (dims, ((), ())), preferred_element_type=jnp.float32)


def folded(n_sp, n_tp):
    return n_sp == 16 and n_tp == 2


class Mover:
    def __init__(self):
        self.me = lax.axis_index("sp")
        self.tp = lax.axis_index("tp")
        self.z, self.y, self.x = self.me // 4, (self.me // 2) % 2, self.me % 2
        self.other = {"x": self.me + 1 - 2 * self.x, "y": self.me + 2 - 4 * self.y}
        self.across = self.me + 3 - 2 * self.x - 4 * self.y
        self.sent = []

    def copy(self, source, target, send, recv, place, core=None):
        core = self.tp if core is None else core
        return pltpu.make_async_remote_copy(
            src_ref=source, dst_ref=target, send_sem=send, recv_sem=recv, device_id=(place, core), device_id_type=MESH
        )

    def piece(self, j):
        z = self.z
        return (z, z + 1 - 2 * (z % 2), 2 - z // 2, 3 - 3 * (z // 2))[j]


class Flow:
    def __init__(self, mover, number, view, first, sems):
        self.m, self.number, self.view, self.first = mover, number, view, first
        self.last = {"x": "y", "y": "x"}[first]
        self.sems = sems

    def own(self, p):
        return self.view(p, self.m.y, self.m.x)

    def pair(self, p):
        every = slice(None)
        return self.view(p, self.m.y, every) if self.first == "x" else self.view(p, every, self.m.x)

    def first_copy(self, p, source=None):
        own = self.own(p) if source is None else source
        slot = self.number * 4 + p if self.number < 2 else self.number + 6
        fs, fr = self.sems["first_send"], self.sems["first_recv"]
        return self.m.copy(own, own, fs.at[self.number], fr.at[slot], self.m.other[self.first])

    def last_copy(self, p, source=None):
        pair = self.pair(p) if source is None else source
        ls, lr = self.sems["last_send"], self.sems["last_recv"]
        return self.m.copy(pair, pair, ls.at[self.number], lr.at[self.number // 2, p], self.m.other[self.last])

    def drain_first(self):
        if self.number < 2:
            self.first_copy(0, self.own(slice(None))).wait_send()
        else:
            self.first_copy(self.m.z).wait_send()

    def drain_last(self):
        self.last_copy(0, self.pair(slice(None))).wait_send()


class Line:
    def __init__(self, mover, number, view, sems):
        self.m, self.number, self.view, self.sems = mover, number, view, sems

    def up(self, p):
        return self.m.copy(
            self.view(p), self.view(p), self.sems["z_send"].at[self.number, p], self.sems["z_recv"].at[self.number, p],
            self.m.me + 4,
        )

    def down(self, p):
        return self.m.copy(
            self.view(p), self.view(p), self.sems["z_send"].at[self.number, p + 1],
            self.sems["z_recv"].at[self.number, p], self.m.me - 4,
        )

    def start_own(self):
        z = self.m.z

        @pl.when(z < 3)
        def _():
            self.up(z).start()

        @pl.when(z > 0)
        def _():
            self.down(z).start()

    def relay(self, step, then):
        z = self.m.z

        @pl.when(z >= step)
        def _():
            p = z - step
            self.up(p).wait_recv()

            @pl.when(z < 3)
            def _():
                self.up(p).start()

            then(p)

        @pl.when(z + step <= 3)
        def _():
            p = z + step
            self.down(p).wait_recv()

            @pl.when(z > 0)
            def _():
                self.down(p).start()

            then(p)

    def drain(self):
        z = self.m.z
        for p in range(4):
            @pl.when((p <= z) & (z < 3))
            def _():
                self.up(p).wait_send()

            @pl.when((p >= z) & (z > 0))
            def _():
                self.down(p).wait_send()


def at_step(z, step, then):
    if step == 0:
        then(z)
        return

    @pl.when(z >= step)
    def _():
        then(z - step)

    @pl.when(z + step <= 3)
    def _():
        then(z + step)


def layer_kernel(
    tokens, gain, wa, wg, taps, conv_gain, wq, wk, wv, wog, wd, bias, extra_in, head_gain, init, woc, wogl, own_out, other_out,
    w1, w2, w3, wo, both, normed, acc1, acc2, acc3, extra, seq, attn, since, act, psend,
    halo_out, halo_in, stat_own, stat_in, packs, state, prefix, before,
    local, first_send, first_recv, last_send, last_recv, z_send, z_recv, misc_send, misc_recv, end_send, end_recv,
    part_send, part_recv,
):
    m = Mover()
    me, tp, z, y, x = m.me, m.tp, m.z, m.y, m.x
    rows = normed.shape[0]
    half = rows // 2
    width = both.shape[2]
    n_key = acc1.shape[1] // 5
    n_conv = 2 * n_key
    heads = n_key // HK
    sems = dict(
        first_send=first_send, first_recv=first_recv, last_send=last_send, last_recv=last_recv,
        z_send=z_send, z_recv=z_recv,
    )

    def lanes(ref, low, size):
        return lambda p, yy, xx: ref.at[p, yy, xx, :, pl.ds(low, size)]

    def depth(low, size):
        return lambda p, yy, xx: wo.at[p, yy, xx, pl.ds(low, size), :]

    mid = w1.shape[-1] // 2
    late = wo.shape[3] // 4
    early = wo.shape[3] // 2 - late
    b1 = Flow(m, 0, lanes(w1, 0, mid), "x", sems)
    b2 = Flow(m, 1, lanes(w1, mid, mid), "y", sems)
    pairs = [
        (Flow(m, 2, lanes(w2, 0, n_conv), "x", sems), Flow(m, 3, lanes(w2, n_conv, n_conv), "y", sems)),
        (Flow(m, 4, lanes(w3, 0, n_key), "x", sems), Flow(m, 5, lanes(w3, n_key, n_key), "y", sems)),
        (Flow(m, 6, depth(0, early), "x", sems), Flow(m, 7, depth(early, early), "y", sems)),
        (Flow(m, 8, depth(2 * early, late), "x", sems), Flow(m, 9, depth(2 * early + late, late), "y", sems)),
    ]
    whole = Line(m, 0, lambda p: w1.at[p, y, x], sems)
    lines = [tuple(Line(m, f.number - 1, f.pair, sems) for f in pair) for pair in pairs]

    loads = [
        (wq, w1.at[z, y, x, :, pl.ds(0, n_key)]),
        (wk, w1.at[z, y, x, :, pl.ds(n_key, n_key)]),
        (wd, w1.at[z, y, x, :, pl.ds(2 * n_key, n_key)]),
        (wv, w1.at[z, y, x, :, pl.ds(3 * n_key, n_conv)]),
        (wa, w2.at[z, y, x, :, pl.ds(0, n_conv)]),
        (wg, w2.at[z, y, x, :, pl.ds(n_conv, n_conv)]),
        (wog, w3.at[z, y, x]),
        (woc, wo.at[z, y, x, pl.ds(0, n_conv), :]),
        (wogl, wo.at[z, y, x, pl.ds(n_conv, n_conv), :]),
        (tokens, both.at[tp]),
        (extra_in, extra),
    ]
    loads = [pltpu.make_async_copy(a, b, local.at[i]) for i, (a, b) in enumerate(loads)]
    for load in loads:
        load.start()

    barrier = pltpu.get_barrier_semaphore()
    def greet(place, core):
        pl.semaphore_signal(barrier, inc=1, device_id=(place, core), device_id_type=MESH)

    for place, core in ((m.other["x"], tp), (m.other["y"], tp), (me, 1 - tp)):
        greet(place, core)

    @pl.when(z < 3)
    def _():
        greet(me + 4, tp)

    @pl.when(z > 0)
    def _():
        greet(me - 4, tp)

    at_end = (z == 0) | (z == 3)

    @pl.when(at_end)
    def _():
        pl.semaphore_wait(barrier, 4)

    @pl.when(jnp.logical_not(at_end))
    def _():
        pl.semaphore_wait(barrier, 5)

    for i in range(4):
        loads[i].wait()
    whole.start_own()
    b1.first_copy(z).start()
    b2.first_copy(z).start()
    loads[9].wait()
    swap = m.copy(both.at[tp], both.at[tp], misc_send.at[0], misc_recv.at[0], me, 1 - tp)
    swap.start()
    loads[4].wait()
    loads[5].wait()
    for f in pairs[0]:
        f.first_copy(z).start()
    loads[6].wait()
    for f in pairs[1]:
        f.first_copy(z).start()
    for i in (7, 8, 10):
        loads[i].wait()

    def head_firsts(step):
        def one(p):
            b1.first_copy(p).wait_recv()
            b1.last_copy(p).start()
            b2.first_copy(p).wait_recv()
            b2.last_copy(p).start()

        at_step(z, step, one)

    def head_line(step):
        def then(p):
            b1.first_copy(p).start()
            b2.first_copy(p).start()

        whole.relay(step, then)

    def begin(k):
        for f in pairs[k]:
            f.first_copy(z).start()

    def enter_one(k, i):
        pairs[k][i].first_copy(z).wait_recv()
        lines[k][i].start_own()

    def enter(k):
        enter_one(k, 0)
        enter_one(k, 1)

    def own_last(k):
        for f in pairs[k]:
            f.last_copy(z).start()

    def pass_on(k, step):
        for f, line in zip(pairs[k], lines[k]):
            line.relay(step, lambda p: f.last_copy(p).start())

    def relay_only(k, step):
        for line in lines[k]:
            line.relay(step, lambda p: None)

    def finish(k, step):
        for f in pairs[k]:
            at_step(z, step, lambda p: f.last_copy(p).start())

    def arrived(k, p):
        every = (p, slice(None), slice(None))
        both_flows = (
            w1.at[(*every, slice(None), pl.ds(0, mid))],
            w2.at[(*every, slice(None), pl.ds(0, n_conv))],
            w3.at[(*every, slice(None), pl.ds(0, n_key))],
            wo.at[(*every, pl.ds(0, early), slice(None))],
            wo.at[(*every, pl.ds(0, late), slice(None))],
        )[k]
        flow = b1 if k == 0 else pairs[k - 1][0]
        flow.last_copy(p, both_flows).wait_recv()

    def norm_tiles(low, high):
        def body(i, carry):
            at = pl.ds(pl.multiple_of(i * 128, 128), 128)
            a = both[0, at, :].astype(jnp.float32)
            b = both[1, at, :].astype(jnp.float32)
            square = jnp.sum(a * a + b * b, axis=1, keepdims=True)
            scale = lax.rsqrt(square / (2 * width) + epsilon)
            normed[at, :width] = (a * scale * gain[:, :width]).astype(jnp.bfloat16)
            normed[at, width:] = (b * scale * gain[:, width:]).astype(jnp.bfloat16)
            return carry

        lax.fori_loop(low, high, body, 0)

    def slab(acc, ref, p, first):
        size = ref.shape[1] * ref.shape[2] * ref.shape[3]

        def body(c, carry):
            at = pl.ds(pl.multiple_of(c * 256, 256), 256)
            left = normed[:, pl.ds(pl.multiple_of(p * size, size), size)]
            right = ref[p, :, :, :, at].reshape(size, 256)
            got = dot(left, right, ((1,), (0,)))
            if first:
                acc[:, at] = got
            else:
                acc[:, at] += got
            return carry

        lax.fori_loop(0, acc.shape[1] // 256, body, 0)

    swap.wait_recv()
    norm_tiles(0, 4)
    head_line(1)
    head_firsts(0)
    norm_tiles(4, 8)
    enter_one(0, 0)
    head_line(2)
    enter_one(0, 1)
    head_firsts(1)
    head_line(3)
    arrived(0, m.piece(0))
    slab(acc1, w1, m.piece(0), True)
    head_firsts(2)
    begin(2)
    begin(3)
    pass_on(0, 1)
    arrived(0, m.piece(1))
    slab(acc1, w1, m.piece(1), False)
    head_firsts(3)
    enter(1)
    own_last(0)
    pass_on(0, 2)
    arrived(0, m.piece(2))
    slab(acc1, w1, m.piece(2), False)
    pass_on(1, 1)
    enter(2)
    arrived(0, m.piece(3))
    slab(acc1, w1, m.piece(3), False)

    state[...] = jnp.zeros_like(state)
    prefix[...] = jnp.zeros_like(prefix)
    r_iota = lax.broadcasted_iota(jnp.int32, (BLOCK, BLOCK), 0)
    c_iota = lax.broadcasted_iota(jnp.int32, (BLOCK, BLOCK), 1)
    causal = r_iota >= c_iota
    lower = causal.astype(jnp.float32)

    def block(i, carry):
        at = pl.ds(pl.multiple_of(i * BLOCK, BLOCK), BLOCK)
        pre = acc1[at, 2 * n_key : 3 * n_key] + bias[...]
        logs = jax.nn.log_sigmoid(pre) / gate_divisor + extra[at, :]
        cum = lax.dot_general(
            lower, logs, (((1,), (0,)), ((), ())), precision=lax.Precision.HIGHEST, preferred_element_type=jnp.float32
        )
        total = cum[BLOCK - 1 :, :]
        middle = cum[BLOCK // 2 - 1 : BLOCK // 2, :]
        query = acc1[at, 0:n_key].astype(jnp.bfloat16).astype(jnp.float32) * HK ** (-0.5)
        keys = acc1[at, n_key : 2 * n_key].astype(jnp.bfloat16).astype(jnp.float32)
        decayed = query * jnp.exp(cum)
        since[at, :] = (decayed * jnp.exp(prefix[...])).astype(jnp.bfloat16)
        decayed = decayed.astype(jnp.bfloat16)
        query = (query * jnp.exp(cum - middle)).astype(jnp.bfloat16)
        inverse = (keys * jnp.exp(middle - cum)).astype(jnp.bfloat16)
        to_end = (keys * jnp.exp(total - cum)).astype(jnp.bfloat16)
        entering = state[...].astype(jnp.bfloat16)
        added = []
        for h in range(heads):
            ks, vs = slice(h * HK, (h + 1) * HK), slice(h * HV, (h + 1) * HV)
            values = acc1[at, 3 * n_key + h * HV : 3 * n_key + (h + 1) * HV].astype(jnp.bfloat16)
            scores = jnp.where(causal, dot(query[:, ks], inverse[:, ks], ((1,), (1,))), 0.0)
            attn[at, vs] = dot(scores.astype(jnp.bfloat16), values, ((1,), (0,))) + dot(
                decayed[:, ks], entering[:, ks], ((1,), (1,))
            )
            added.append(dot(values, to_end[:, ks], ((0,), (0,))))
        state[...] = state[...] * jnp.exp(total) + jnp.concatenate(added, axis=1)
        prefix[...] = prefix[...] + total
        return carry

    blocks = rows // BLOCK

    def attend(i, carry):
        block(i, 0)

        @pl.when(i == blocks // 2)
        def _():
            pass_on(0, 3)

        @pl.when((i == blocks // 2) & at_end)
        def _():
            own_last(1)

        @pl.when(i == blocks - 3)
        def _():
            relay_only(1, 2)

        return carry

    lax.fori_loop(0, blocks, attend, 0)

    def pack(slot, decay, end):
        packs[slot, 0:HV, :] = end.astype(jnp.bfloat16)
        packs[slot, HV:, :] = jnp.broadcast_to(decay, (16, n_key)).astype(jnp.bfloat16)

    def read(slot):
        return packs[slot, HV : HV + 1, :].astype(jnp.float32), packs[slot, 0:HV, :].astype(jnp.float32)

    def end_copy(source, target, number, place):
        return m.copy(packs.at[source], packs.at[target], end_send.at[number], end_recv.at[target], place)

    def join(early, late):
        return early[0] * late[0], early[1] * late[0] + late[1]

    near_ends = [
        end_copy(0, 1, 0, m.other["x"]),
        end_copy(0, 2, 1, m.other["y"]),
        end_copy(0, 3, 2, m.across),
    ]
    pack(0, jnp.exp(prefix[...]), state[...])

    arrived(1, m.piece(0))
    slab(acc2, w2, m.piece(0), True)
    for end in near_ends:
        end.start()

    @pl.when(jnp.logical_not(at_end))
    def _():
        own_last(1)

    finish(1, 2)
    pass_on(2, 1)
    enter(3)
    arrived(1, m.piece(1))
    slab(acc2, w2, m.piece(1), False)
    arrived(1, m.piece(2))
    slab(acc2, w2, m.piece(2), False)
    arrived(1, m.piece(3))
    slab(acc2, w2, m.piece(3), False)
    pass_on(1, 3)
    own_last(2)

    def join_near():
        for end in near_ends:
            end.wait_recv()
        run = (jnp.ones((1, n_key), jnp.float32), jnp.zeros((HV, n_key), jnp.float32))
        pre = run
        for yy in range(2):
            for xx in range(2):
                past = yy * 2 + xx < y * 2 + x
                run = join(run, read((y + yy - 2 * y * yy) * 2 + x + xx - 2 * x * xx))
                pre = jnp.where(past, run[0], pre[0]), jnp.where(past, run[1], pre[1])
        before[0:HV, :] = pre[1]
        before[HV:, :] = jnp.broadcast_to(pre[0], (8, n_key))
        pack(4, *run)

    def far_end(k):
        return end_copy(4, 4 + k, 2 + k, me + 4 * k)

    pad = seq.shape[1] - rows

    def gate_tiles(low, high):
        def body(i, carry):
            at = pl.ds(pl.multiple_of(i * 128, 128), 128)
            for c in range(n_conv // 128):
                a = acc2[at, c * 128 : (c + 1) * 128].astype(jnp.bfloat16).astype(jnp.float32)
                g = acc2[at, n_conv + c * 128 : n_conv + (c + 1) * 128].astype(jnp.bfloat16).astype(jnp.float32)
                value = (a * jax.nn.sigmoid(g)).astype(jnp.bfloat16)
                seq[c, pl.ds(pl.multiple_of(i * 128 + pad, 32), 128), :] = value.astype(jnp.float32)
            return carry

        lax.fori_loop(low, high, body, 0)

    gate_tiles(rows // 128 - 1, rows // 128)
    for c in range(n_conv // 128):
        halo_out[:, c * 128 : (c + 1) * 128] = seq[c, rows : rows + pad, :].astype(jnp.bfloat16)
    gate_tiles(0, rows // 128 - 1)
    halo = m.copy(halo_out, halo_in, misc_send.at[1], misc_recv.at[1], me + 1)

    @pl.when(me < 15)
    def _():
        halo.start()

    n_taps = taps.shape[0]
    shift = pad - (n_taps - 1)

    def conv_chunk(i):
        base = pl.multiple_of(i * 128, 128)
        sums = jnp.zeros((128, 128), jnp.float32)
        squares = jnp.zeros((128, 128), jnp.float32)
        for c in range(n_conv // 128):
            part = seq[c, pl.ds(base, 128 + pad), :]
            total = jnp.zeros((128, 128), jnp.float32)
            for turn in range(8):
                moved = part if turn == 0 else pltpu.roll(part, 128 + pad - turn, 0)
                for tap in range(n_taps):
                    if (shift + tap) % 8 == turn:
                        start = shift + tap - turn
                        total = total + taps[tap : tap + 1, c * 128 : (c + 1) * 128] * moved[start : start + 128]
            acc2[pl.ds(base, 128), c * 128 : (c + 1) * 128] = total
            sums = sums + total
            squares = squares + total * total
        first = jnp.sum(sums, axis=1, keepdims=True)
        second = jnp.sum(squares, axis=1, keepdims=True)
        lane = lax.broadcasted_iota(jnp.int32, (128, 128), 1)
        stat_own[pl.ds(base, 128), :] = jnp.where(lane == 0, first, second)

    chunks = rows // 128

    def conv_loop(i, carry):
        conv_chunk(i)

        @pl.when((i == chunks // 2) & jnp.logical_not(at_end))
        def _():
            pass_on(2, 2)

        @pl.when(i == chunks - 3)
        def _():
            join_near()

        @pl.when(i == chunks - 1)
        def _():
            for k in (1, 2, 3):
                @pl.when(z + k <= 3)
                def _():
                    far_end(k).start()

        return carry

    lax.fori_loop(1, chunks, conv_loop, 0)

    @pl.when(at_end)
    def _():
        pass_on(2, 2)

    arrived(2, m.piece(0))
    slab(acc3, w3, m.piece(0), True)
    pass_on(3, 1)
    own_last(3)
    arrived(2, m.piece(1))
    slab(acc3, w3, m.piece(1), False)
    arrived(2, m.piece(2))
    slab(acc3, w3, m.piece(2), False)
    arrived(2, m.piece(3))
    slab(acc3, w3, m.piece(3), False)
    @pl.when(me > 0)
    def _():
        halo.wait_recv()
        for c in range(n_conv // 128):
            seq[c, 0:pad, :] = halo_in[:, c * 128 : (c + 1) * 128].astype(jnp.float32)

    @pl.when(me == 0)
    def _():
        seq[:, 0:pad, :] = jnp.zeros((n_conv // 128, pad, 128), jnp.float32)

    lax.fori_loop(0, 1, conv_loop, 0)

    stats = m.copy(stat_own, stat_in, misc_send.at[2], misc_recv.at[2], me, 1 - tp)

    def conv_finish(i, carry):
        at = pl.ds(pl.multiple_of(i * 128, 128), 128)
        both_stats = stat_own[at, :] + stat_in[at, :]
        mean_val = both_stats[:, 0:1] / (2 * n_conv)
        square_mean = both_stats[:, 1:2] / (2 * n_conv)
        scale = lax.rsqrt(square_mean - mean_val * mean_val + epsilon)
        value = (acc2[at, 0:n_conv] - mean_val) * scale * conv_gain[...]
        act[at, 0:n_conv] = (value * jax.nn.sigmoid(value)).astype(jnp.bfloat16)
        return carry

    stats.start()

    @pl.when(jnp.logical_not(at_end))
    def _():
        pass_on(3, 2)

    stats.wait_recv()
    lax.fori_loop(0, chunks, conv_finish, 0)
    pass_on(2, 3)

    for k in (1, 2, 3):
        @pl.when(z - k >= 0)
        def _():
            end_copy(4, 4 + k, 2 + k, me).wait_recv()
            pre = join(read(4 + k), (before[HV : HV + 1, :], before[0:HV, :]))
            before[0:HV, :] = pre[1]
            before[HV:, :] = jnp.broadcast_to(pre[0], (8, n_key))

    entry = jnp.concatenate([init[h].T for h in range(heads)], axis=1)
    state[...] = entry * before[HV : HV + 1, :] + before[0:HV, :]

    def gla_finish(i, carry):
        at = pl.ds(pl.multiple_of(i * 256, 256), 256)
        entering = state[...].astype(jnp.bfloat16)
        for h in range(heads):
            ks, vs = slice(h * HK, (h + 1) * HK), slice(h * HV, (h + 1) * HV)
            value = attn[at, vs] + dot(since[at, ks], entering[:, ks], ((1,), (1,)))
            value = value * lax.rsqrt(jnp.mean(value * value, axis=-1, keepdims=True) + epsilon) * head_gain[...]
            gate = acc3[at, vs].astype(jnp.bfloat16).astype(jnp.float32)
            act[at, n_conv + h * HV : n_conv + (h + 1) * HV] = (value * (gate * jax.nn.sigmoid(gate))).astype(jnp.bfloat16)
        return carry

    lax.fori_loop(0, rows // 256, gla_finish, 0)

    def part_copy(b):
        at = pl.ds(pl.multiple_of(b * 256, 256), 256)
        return m.copy(psend.at[b], other_out.at[:, at], part_send, part_recv, me, 1 - tp)

    def project(p, yy, core):
        weight = jnp.concatenate([wo[p, yy, 0], wo[p, yy, 1]], axis=1)
        left = act[pl.ds(pl.multiple_of(core * half, half), half), :]
        return dot(left, weight, ((1,), (0,))).astype(jnp.bfloat16)

    def out_pieces(j):
        p = m.piece(j)

        def theirs(yy, carry):
            psend[p * 2 + yy] = project(p, yy, 1 - tp)
            return carry

        def ours(yy, carry):
            part_copy(p * 2 + yy).start()
            own_out[:, pl.ds(pl.multiple_of((p * 2 + yy) * 256, 256), 256)] = project(p, yy, tp)
            return carry

        arrived(3, p)
        arrived(4, p)
        lax.fori_loop(0, 2, theirs, 0)
        lax.fori_loop(0, 2, ours, 0)

    def rows_of(core):
        return pl.ds(pl.multiple_of(core * half, half), half)

    def last_part(yy, low, high):
        p = m.piece(3)
        weight = jnp.concatenate([wo[p, yy, 0, low:high, :], wo[p, yy, 1, low:high, :]], axis=1)
        return lambda core: dot(act[rows_of(core), low:high], weight, ((1,), (0,)))

    def last_begin():
        def body(yy, carry):
            part = last_part(yy, 0, 2 * early)
            at = pl.ds(pl.multiple_of(yy * 256, 256), 256)
            acc2[0:half, at] = part(1 - tp)
            acc2[half:, at] = part(tp)
            return carry

        arrived(3, m.piece(3))
        lax.fori_loop(0, 2, body, 0)

    def last_end():
        b = m.piece(3) * 2

        def theirs(yy, carry):
            at = pl.ds(pl.multiple_of(yy * 256, 256), 256)
            part = last_part(yy, 2 * early, 2 * early + 2 * late)
            psend[b + yy] = (acc2[0:half, at] + part(1 - tp)).astype(jnp.bfloat16)
            return carry

        def ours(yy, carry):
            part_copy(b + yy).start()
            at = pl.ds(pl.multiple_of(yy * 256, 256), 256)
            part = last_part(yy, 2 * early, 2 * early + 2 * late)
            own_out[:, pl.ds(pl.multiple_of((b + yy) * 256, 256), 256)] = (acc2[half:, at] + part(tp)).astype(jnp.bfloat16)
            return carry

        arrived(4, m.piece(3))
        lax.fori_loop(0, 2, theirs, 0)
        lax.fori_loop(0, 2, ours, 0)

    def drain_early():
        swap.wait_send()
        stats.wait_send()

        @pl.when(me < 15)
        def _():
            halo.wait_send()

        for end in near_ends:
            end.wait_send()
        for k in (1, 2, 3):
            @pl.when(z + k <= 3)
            def _():
                far_end(k).wait_send()

        for f in (b1, b2, *pairs[0], *pairs[1]):
            f.drain_first()
            f.drain_last()
        for f in (*pairs[2], *pairs[3]):
            f.drain_first()
        whole.drain()
        for pair in lines:
            for line in pair:
                line.drain()

    out_pieces(0)

    @pl.when(at_end)
    def _():
        pass_on(3, 2)

    out_pieces(1)
    pass_on(3, 3)
    last_begin()
    out_pieces(2)
    drain_early()
    last_end()

    for f in (*pairs[2], *pairs[3]):
        f.drain_last()
    m.copy(psend, psend, part_send, part_recv, me, 1 - tp).wait_send()
    m.copy(other_out, other_out, part_send, part_recv, me, 1 - tp).wait_recv()


def fused_layer(
    tokens, norm_gain, w_conv_a, w_conv_gate, conv_weight, conv_gain, w_query, w_key, w_value, w_outgate,
    w_decay, decay_bias, decay_extra, head_gain, init_state, w_out_conv, w_out_gla,
):
    rows, width = tokens.shape
    depth = w_query.shape[0]
    n_key = w_query.shape[1]
    n_conv = w_conv_a.shape[1]
    cols = w_out_conv.shape[1]
    half = rows // 2
    pad = 32
    bf16, f32 = jnp.bfloat16, jnp.float32
    dma = pltpu.SemaphoreType.DMA
    vm = pl.BlockSpec(memory_space=pltpu.VMEM)
    hbm = pl.BlockSpec(memory_space=pl.ANY)
    share = pltpu.VMEM((half, 2 * width), bf16)
    own, other = pl.pallas_call(
        layer_kernel,
        out_shape=[share, share],
        in_specs=[hbm, vm, hbm, hbm, vm, vm, hbm, hbm, hbm, hbm, hbm, vm, hbm, vm, vm, hbm, hbm],
        out_specs=[vm, vm],
        scratch_shapes=[
            pltpu.VMEM((4, 2, 2, depth, 5 * n_key), bf16),
            pltpu.VMEM((4, 2, 2, depth, 2 * n_conv), bf16),
            pltpu.VMEM((4, 2, 2, depth, n_conv), bf16),
            pltpu.VMEM((4, 2, 2, 2 * n_conv, cols), bf16),
            pltpu.VMEM((2, rows, width), bf16),
            pltpu.VMEM((rows, 2 * width), bf16),
            pltpu.VMEM((rows, 5 * n_key), f32),
            pltpu.VMEM((rows, 2 * n_conv), f32),
            pltpu.VMEM((rows, n_conv), f32),
            pltpu.VMEM((rows, n_key), f32),
            pltpu.VMEM((n_conv // 128, rows + pad, 128), f32),
            pltpu.VMEM((rows, n_conv), f32),
            pltpu.VMEM((rows, n_key), bf16),
            pltpu.VMEM((rows, 2 * n_conv), bf16),
            pltpu.VMEM((8, half, 256), bf16),
            pltpu.VMEM((pad, n_conv), bf16),
            pltpu.VMEM((pad, n_conv), bf16),
            pltpu.VMEM((rows, 128), f32),
            pltpu.VMEM((rows, 128), f32),
            pltpu.VMEM((8, HV + 16, n_key), bf16),
            pltpu.VMEM((HV, n_key), f32),
            pltpu.VMEM((1, n_key), f32),
            pltpu.VMEM((HV + 8, n_key), f32),
            dma((11,)), dma((10,)), dma((16,)), dma((10,)), dma((5, 4)), dma((9, 5)), dma((9, 4)),
            dma((3,)), dma((3,)), dma((6,)), dma((8,)), dma(()), dma(()),
        ],
        compiler_params=pltpu.CompilerParams(collective_id=0, has_side_effects=True, vmem_limit_bytes=56 * 2**20),
        name="layer",
    )(
        tokens, norm_gain[None, :], w_conv_a, w_conv_gate, conv_weight, conv_gain[None, :], w_query, w_key, w_value,
        w_outgate, w_decay, decay_bias[None, :], decay_extra, head_gain[None, :], init_state, w_out_conv, w_out_gla,
    )
    return (own.astype(f32) + other.astype(f32)).astype(bf16)


def local_kernel(heads, pieces, q_ref, k_ref, v_ref, pre_ref, extra_ref, bias_ref, attn_ref, since_ref, end_ref, log_ref, state, prefix):
    step = pl.program_id(0)

    @pl.when(step == 0)
    def _():
        state[...] = jnp.zeros_like(state)
        prefix[...] = jnp.zeros_like(prefix)

    rows = lax.broadcasted_iota(jnp.int32, (BLOCK, BLOCK), 0)
    columns = lax.broadcasted_iota(jnp.int32, (BLOCK, BLOCK), 1)
    causal = rows >= columns
    lower = causal.astype(jnp.float32)
    for piece in range(pieces):
        at = pl.ds(piece * BLOCK, BLOCK)
        pre = pre_ref[at, :] + bias_ref[...]
        logs = jax.nn.log_sigmoid(pre) / gate_divisor + extra_ref[at, :]
        cum = lax.dot_general(
            lower, logs, (((1,), (0,)), ((), ())), precision=lax.Precision.HIGHEST, preferred_element_type=jnp.float32
        )
        total = cum[BLOCK - 1 :, :]
        middle = cum[BLOCK // 2 - 1 : BLOCK // 2, :]
        query = q_ref[at, :].astype(jnp.float32) * HK ** (-0.5)
        keys = k_ref[at, :].astype(jnp.float32)
        decayed = query * jnp.exp(cum)
        since_ref[at, :] = (decayed * jnp.exp(prefix[...])).astype(jnp.bfloat16)
        decayed = decayed.astype(jnp.bfloat16)
        query = (query * jnp.exp(cum - middle)).astype(jnp.bfloat16)
        inverse = (keys * jnp.exp(middle - cum)).astype(jnp.bfloat16)
        to_end = (keys * jnp.exp(total - cum)).astype(jnp.bfloat16)
        entering = state[...].astype(jnp.bfloat16)
        added = []
        for h in range(heads):
            ks, vs = slice(h * HK, (h + 1) * HK), slice(h * HV, (h + 1) * HV)
            values = v_ref[at, vs]
            scores = jnp.where(causal, dot(query[:, ks], inverse[:, ks], ((1,), (1,))), 0.0)
            attn_ref[at, vs] = dot(scores.astype(jnp.bfloat16), values, ((1,), (0,))) + dot(
                decayed[:, ks], entering[:, ks], ((1,), (1,))
            )
            added.append(dot(values, to_end[:, ks], ((0,), (0,))))
        added = added[0] if heads == 1 else jnp.concatenate(added, axis=1)
        state[...] = state[...] * jnp.exp(total) + added
        prefix[...] = prefix[...] + total
    end_ref[...] = state[...]
    log_ref[...] = prefix[...]


def gla_local(query, keys, values, decay_pre, decay_extra, decay_bias):
    rows, width = query.shape
    heads = width // HK
    pieces = 4
    tile = pieces * BLOCK

    def tiled(array):
        return pl.BlockSpec((tile, array.shape[1]), lambda i: (i, 0))

    def whole(shape):
        return pl.BlockSpec(shape, lambda i: (0, 0))

    return pl.pallas_call(
        functools.partial(local_kernel, heads, pieces),
        grid=(rows // tile,),
        in_specs=[tiled(query), tiled(keys), tiled(values), tiled(decay_pre), tiled(decay_extra), whole((1, width))],
        out_specs=[tiled(values), tiled(query), whole((HV, width)), whole((1, width))],
        out_shape=[
            jax.ShapeDtypeStruct(values.shape, jnp.float32),
            jax.ShapeDtypeStruct(query.shape, jnp.bfloat16),
            jax.ShapeDtypeStruct((HV, width), jnp.float32),
            jax.ShapeDtypeStruct((1, width), jnp.float32),
        ],
        scratch_shapes=[pltpu.VMEM((HV, width), jnp.float32), pltpu.VMEM((1, width), jnp.float32)],
        cost_estimate=pl.CostEstimate(flops=10**10, bytes_accessed=10**7, transcendentals=10**6),
        name="gla_local",
    )(query, keys, values, decay_pre, decay_extra, decay_bias[None, :])


def finish_kernel(heads, size, where_ref, attn_ref, since_ref, gate_ref, ends_ref, init_ref, gain_ref, out_ref, state):
    me = where_ref[0]

    @pl.when(pl.program_id(0) == 0)
    def _():
        state[...] = init_ref[...]

        def one(device, carry):
            at = device
            decay = ends_ref[pl.ds(pl.multiple_of(at * size + HV, 16), 16), :].astype(jnp.float32)[:1]
            end = ends_ref[pl.ds(pl.multiple_of(at * size, 16), HV), :].astype(jnp.float32)
            state[...] = state[...] * decay + end
            return carry

        lax.fori_loop(0, me, one, 0)

    entering = state[...].astype(jnp.bfloat16)
    for h in range(heads):
        ks, vs = slice(h * HK, (h + 1) * HK), slice(h * HV, (h + 1) * HV)
        attn = attn_ref[:, vs] + dot(since_ref[:, ks], entering[:, ks], ((1,), (1,)))
        attn = attn * lax.rsqrt(jnp.mean(attn * attn, axis=-1, keepdims=True) + epsilon) * gain_ref[...]
        gate = gate_ref[:, vs].astype(jnp.float32)
        out_ref[:, vs] = (attn * (gate * jax.nn.sigmoid(gate))).astype(jnp.bfloat16)


def gla_finish(attn, since, out_gate, ends, init_state, head_gain, me):
    rows, width = since.shape
    heads = width // HK
    tile = 256

    def tiled(array):
        return pl.BlockSpec((tile, array.shape[1]), lambda i, w: (i, 0))

    def whole(array):
        return pl.BlockSpec(array.shape, lambda i, w: (0, 0))

    init = init_state.transpose(2, 0, 1).reshape(HV, width)
    gain = head_gain[None, :]
    return pl.pallas_call(
        functools.partial(finish_kernel, heads, HV + 16),
        grid_spec=pltpu.PrefetchScalarGridSpec(
            num_scalar_prefetch=1,
            grid=(rows // tile,),
            in_specs=[tiled(attn), tiled(since), tiled(out_gate), whole(ends), whole(init), whole(gain)],
            out_specs=tiled(attn),
            scratch_shapes=[pltpu.VMEM((HV, width), jnp.float32)],
        ),
        out_shape=jax.ShapeDtypeStruct(attn.shape, jnp.bfloat16),
        cost_estimate=pl.CostEstimate(flops=3 * 10**9, bytes_accessed=10**7, transcendentals=10**6),
        name="gla_finish",
    )(me[None], attn, since, out_gate, ends, init, gain)


def conv_branch(gated, conv_weight, conv_gain):
    taps = conv_weight.shape[0]
    row_count = gated.shape[0]
    count = lax.axis_size("sp")
    earlier = lax.ppermute(gated[row_count - taps + 1 :], "sp", [(i, i + 1) for i in range(count - 1)])
    extended = jnp.concatenate([earlier, gated], axis=0).astype(jnp.float32)
    conv_sum = jnp.zeros(gated.shape, jnp.float32)
    for tap in range(taps):
        conv_sum = conv_sum + conv_weight[tap][None, :] * extended[tap : tap + row_count]
    row_sums, row_squares = lax.psum((jnp.sum(conv_sum, axis=1), jnp.sum(conv_sum * conv_sum, axis=1)), "tp")
    mean_val = (row_sums / D_CONV)[:, None]
    square_mean = (row_squares / D_CONV)[:, None]
    conv_norm = (conv_sum - mean_val) * lax.rsqrt(square_mean - mean_val * mean_val + epsilon) * conv_gain
    return jax.nn.silu(conv_norm).astype(jnp.bfloat16)


def project(hidden, weight):
    return dot(hidden, weight, ((1,), (0,)))


def plain_layer(
    tokens, norm_gain, w_conv_a, w_conv_gate, conv_weight, conv_gain, w_query, w_key, w_value, w_outgate,
    w_decay, decay_bias, decay_extra, head_gain, init_state, w_out_conv, w_out_gla,
):
    me = lax.axis_index("sp")

    def gather(shard):
        return lax.all_gather(shard, "sp", axis=0, tiled=True)

    widened = lax.all_gather(tokens, "tp", axis=1, tiled=True).astype(jnp.float32)
    normed = (
        widened * lax.rsqrt(jnp.mean(widened * widened, axis=-1, keepdims=True) + epsilon) * norm_gain
    ).astype(jnp.bfloat16)
    half = w_query.shape[1]
    conv_a = project(normed, gather(w_conv_a)).astype(jnp.bfloat16)
    conv_gate = project(normed, gather(w_conv_gate)).astype(jnp.bfloat16)
    full_qkd = gather(jnp.concatenate([w_query, w_key, w_decay], axis=1))
    full_v = gather(w_value)
    gated = (conv_a.astype(jnp.float32) * jax.nn.sigmoid(conv_gate.astype(jnp.float32))).astype(jnp.bfloat16)
    conv_out = conv_branch(gated, conv_weight, conv_gain)
    query_keys = project(normed, full_qkd[:, : 2 * half]).astype(jnp.bfloat16)
    decay_pre = project(normed, full_qkd[:, 2 * half :])
    values = project(normed, full_v).astype(jnp.bfloat16)
    attn, since, end, end_log = gla_local(
        query_keys[:, :half], query_keys[:, half:], values, decay_pre, decay_extra, decay_bias
    )
    packed = jnp.concatenate([end, jnp.broadcast_to(jnp.exp(end_log), (16, half))], axis=0).astype(jnp.bfloat16)
    ends = gather(packed)
    out_gate = project(normed, gather(w_outgate)).astype(jnp.bfloat16)
    gla_out = gla_finish(attn, since, out_gate, ends, init_state, head_gain, me)
    total = dot(conv_out, gather(w_out_conv.T), ((1,), (1,))) + dot(gla_out, gather(w_out_gla.T), ((1,), (1,)))
    return lax.psum_scatter(total.astype(jnp.bfloat16), "tp", scatter_dimension=0, tiled=True)


def per_device(*arrays):
    if folded(lax.axis_size("sp"), lax.axis_size("tp")):
        return fused_layer(*arrays)
    return plain_layer(*arrays)


def solution(mesh):
    placed = (
        P("sp", "tp"), P(), P("sp", "tp"), P("sp", "tp"), P(None, "tp"), P("tp"), P("sp", "tp"), P("sp", "tp"),
        P("sp", "tp"), P("sp", "tp"), P("sp", "tp"), P("tp"), P("sp", "tp"), P(), P("tp", None, None),
        P("tp", "sp"), P("tp", "sp"),
    )
    return jax.shard_map(
        per_device, mesh=mesh, in_specs=placed, out_specs=P(("sp", "tp"), None), check_vma=False
    )
```
